128 devices in a mesh: sp: 32 (over z, y, core), tp: 4 (over x).
Axes of the slice: x: 4, y: 4, z: 4, core: 2. Of those that a mesh axis runs over, the one named last changes fastest.
Arguments:
- queries: bfloat16 [24576, 1024], P('sp', 'tp'), may hold values from -6 to 6
- keys: bfloat16 [24576, 1024], P('sp', 'tp'), may hold values from -6 to 6
- values: bfloat16 [24576, 2048], P('sp', 'tp'), may hold values from -6 to 6
- out_gate: bfloat16 [24576, 2048], P('sp', 'tp'), may hold values from -6 to 6
- input_gates: float32 [2, 4, 24576], P(None, 'tp', 'sp'), may hold values from -4 to 300
- forget_gates: float32 [2, 4, 24576], P(None, 'tp', 'sp'), may hold values from -1 to 16
- doc_ids: int32 [24576], P('sp'), may hold values from 0 to 15, never falling along the last dimension, each value on 1 to 3072 neighbouring positions
- head_gain: float32 [2048], P('tp'), may hold values from 0.1 to 1.9
- w_out: bfloat16 [2048, 2048], P('tp'), may hold values from -0.25 to 0.25
- resid: bfloat16 [24576, 2048], P(('sp', 'tp')), may hold values from -30 to 30
- norm_gain: float32 [2048], replicated, may hold values from 0.1 to 1.9
- w_up: bfloat16 [2048, 8192], P('sp', 'tp'), may hold values from -0.125 to 0.125
- w_down: bfloat16 [8192, 2048], P('tp', 'sp'), may hold values from -0.0625 to 0.0625
Outputs:
- layer_out: bfloat16 [24576, 2048], P(('sp', 'tp'))
The draws below stay inside these ranges and needn't reach their ends.
Inputs may be any that keep to these rules, and one draw needn't show every extreme that they name: `doc_ids`: document numbers never fall along the positions.
All inputs are finite; a program needn't handle non-finite values.
Results may differ from the reference program's by a relative error of at most 0.013.
Values may be sent and summed in bfloat16 or wider, within the bound.
A program may use at most 128 MiB of HBM per device.

```python
import math
import jax
import jax.numpy as jnp
import numpy as np
from jax import lax

D = 2048
HEADS = 4
DQK = 256
DV = 512
FF = 8192
TOK_DEV = 768
TOKENS = 24576
N_SP = 32


def draw_resid(key, part):
    keys = jax.random.split(key, 2)
    base = jax.random.normal(keys[0], (TOKENS, D), jnp.float32)
    rows = jnp.exp(jax.random.uniform(keys[1], (TOKENS, 1), jnp.float32, -1.2, 1.2))
    cols = jnp.exp(jnp.linspace(-0.9, 0.9, D, dtype=jnp.float32))[None, :]
    return jnp.clip(base * rows * cols, -30.0, 30.0).astype(jnp.bfloat16)


def draw_input_gates(key, part):
    keys = jax.random.split(key, 1)
    gates = jnp.clip(jax.random.normal(keys[0], (2, HEADS, TOKENS), jnp.float32), -4.0, 4.0)
    return gates


def draw_forget_gates(key, part):
    keys = jax.random.split(key, 6)
    share = 0.5
    slow = jax.random.uniform(keys[0], (2, HEADS, 1), jnp.float32) < share
    fast_rate = jnp.exp(jax.random.uniform(keys[1], (2, HEADS, 1), jnp.float32, jnp.log(1.0 / 100.0), jnp.log(1.0 / 30.0)))
    rate = jnp.where(slow, 0.3 / TOKENS, fast_rate)
    factor = jnp.exp(jax.random.uniform(keys[2], (2, HEADS, TOKENS // TOK_DEV), jnp.float32, -0.7, 0.7))
    factor = jnp.repeat(factor, TOK_DEV, axis=2)
    noise = jnp.clip(jax.random.normal(keys[3], (2, HEADS, TOKENS), jnp.float32), -3.0, 3.0)
    pre = -jnp.log(rate * factor) + noise
    spots = jax.random.randint(keys[4], (2, HEADS, 3), 0, TOKENS)
    hit = jnp.any(jnp.arange(TOKENS)[None, None, None, :] == spots[..., None], axis=2)
    drop = jax.random.uniform(keys[5], (2, HEADS, TOKENS), jnp.float32, 0.0, 1.4)
    return jnp.where(hit, drop, pre)


def shard_levels(stream_key, extent, cuts, least, high):
    def one(axis_at, shards_of):
        steps = jax.random.uniform(jax.random.fold_in(jax.random.fold_in(stream_key, 6), axis_at), (shards_of,), jnp.float32, least / len(cuts), high / len(cuts))
        return jnp.repeat(jnp.exp(steps), extent[axis_at] // shards_of).reshape((-1,) + (1,) * (len(extent) - axis_at - 1))

    gain = one(*cuts[0])
    for cut in cuts[1:]:
        gain = gain * one(*cut)
    return gain


def profile(amount, total, limit, skew):
    loads = [(1 << 20) // math.isqrt(rank ** skew) + 1 for rank in range(2, amount + 1)]
    rest, holding = total - limit - (amount - 1), [1] * (amount - 1)
    while rest > 0:
        candidates = [i for i in range(amount - 1) if holding[i] < limit]
        pool, budget = sum([loads[i] for i in candidates]), rest
        for i in candidates:
            addition = min(limit - holding[i], max(1, budget * loads[i] // pool), rest)
            holding[i] = holding[i] + addition
            rest = rest - addition
    return np.array([limit] + holding)


def uneven_parts(own_key, count, total, bound, lean):
    if count == 2:
        one = jax.random.randint(own_key, (), max(1, total - bound), min(bound, total - 1) + 1)
        return jnp.stack([one, total - one])
    tallies = jnp.asarray(profile(count, total, bound, lean), jnp.int32)
    pairs = (count - 1) // 2
    source_of, sink = tallies[1:1 + 2 * pairs:2], tallies[2:2 + 2 * pairs:2]
    room = jnp.minimum(source_of - 1, bound - sink)
    moved = jax.random.randint(jax.random.fold_in(own_key, 1), (pairs,), 0, 1 << 20) % (room + 1)
    tallies = tallies.at[1:1 + 2 * pairs:2].set(source_of - moved).at[2:2 + 2 * pairs:2].set(sink + moved)
    return tallies[jax.random.permutation(jax.random.fold_in(own_key, 2), count)]


def gaussian(key, shape, deviation, most, cuts=(), kind=jnp.bfloat16):
    entries = deviation * jax.random.normal(key, shape, jnp.float32)
    if cuts:
        entries = entries * shard_levels(key, shape, cuts, -0.22, 0.18)
    return jnp.clip(entries, -most, most).astype(kind)


def setup_inputs(seed: int = 0) -> dict:
    arg_keys = jax.random.split(jax.random.key(seed), 14)
    queries = gaussian(arg_keys[0], (TOKENS, HEADS * DQK), 1.0, 6.0, ((0, 32), (1, 4)))
    keys = gaussian(arg_keys[1], (TOKENS, HEADS * DQK), 1.0, 6.0, ((0, 32), (1, 4)))
    values = gaussian(arg_keys[2], (TOKENS, HEADS * DV), 1.0, 6.0, ((0, 32), (1, 4)))
    out_gate = gaussian(arg_keys[3], (TOKENS, HEADS * DV), 1.0, 6.0, ((0, 32), (1, 4)))
    input_gates = draw_input_gates(jax.random.fold_in(arg_keys[13], 71), 0)
    forget_gates = draw_forget_gates(jax.random.fold_in(arg_keys[13], 71), 0)
    doc_ids = jnp.searchsorted(jnp.cumsum(uneven_parts(arg_keys[6], N_SP // 2, TOKENS, 4 * TOK_DEV, 0)), jnp.arange(TOKENS), side="right").astype(jnp.int32)
    head_gain = jnp.clip(1.0 + 0.18 * jax.random.normal(arg_keys[7], (HEADS * DV,), jnp.float32), 0.1, 1.9)
    w_out = gaussian(arg_keys[8], (HEADS * DV, D), (HEADS * DV // 4) ** -0.5, 0.25, ((0, 4),))
    resid = draw_resid(jax.random.fold_in(arg_keys[13], 71), 0)
    norm_gain = jnp.clip(1.0 + 0.18 * jax.random.normal(arg_keys[10], (D,), jnp.float32), 0.1, 1.9)
    w_up = gaussian(arg_keys[11], (D, FF), D ** -0.5, 0.125, ((0, 32), (1, 4)))
    w_down = gaussian(arg_keys[12], (FF, D), FF ** -0.5, 0.0625, ((0, 4), (1, 32)))
    return dict(queries=queries, keys=keys, values=values, out_gate=out_gate, input_gates=input_gates, forget_gates=forget_gates, doc_ids=doc_ids, head_gain=head_gain, w_out=w_out, resid=resid, norm_gain=norm_gain, w_up=w_up, w_down=w_down)


eps = 1e-06
far_low = -1e+30

def summarize(keys_blk, values_blk, in_gate, forget_pre, doc_pos):
    logf = jax.nn.log_sigmoid(forget_pre)
    cum = jnp.cumsum(logf)
    length = keys_blk.shape[0]
    last_doc = doc_pos[length - 1]
    tail = doc_pos == last_doc
    total = cum[length - 1]
    exponent = jnp.where(tail, total - cum + in_gate, far_low)
    peak = jnp.max(exponent)
    scaled = jnp.exp(exponent - peak)
    weighted = (keys_blk.astype(jnp.float32) * scaled[:, None]).astype(jnp.bfloat16)
    memory = jnp.einsum('sd,sv->dv', weighted.astype(jnp.float32), values_blk.astype(jnp.float32))
    norm_keys = lax.optimization_barrier(jnp.sum(weighted.astype(jnp.float32), axis=0))
    return (memory, norm_keys, peak, total, doc_pos[0], last_doc, jnp.zeros((), jnp.float32))

def emit(queries_blk, keys_blk, values_blk, in_gate, forget_pre, doc_pos, state):
    memory, norm_keys, top_in, total_in, first_in, last_in, empty_in = state
    scale = queries_blk.shape[1] ** (-0.5)
    logf = jax.nn.log_sigmoid(forget_pre)
    cum = jnp.cumsum(logf)
    length = queries_blk.shape[0]
    place = jnp.arange(length)
    keep = (place[:, None] >= place[None, :]) & (doc_pos[:, None] == doc_pos[None, :])
    exponent = jnp.where(keep, cum[:, None] - cum[None, :] + in_gate[None, :], far_low)
    usable = (doc_pos == last_in) & (empty_in < 0.5)
    carried = jnp.where(usable, cum + top_in, far_low)
    peak = jnp.maximum(carried, lax.optimization_barrier(jnp.max(exponent, axis=1)))
    scores = jnp.einsum('td,sd->ts', queries_blk.astype(jnp.float32), keys_blk.astype(jnp.float32)) * scale
    weights = jnp.where(keep, scores * jnp.exp(exponent - peak[:, None]), 0.0)
    inter = jnp.where(usable, jnp.exp(carried - peak), 0.0)
    query_wide = queries_blk.astype(jnp.float32)
    numer = jnp.dot(weights.astype(jnp.bfloat16), values_blk, preferred_element_type=jnp.float32)
    numer = numer + (inter * scale)[:, None] * jnp.dot(query_wide, memory, precision=lax.Precision.HIGHEST)
    denom = lax.optimization_barrier(jnp.sum(weights, axis=1)) + inter * scale * jnp.dot(query_wide, norm_keys, precision=lax.Precision.HIGHEST)
    return numer / jnp.maximum(jnp.abs(denom), 1.0)[:, None]

def combine(early, late):
    e_mem, e_keys, e_top, e_total, e_first, e_last, e_empty = early
    l_mem, l_keys, l_top, l_total, l_first, l_last, l_empty = late
    linked = (l_first == e_last) & (l_first == l_last) & (e_empty < 0.5)
    top = jnp.where(linked, jnp.maximum(l_top, e_top + l_total), l_top)
    early_part = jnp.where(linked, jnp.exp(jnp.minimum(e_top + l_total - top, 0.0)), 0.0)
    late_part = jnp.exp(l_top - top)
    joined = (early_part * e_mem + late_part * l_mem, early_part * e_keys + late_part * l_keys, top, e_total + l_total, jnp.where(e_empty > 0.5, l_first, e_first), l_last, jnp.zeros_like(l_empty))
    return tuple((jnp.where(l_empty > 0.5, a, b) for a, b in zip(early, joined)))

def run_direction(queries_h, keys_h, values_h, in_gate, forget_pre, doc_pos):

    def blocks(arr):
        return arr.reshape((N_SP, TOK_DEV) + arr.shape[1:])

    def step(state, pieces):
        q_blk, k_blk, v_blk, i_blk, f_blk, d_blk = pieces
        result = emit(q_blk, k_blk, v_blk, i_blk, f_blk, d_blk, state)
        return (combine(state, summarize(k_blk, v_blk, i_blk, f_blk, d_blk)), result)
    start = (jnp.zeros((DQK, DV), jnp.float32), jnp.zeros((DQK,), jnp.float32), jnp.full((), far_low, jnp.float32), jnp.zeros((), jnp.float32), jnp.full((), -1.0, jnp.float32), jnp.full((), -1.0, jnp.float32), jnp.ones((), jnp.float32))
    final, results = lax.scan(step, start, (blocks(queries_h), blocks(keys_h), blocks(values_h), blocks(in_gate), blocks(forget_pre), blocks(doc_pos)))
    return results.reshape(TOKENS, DV)

def reference(queries, keys, values, out_gate, input_gates, forget_gates, doc_ids, head_gain, w_out, resid, norm_gain, w_up, w_down):
    doc_pos = doc_ids.astype(jnp.float32)
    summed = jnp.zeros((TOKENS, D), jnp.float32)
    for head in range(HEADS):
        q_head = queries[:, head * DQK:(head + 1) * DQK]
        k_head = keys[:, head * DQK:(head + 1) * DQK]
        v_head = values[:, head * DV:(head + 1) * DV]
        forward = run_direction(q_head, k_head, v_head, input_gates[0, head], forget_gates[0, head], doc_pos)
        backward = run_direction(q_head[::-1], k_head[::-1], v_head[::-1], input_gates[1, head, ::-1], forget_gates[1, head, ::-1], doc_pos[::-1])[::-1]
        memory = forward + backward
        normed = memory * lax.rsqrt(lax.optimization_barrier(jnp.mean(memory * memory, axis=-1, keepdims=True)) + eps)
        gate = jax.nn.sigmoid(out_gate[:, head * DV:(head + 1) * DV].astype(jnp.float32))
        readout = (normed * head_gain[head * DV:(head + 1) * DV] * gate).astype(jnp.bfloat16)
        part = jnp.dot(readout, w_out[head * DV:(head + 1) * DV], preferred_element_type=jnp.float32).astype(jnp.bfloat16)
        summed = summed + lax.optimization_barrier(part).astype(jnp.float32)
    mixed = resid.astype(jnp.float32) + summed
    scaled = (mixed * lax.rsqrt(lax.optimization_barrier(jnp.mean(mixed * mixed, axis=-1, keepdims=True)) + eps) * norm_gain).astype(jnp.bfloat16)
    width = FF // HEADS

    def feed(rows_blk):
        hidden = jnp.square(jax.nn.relu(jnp.dot(rows_blk, w_up, preferred_element_type=jnp.float32))).astype(jnp.bfloat16)
        total = jnp.zeros((rows_blk.shape[0], D), jnp.float32)
        for group in range(HEADS):
            part = jnp.dot(hidden[:, group * width:(group + 1) * width], w_down[group * width:(group + 1) * width], preferred_element_type=jnp.float32).astype(jnp.bfloat16)
            total = total + lax.optimization_barrier(part).astype(jnp.float32)
        return total
    mixer = lax.map(feed, scaled.reshape(N_SP, TOK_DEV, D)).reshape(TOKENS, D)
    return (mixed + mixer).astype(jnp.bfloat16)
```

```python
import functools

import jax
import jax.numpy as jnp
from jax import lax
from jax.experimental import pallas as pl
from jax.experimental.pallas import tpu as pltpu
from jax.sharding import Mesh
from jax.sharding import PartitionSpec as P

MESH = pl.DeviceIdType.MESH
F32 = jnp.float32
BF16 = jnp.bfloat16
EPS = 1e-06
FAR_LOW = -1e30

T = 768
ROWS = 192
HALF = 96
DK = 256
DV = 512
D = 2048
SROWS = 272
SCALE = DK ** (-0.5)
N_SEMS = 96


class Copies:
    def __init__(self, send, recv, loc):
        self.send, self.recv, self.loc = send, recv, loc
        self.at = 0
        self.at_loc = 0
        self.all = []

    def remote(self, src, dst, dev):
        k = self.at
        self.at += 1
        assert k < N_SEMS
        c = pltpu.make_async_remote_copy(
            src_ref=src,
            dst_ref=dst,
            send_sem=self.send.at[k],
            recv_sem=self.recv.at[k],
            device_id=dev,
            device_id_type=MESH,
        )
        self.all.append(c)
        return c

    def local(self, src, dst):
        k = self.at_loc
        self.at_loc += 1
        return pltpu.make_async_copy(src, dst, self.loc.at[k])


class Ring:
    def __init__(self, cp, plus, minus, own, put_plus, put_minus, near0, near1, far0, far1):
        self.p0 = cp.remote(own(0), put_plus(0), plus)
        self.m0 = cp.remote(own(1), put_minus(1), minus)
        self.p1 = cp.remote(own(1), put_plus(1), plus)
        self.m1 = cp.remote(own(0), put_minus(0), minus)
        self.rp = cp.remote(near0, far0, plus)
        self.rm = cp.remote(near1, far1, minus)

    def start(self):
        for c in (self.p0, self.m0, self.p1, self.m1):
            c.start()

    def relay(self):
        self.p0.wait_recv()
        self.rp.start()
        self.m0.wait_recv()
        self.rm.start()

    def near(self):
        self.p1.wait_recv()
        self.m1.wait_recv()

    def far(self):
        self.rp.wait_recv()
        self.rm.wait_recv()


def slot_ring(cp, axis, p, slot):
    plus, minus = lax.rem(p + 1, 4), lax.rem(p + 3, 4)
    own = lambda h: slot(p, h)
    return Ring(
        cp, {axis: plus}, {axis: minus}, own, own, own,
        slot(minus, 0), slot(plus, 1), slot(minus, 0), slot(plus, 1),
    )


def roll_lanes(x, shift):
    return pltpu.roll(x, shift % T, 1)


def kernel(
    ig_ref, fg_ref, doc_ref, gain_ref, ngain_ref,
    q_h, k_h, v_h, og_h, wout_h, resid_h, wup_h, wdn_h,
    out_ref,
    wu, wd, wo, wa, wb, q, k, v, og, resid,
    arow, cols, numf, numb, dens,
    st_own, st_par, sc_pair, q_send, q_recv, sc_recv, cin,
    ro_out, ro, mixed, nrm, hid, part, acc2, add_in, rs_in,
    send_sem, recv_sem, loc_sem,
):
    z, y, c, x = (lax.axis_index(a) for a in ("z", "y", "c", "x"))
    other = 1 - c
    n = z * 4 + y
    n_up, n_dn = lax.rem(n + 1, 16), lax.rem(n + 15, 16)
    chip_up = {"z": lax.div(n_up, 4), "y": lax.rem(n_up, 4)}
    chip_dn = {"z": lax.div(n_dn, 4), "y": lax.rem(n_dn, 4)}
    partner = {"c": other}
    xp, xm, xf = lax.rem(x + 1, 4), lax.rem(x + 3, 4), lax.rem(x + 2, 4)
    cp = Copies(send_sem, recv_sem, loc_sem)

    l_wd = cp.local(wdn_h, wa)
    l_wu = cp.local(wup_h, wu.at[z, y, c])
    l_k = cp.local(k_h, k)
    l_v = cp.local(v_h, v)
    l_q = cp.local(q_h, q)
    l_wo = [cp.local(wout_h.at[pl.ds(256 * i, 256)], wo.at[x, i]) for i in range(2)]
    l_og = cp.local(og_h, og)
    l_re = cp.local(resid_h, resid)
    for l in (l_wd, l_wu, l_k, l_v, l_q, *l_wo, l_og, l_re):
        l.start()

    barrier = pltpu.get_barrier_semaphore()
    peers = (
        partner, {"y": lax.rem(y + 1, 4)}, {"y": lax.rem(y + 3, 4)}, {"z": lax.rem(z + 1, 4)},
        {"z": lax.rem(z + 3, 4)}, {"x": xp}, {"x": xm}, {"x": xf}, chip_up, chip_dn,
    )
    for dev in peers:
        pl.semaphore_signal(barrier, inc=1, device_id=dev, device_id_type=MESH)
    pl.semaphore_wait(barrier, len(peers))

    a1 = slot_ring(cp, "y", y, lambda p, h: wu.at[z, p, c, pl.ds(32 * h, 32)])
    a2 = slot_ring(cp, "z", z, lambda p, h: wu.at[p, :, c, pl.ds(32 * h, 32)])
    b1 = slot_ring(cp, "z", z, lambda p, h: wd.at[p, y, c, pl.ds(512 * h, 512)])
    b2 = slot_ring(cp, "y", y, lambda p, h: wd.at[:, p, c, pl.ds(512 * h, 512)])
    wr = slot_ring(cp, "x", x, lambda p, h: wo.at[p, c, pl.ds(128 * h, 128)])

    l_wd.wait()
    d_wd = cp.remote(wa.at[pl.ds(pl.multiple_of(1024 * other, 1024), 1024)], wb, partner)
    d_wd.start()
    l_wu.wait()
    a1.start()
    for l in l_wo:
        l.wait()
    wr.start()

    def row(ref, i):
        return jnp.broadcast_to(ref[i], (8, T))

    lane = lax.broadcasted_iota(jnp.int32, (8, T), 1)
    rowi = lax.broadcasted_iota(jnp.int32, (8, T), 0)
    doc = jnp.broadcast_to(doc_ref[...], (8, T)).astype(F32)

    def log_sigmoid(f):
        return jnp.minimum(f, 0.0) - jnp.log1p(jnp.exp(-jnp.abs(f)))

    cumf, cumb = log_sigmoid(row(fg_ref, 0)), log_sigmoid(row(fg_ref, 1))
    sh = 1
    while sh < T:
        cumf = cumf + jnp.where(lane >= sh, roll_lanes(cumf, sh), 0.0)
        cumb = cumb + jnp.where(lane < T - sh, roll_lanes(cumb, T - sh), 0.0)
        sh *= 2
    af, ab = row(ig_ref, 0) - cumf, row(ig_ref, 1) - cumb
    mf, mb = af, ab
    sh = 1
    while sh < T:
        same_f = (lane >= sh) & (roll_lanes(doc, sh) == doc)
        same_b = (lane < T - sh) & (roll_lanes(doc, T - sh) == doc)
        mf = jnp.where(same_f, jnp.maximum(mf, roll_lanes(mf, sh)), mf)
        mb = jnp.where(same_b, jnp.maximum(mb, roll_lanes(mb, T - sh)), mb)
        sh *= 2
    doc0, docl = doc[:, 0:1], doc[:, T - 1 : T]
    mxf, mxb = mf[:, T - 1 : T], mb[:, 0:1]
    totf, totb = cumf[:, T - 1 : T], cumb[:, 0:1]
    wf = jnp.where(doc == docl, jnp.exp(af - mxf), 0.0)
    wbk = jnp.where(doc == doc0, jnp.exp(ab - mxb), 0.0)
    arow[0] = af
    arow[1] = ab
    arow[2] = doc
    stack = jnp.where(
        rowi == 0, mf,
        jnp.where(rowi == 1, mb, jnp.where(rowi == 2, doc, jnp.where(rowi == 3, wf, wbk))),
    )
    cols[...] = stack.T
    r8 = lax.broadcasted_iota(jnp.int32, (8, 128), 0)
    scal = jnp.zeros((8, 128), F32)
    for i, val in enumerate((totf + mxf, totb + mxb, totf, totb, doc0, docl)):
        scal = jnp.where(r8 == i, jnp.broadcast_to(val, (8, 128)), scal)
    sc_pair[c] = scal

    d_wd.wait_recv()
    ei = lax.broadcasted_iota(jnp.int32, (64, 128), 0)
    ej = lax.broadcasted_iota(jnp.int32, (64, 128), 1)
    put_own = jnp.where(ej == ei + 64 * c, 1.0, 0.0).astype(BF16)
    put_par = jnp.where(ej == ei + 64 * other, 1.0, 0.0).astype(BF16)
    mine = wa[pl.ds(pl.multiple_of(1024 * c, 1024), 1024), :]
    wd[z, y, c] = (
        jnp.dot(mine, put_own, preferred_element_type=F32)
        + jnp.dot(wb[...], put_par, preferred_element_type=F32)
    ).astype(BF16)
    b1.start()

    l_k.wait()
    l_v.wait()
    keys = k[...].astype(F32)
    for d in range(2):
        weighted = (keys * cols[:, 3 + d : 4 + d]).astype(BF16)
        st = lax.dot_general(
            v[...], weighted, (((0,), (0,)), ((), ())), preferred_element_type=F32
        ).astype(BF16)
        norm = jnp.sum(weighted.astype(F32), axis=0, keepdims=True)
        tail = jnp.broadcast_to(norm, (16, DK)).astype(BF16)
        for h in range(2):
            st_own[d, h, 0:256, :] = st[256 * h : 256 * h + 256]
            st_own[d, h, 256:SROWS, :] = tail
    d_st = cp.remote(st_own, st_par, partner)
    d_sc = cp.remote(sc_pair.at[c], sc_pair.at[c], partner)
    d_sc.start()
    d_st.start()
    a1.relay()

    def pick(ref, i):
        return ref[i : i + 1, 0:1]

    def pair_terms(s0, s1, d):
        early, late = (s0, s1) if d == 0 else (s1, s0)
        e_last = early[5 - d : 6 - d, 0:1]
        l_first, l_last = late[4 + d : 5 + d, 0:1], late[5 - d : 6 - d, 0:1]
        linked = (l_first == e_last) & (l_first == l_last)
        e_top = early[d : d + 1, 0:1] + late[2 + d : 3 + d, 0:1]
        l_top = late[d : d + 1, 0:1]
        top = jnp.where(linked, jnp.maximum(l_top, e_top), l_top)
        f_early = jnp.where(linked, jnp.exp(jnp.minimum(e_top - top, 0.0)), 0.0)
        f_late = jnp.exp(l_top - top)
        total = early[2 + d : 3 + d, 0:1] + late[2 + d : 3 + d, 0:1]
        return top, total, f_early, f_late, l_last

    d_sc.wait_recv()
    d_st.wait_recv()
    s0, s1 = sc_pair[0], sc_pair[1]
    cq = []
    cs = []
    for d in range(2):
        pos = c if d == 0 else other
        _, _, f_early, f_late, _ = pair_terms(s0, s1, d)
        f_own = jnp.where(pos == 0, f_early, f_late)
        f_par = jnp.where(pos == 0, f_late, f_early)
        q_send[d] = (f_own * st_own[d, c].astype(F32) + f_par * st_par[d, c].astype(F32)).astype(BF16)
        to = chip_up if d == 0 else chip_dn
        cs.append(cp.remote(sc_pair, sc_recv.at[d, 0], to))
        cq.append(cp.remote(q_send.at[d], q_recv.at[d, 0, c], to))
        cs[-1].start()
        cq[-1].start()

    l_q.wait()

    def intra(r0, size):
        qb = q[r0 : r0 + size, :]
        mfc, mbc, dc = (cols[r0 : r0 + size, i : i + 1] for i in range(3))
        score = (
            lax.dot_general(qb, k[...], (((1,), (1,)), ((), ())), preferred_element_type=F32)
            * SCALE
        )
        for d in range(2):
            lo, hi = (0, r0 + size) if d == 0 else (r0, T)
            ti = r0 + lax.broadcasted_iota(jnp.int32, (size, hi - lo), 0)
            si = lo + lax.broadcasted_iota(jnp.int32, (size, hi - lo), 1)
            keep = ((si <= ti) if d == 0 else (si >= ti)) & (arow[2, 0:1, lo:hi] == dc)
            e = jnp.exp(jnp.minimum(arow[d, 0:1, lo:hi] - (mfc if d == 0 else mbc), 0.0))
            w = jnp.where(keep, score[:, lo:hi] * e, 0.0)
            dens[r0 : r0 + size, d : d + 1] = jnp.sum(w, axis=1, keepdims=True)
            num = jnp.dot(w.astype(BF16), v[lo:hi, :], preferred_element_type=F32)
            (numf if d == 0 else numb)[r0 : r0 + size, :] = num

    intra(0, 256)
    a1.near()
    a1.far()
    a2.start()
    intra(256, 256)
    b1.relay()
    intra(512, 256)

    rq, rs, dq = [], [], []
    for d in range(2):
        to = chip_up if d == 0 else chip_dn
        rs.append(cp.remote(sc_recv.at[d, 0], sc_recv.at[d, 1], to))
        rq.append(cp.remote(q_recv.at[d, 0, c], q_recv.at[d, 1, c], to))
        dq.append(cp.remote(q_recv.at[d, 0, c], q_recv.at[d, 0, c], partner))
        cs[d].wait_recv()
        rs[d].start()
        cq[d].wait_recv()
        rq[d].start()
        dq[d].start()
    b1.near()
    b1.far()
    b2.start()
    wr.relay()

    fw = [
        cp.remote(wu.at[z, :, c], wu.at[z, :, c], partner),
        cp.remote(wd.at[:, y, c], wd.at[:, y, c], partner),
    ]
    for f in fw:
        f.start()

    dq2 = []
    for d in range(2):
        rs[d].wait_recv()
        rq[d].wait_recv()
        dq2.append(cp.remote(q_recv.at[d, 1, c], q_recv.at[d, 1, c], partner))
        dq2[d].start()

    scal_in = []
    for d in range(2):
        pos = c if d == 0 else other
        chip = n if d == 0 else 15 - n
        own_s = sc_pair[c]
        par_s = sc_pair[other]
        first = own_s[4 + d : 5 + d, 0:1]
        t1, tot1, _, _, last1 = pair_terms(sc_recv[d, 0, 0], sc_recv[d, 0, 1], d)
        t2, _, _, _, last2 = pair_terms(sc_recv[d, 1, 0], sc_recv[d, 1, 1], d)
        l0 = (par_s[5 - d : 6 - d, 0:1] == first) & (pos == 1)
        l1 = (last1 == first) & (chip >= 1)
        l2 = (last2 == first) & (chip >= 2)
        shift = jnp.where(pos == 1, par_s[2 + d : 3 + d, 0:1], 0.0)
        e0 = jnp.where(l0, par_s[d : d + 1, 0:1], FAR_LOW)
        e1 = jnp.where(l1, t1 + shift, FAR_LOW)
        e2 = jnp.where(l2, t2 + tot1 + shift, FAR_LOW)
        top = jnp.maximum(e0, jnp.maximum(e1, e2))
        g0 = jnp.where(l0, jnp.exp(e0 - top), 0.0)
        g1 = jnp.where(l1, jnp.exp(e1 - top), 0.0)
        g2 = jnp.where(l2, jnp.exp(e2 - top), 0.0)
        late = jnp.where(pos == 1, 1.0, 0.0)
        linked = late * jnp.where(l0, 1.0, 0.0) + (1.0 - late) * jnp.where(l1, 1.0, 0.0)
        dq[d].wait_recv()
        dq2[d].wait_recv()
        for h in range(2):
            cin[d, h] = (
                g0 * st_par[d, h].astype(F32)
                + g1 * q_recv[d, 0, h].astype(F32)
                + g2 * q_recv[d, 1, h].astype(F32)
            ).astype(BF16)
        scal_in.append((top, linked, first))

    l_og.wait()
    ca = []
    for step, to in enumerate((xf, xp, xm, x)):
        r0 = pl.multiple_of(to * ROWS, 64)
        rows = pl.ds(r0, ROWS)
        qb = q[rows, :]
        qw = qb.astype(F32)
        dc = cols[rows, 2:3]
        memory = None
        for d in range(2):
            top, linked, first = scal_in[d]
            m_loc = cols[rows, d : d + 1]
            usable = jnp.where(dc == first, linked, 0.0) > 0.5
            m = jnp.where(usable, jnp.maximum(m_loc, top), m_loc)
            keep = jnp.exp(m_loc - m)
            inter = jnp.where(usable, jnp.exp(jnp.minimum(top - m, 0.0)), 0.0) * SCALE
            nt = (((1,), (1,)), ((), ()))
            qc = jnp.concatenate(
                [
                    lax.dot_general(qb, cin[d, h, 0:256, :], nt, preferred_element_type=F32)
                    for h in range(2)
                ],
                axis=1,
            )
            norm = cin[d, 0, 256:257, :].astype(F32)
            num = keep * (numf if d == 0 else numb)[rows, :] + inter * qc
            den = keep * dens[rows, d : d + 1] + inter * jnp.sum(qw * norm, axis=1, keepdims=True)
            h_dir = num / jnp.maximum(jnp.abs(den), 1.0)
            memory = h_dir if memory is None else memory + h_dir
        normed = memory * lax.rsqrt(jnp.mean(memory * memory, axis=1, keepdims=True) + EPS)
        gate = 1.0 / (1.0 + jnp.exp(-og[rows, :].astype(F32)))
        readout = (normed * gain_ref[...] * gate).astype(BF16)
        if step < 3:
            ro_out[step] = readout
            cc = cp.remote(ro_out.at[step], ro.at[x], {"x": to})
            cc.start()
            ca.append(cc)
        else:
            ro[x] = readout

    a2.relay()
    wr.near()
    fo = [cp.remote(wo.at[p, c], wo.at[p, c], partner) for p in (xm, xp, xf)]
    fo[0].start()
    fo[1].start()
    b2.relay()
    wr.far()
    fo[2].start()
    l_re.wait()
    for cc in ca:
        cc.wait_recv()
    for f in fo:
        f.wait_recv()

    mixed[...] = resid[...].astype(F32)

    @pl.loop(0, 4)
    def _(t):
        cs_ = pl.ds(pl.multiple_of(t * 512, 512), 512)
        tot = mixed[:, cs_]
        for h in range(4):
            w = wo[h, :, :, cs_].reshape(512, 512)
            tot = tot + jnp.dot(ro[h], w, preferred_element_type=F32).astype(BF16).astype(F32)
        mixed[:, cs_] = tot

    mx = mixed[...]
    factor = lax.rsqrt(jnp.mean(mx * mx, axis=1, keepdims=True) + EPS)
    nrm[0] = (mx * factor * ngain_ref[...]).astype(BF16)

    h01 = lambda j, h: nrm.at[j, pl.ds(HALF * h, HALF)]
    ag = Ring(
        cp, {"x": xp}, {"x": xm},
        lambda h: h01(0, h),
        lambda h: h01(1 + h, 0),
        lambda h: h01(2 - h, 1),
        h01(1, 0), h01(1, 1), h01(3, 0), h01(3, 1),
    )
    ag.start()

    def forward(ring_wait, refs):
        ring_wait()
        out = [cp.remote(r, r, partner) for r in refs]
        for f in out:
            f.start()
        return out

    zp, zm, zf = lax.rem(z + 1, 4), lax.rem(z + 3, 4), lax.rem(z + 2, 4)
    yp, ym, yf = lax.rem(y + 1, 4), lax.rem(y + 3, 4), lax.rem(y + 2, 4)
    fw += forward(a2.near, [wu.at[zp, :, c], wu.at[zm, :, c]])
    fw += forward(b2.near, [wd.at[:, yp, c], wd.at[:, ym, c]])
    fw += forward(a2.far, [wu.at[zf, :, c]])
    fw += forward(b2.far, [wd.at[:, yf, c]])
    for f in fw:
        f.wait_recv()

    def mixer(j, sink):
        rows = nrm[j]

        @pl.loop(0, 4)
        def _(t):
            cs_ = pl.ds(pl.multiple_of(t * 512, 512), 512)
            w = wu[:, :, :, :, cs_].reshape(D, 512)
            pre = jnp.maximum(jnp.dot(rows, w, preferred_element_type=F32), 0.0)
            hid[:, cs_] = (pre * pre).astype(BF16)

        @pl.loop(0, 4)
        def _(t):
            cs_ = pl.ds(pl.multiple_of(t * 512, 512), 512)
            w = jnp.concatenate([wd[t, i].reshape(D, 128) for i in range(4)], axis=1)
            sink(cs_, jnp.dot(hid[...], w, preferred_element_type=F32))

    def add_own(cs_, val):
        mixed[:, cs_] += val

    def to_part(j):
        def sink(cs_, val):
            part[j, :, cs_] = val.astype(BF16)

        return sink

    def to_acc(cs_, val):
        acc2[:, cs_] = val

    mixer(0, add_own)
    ag.relay()
    mixer(1, to_part(0))
    lo, hi = pl.ds(0, HALF), pl.ds(HALF, HALF)
    rs1 = [
        cp.remote(part.at[0, hi], rs_in.at[0, hi], {"x": xp}),
        cp.remote(part.at[0, lo], rs_in.at[1, lo], {"x": xm}),
    ]
    for r in rs1:
        r.start()
    ag.near()
    mixer(2, to_acc)
    ag.far()
    mixer(3, to_part(1))
    rs2 = [
        cp.remote(part.at[1, lo], add_in.at[0], {"x": xp}),
        cp.remote(part.at[1, hi], add_in.at[1], {"x": xm}),
    ]
    for r in rs2:
        r.start()
    rs3 = [
        cp.remote(part.at[2, hi], rs_in.at[0, lo], {"x": xp}),
        cp.remote(part.at[2, lo], rs_in.at[1, hi], {"x": xm}),
    ]
    rs2[0].wait_recv()
    part[2, HALF:ROWS, :] = (acc2[HALF:ROWS, :] + add_in[0].astype(F32)).astype(BF16)
    rs3[0].start()
    rs2[1].wait_recv()
    part[2, 0:HALF, :] = (acc2[0:HALF, :] + add_in[1].astype(F32)).astype(BF16)
    rs3[1].start()
    for r in (*rs1, *rs3):
        r.wait_recv()
    out_ref[...] = (mixed[...] + rs_in[0].astype(F32) + rs_in[1].astype(F32)).astype(BF16)
    for r in cp.all:
        r.wait_send()


def shards(
    queries, keys, values, out_gate, input_gates, forget_gates, doc_ids,
    head_gain, w_out, resid, norm_gain, w_up, w_down,
):
    vmem = pl.BlockSpec(memory_space=pltpu.VMEM)
    hbm = pl.BlockSpec(memory_space=pl.ANY)
    return pl.pallas_call(
        kernel,
        out_shape=jax.ShapeDtypeStruct((ROWS, D), BF16),
        in_specs=[vmem] * 5 + [hbm] * 8,
        out_specs=vmem,
        scratch_shapes=[
            pltpu.VMEM((4, 4, 2, 64, D), BF16),
            pltpu.VMEM((4, 4, 2, 1024, 128), BF16),
            pltpu.VMEM((4, 2, 256, D), BF16),
            pltpu.VMEM((D, 64), BF16),
            pltpu.VMEM((1024, 64), BF16),
            pltpu.VMEM((T, DK), BF16),
            pltpu.VMEM((T, DK), BF16),
            pltpu.VMEM((T, DV), BF16),
            pltpu.VMEM((T, DV), BF16),
            pltpu.VMEM((ROWS, D), BF16),
            pltpu.VMEM((3, 8, T), F32),
            pltpu.VMEM((T, 8), F32),
            pltpu.VMEM((T, DV), F32),
            pltpu.VMEM((T, DV), F32),
            pltpu.VMEM((T, 8), F32),
            pltpu.VMEM((2, 2, SROWS, DK), BF16),
            pltpu.VMEM((2, 2, SROWS, DK), BF16),
            pltpu.VMEM((2, 8, 128), F32),
            pltpu.VMEM((2, SROWS, DK), BF16),
            pltpu.VMEM((2, 2, 2, SROWS, DK), BF16),
            pltpu.VMEM((2, 2, 2, 8, 128), F32),
            pltpu.VMEM((2, 2, SROWS, DK), BF16),
            pltpu.VMEM((3, ROWS, DV), BF16),
            pltpu.VMEM((4, ROWS, DV), BF16),
            pltpu.VMEM((ROWS, D), F32),
            pltpu.VMEM((4, ROWS, D), BF16),
            pltpu.VMEM((ROWS, D), BF16),
            pltpu.VMEM((3, ROWS, D), BF16),
            pltpu.VMEM((ROWS, D), F32),
            pltpu.VMEM((2, HALF, D), BF16),
            pltpu.VMEM((2, ROWS, D), BF16),
            pltpu.SemaphoreType.DMA((N_SEMS,)),
            pltpu.SemaphoreType.DMA((N_SEMS,)),
            pltpu.SemaphoreType.DMA((10,)),
        ],
        compiler_params=pltpu.CompilerParams(
            collective_id=0, has_side_effects=True, vmem_limit_bytes=66 * 1024 * 1000
        ),
        name="layer",
    )(
        input_gates, forget_gates, doc_ids.reshape(1, T), head_gain.reshape(1, DV),
        norm_gain.reshape(1, D), queries, keys, values, out_gate, w_out, resid, w_up, w_down,
    )


def solution(mesh):
    split = Mesh(mesh.devices.reshape(4, 4, 2, mesh.shape["tp"]), ("z", "y", "c", "x"))
    sp = ("z", "y", "c")
    return jax.shard_map(
        shards,
        mesh=split,
        in_specs=(
            P(sp, "x"), P(sp, "x"), P(sp, "x"), P(sp, "x"),
            P(None, "x", sp), P(None, "x", sp), P(sp), P("x"), P("x", None),
            P((*sp, "x"), None), P(), P(sp, "x"), P("x", sp),
        ),
        out_specs=P((*sp, "x"), None),
        check_vma=False,
    )
```

```python
import contextlib

import jax
import jax.numpy as jnp
from jax import lax
from jax.experimental import pallas as pl
from jax.experimental.pallas import tpu as pltpu
from jax.sharding import Mesh
from jax.sharding import PartitionSpec as P

MESH = pl.DeviceIdType.MESH
F32 = jnp.float32
BF16 = jnp.bfloat16
EPS = 1e-06
FAR_LOW = -1e30

T = 768
ROWS = 192
HALF = 96
DK = 256
DV = 512
D = 2048
SROWS = 272
SCALE = DK ** (-0.5)
N_SEMS = 112


class Stages:
    def __init__(self):
        self.scopes = contextlib.ExitStack()

    def __call__(self, name=None):
        self.scopes.close()
        if name:
            self.scopes.enter_context(jax.named_scope(name))


class Copies:
    def __init__(self, send, recv, loc):
        self.send, self.recv, self.loc = send, recv, loc
        self.at = 0
        self.at_loc = 0
        self.all = []

    def remote(self, src, dst, dev):
        k = self.at
        self.at += 1
        assert k < N_SEMS
        c = pltpu.make_async_remote_copy(
            src_ref=src,
            dst_ref=dst,
            send_sem=self.send.at[k],
            recv_sem=self.recv.at[k],
            device_id=dev,
            device_id_type=MESH,
        )
        self.all.append(c)
        return c

    def local(self, src, dst):
        k = self.at_loc
        self.at_loc += 1
        return pltpu.make_async_copy(src, dst, self.loc.at[k])


class Ring:
    def __init__(self, cp, plus, minus, own, put_plus, put_minus, near0, near1, far0, far1):
        self.p0 = cp.remote(own(0), put_plus(0), plus)
        self.m0 = cp.remote(own(1), put_minus(1), minus)
        self.p1 = cp.remote(own(1), put_plus(1), plus)
        self.m1 = cp.remote(own(0), put_minus(0), minus)
        self.rp = cp.remote(near0, far0, plus)
        self.rm = cp.remote(near1, far1, minus)

    def start0(self):
        self.p0.start()
        self.m0.start()

    def start1(self):
        self.p1.start()
        self.m1.start()

    def start(self):
        self.start0()
        self.start1()

    def relay(self):
        self.p0.wait_recv()
        self.rp.start()
        self.m0.wait_recv()
        self.rm.start()

    def near(self):
        self.p1.wait_recv()
        self.m1.wait_recv()

    def far(self):
        self.rp.wait_recv()
        self.rm.wait_recv()


def slot_ring(cp, axis, p, slot):
    plus, minus = lax.rem(p + 1, 4), lax.rem(p + 3, 4)
    own = lambda h: slot(p, h)
    return Ring(
        cp, {axis: plus}, {axis: minus}, own, own, own,
        slot(minus, 0), slot(plus, 1), slot(minus, 0), slot(plus, 1),
    )


def roll_lanes(x, shift):
    return pltpu.roll(x, shift % T, 1)


def kernel(
    ig_ref, fg_ref, doc_ref, gain_ref, ngain_ref,
    q_h, k_h, v_h, og_h, wout_h, resid_h, wup_h, wdn_h,
    own_out, rs_in,
    wu, wd, wox, wop, wa, wb, q, k, v, og, resid,
    arow, cols, numf, numb, dens,
    st_own, st_par, sc_pair, q_send, q_recv, sc_recv, cin,
    ro_out, ro_st, ro, mixed, nrm, hid, part, acc2, add_in,
    send_sem, recv_sem, loc_sem,
):
    z, y, c, x = (lax.axis_index(a) for a in ("z", "y", "c", "x"))
    other = 1 - c
    n = z * 4 + y
    n_up, n_dn = lax.rem(n + 1, 16), lax.rem(n + 15, 16)
    chip_up = {"z": lax.div(n_up, 4), "y": lax.rem(n_up, 4)}
    chip_dn = {"z": lax.div(n_dn, 4), "y": lax.rem(n_dn, 4)}
    partner = {"c": other}
    xp, xm, xf = lax.rem(x + 1, 4), lax.rem(x + 3, 4), lax.rem(x + 2, 4)
    cp = Copies(send_sem, recv_sem, loc_sem)
    stage = Stages()
    stage("loads")

    l_wd = cp.local(wdn_h, wa)
    l_wu = cp.local(wup_h, wu.at[z, y, c])
    l_wo = [cp.local(wout_h.at[pl.ds(8 * i, 8)], wox.at[0, i]) for i in range(2)]
    l_k = cp.local(k_h, k)
    l_v = cp.local(v_h, v)
    l_q = cp.local(q_h, q)
    l_og = cp.local(og_h, og)
    l_wp = [
        cp.local(wout_h.at[pl.ds(16, 16), :, pl.ds(1024 * i, 1024)], wop.at[i, 0]) for i in range(2)
    ]
    l_re = cp.local(resid_h, resid)
    for l in (l_wd, l_wu, *l_wo, l_k, l_v, l_q, l_og, *l_wp, l_re):
        l.start()

    stage("barrier")
    barrier = pltpu.get_barrier_semaphore()
    peers = (
        partner, {"y": lax.rem(y + 1, 4)}, {"y": lax.rem(y + 3, 4)}, {"z": lax.rem(z + 1, 4)},
        {"z": lax.rem(z + 3, 4)}, {"x": xp}, {"x": xm}, {"x": xf}, chip_up, chip_dn,
    )
    for dev in peers:
        pl.semaphore_signal(barrier, inc=1, device_id=dev, device_id_type=MESH)
    pl.semaphore_wait(barrier, len(peers))

    stage("first_sends")
    a1 = slot_ring(cp, "y", y, lambda p, h: wu.at[z, p, c, pl.ds(32 * h, 32)])
    a2 = slot_ring(cp, "z", z, lambda p, h: wu.at[p, :, c, pl.ds(32 * h, 32)])
    b1 = slot_ring(cp, "z", z, lambda p, h: wd.at[p, y, c, pl.ds(512 * h, 512)])
    b2 = slot_ring(cp, "y", y, lambda p, h: wd.at[:, p, c, pl.ds(512 * h, 512)])

    wx = lambda j, h: wox.at[j, c, pl.ds(4 * h, 4)]
    wr = Ring(
        cp, {"x": xp}, {"x": xm},
        lambda h: wx(0, h), lambda h: wx(3, h), lambda h: wx(1, h),
        wx(3, 0), wx(1, 1), wx(2, 0), wx(2, 1),
    )
    a_pos, b_pos = jnp.where(c == 0, z, y), jnp.where(c == 0, y, z)
    piece = a_pos * 4 + b_pos
    cols_c = pl.ds(pl.multiple_of(1024 * c, 1024), 1024)
    wp = [
        cp.remote(wout_h.at[16 + piece, :, cols_c], wop.at[c, j, piece], {"x": to})
        for to, j in ((xp, 3), (xm, 1), (xf, 2))
    ]

    def dev_b(step):
        return {
            "z": jnp.where(c == 0, z, lax.rem(z + step, 4)),
            "y": jnp.where(c == 0, lax.rem(y + step, 4), y),
        }

    def dev_a(step):
        return {
            "z": jnp.where(c == 0, lax.rem(z + step, 4), z),
            "y": jnp.where(c == 0, y, lax.rem(y + step, 4)),
        }

    def piece_ring(plus, minus, pos, slot):
        own = lambda h: slot(pos, h)
        up, down = lax.rem(pos + 1, 4), lax.rem(pos + 3, 4)
        return Ring(
            cp, plus, minus, own, own, own,
            slot(down, 0), slot(up, 1), slot(down, 0), slot(up, 1),
        )

    c1 = piece_ring(
        dev_b(1), dev_b(3), b_pos,
        lambda p, h: wop.at[c, pl.ds(1, 3), a_pos * 4 + p, :, pl.ds(512 * h, 512)],
    )
    c2 = piece_ring(
        dev_a(1), dev_a(3), a_pos,
        lambda p, h: wop.at[c, pl.ds(1, 3), pl.ds(4 * p, 4), :, pl.ds(512 * h, 512)],
    )

    for w in wp:
        w.start()
    l_wd.wait()
    d_wd = cp.remote(wa.at[:, pl.ds(pl.multiple_of(1024 * other, 1024), 1024)], wb, partner)
    d_wd.start()
    l_wu.wait()
    a1.start()
    for l in l_wo:
        l.wait()
    wr.start()

    stage("gates")
    def row(ref, i):
        return jnp.broadcast_to(ref[i], (8, T))

    lane = lax.broadcasted_iota(jnp.int32, (8, T), 1)
    rowi = lax.broadcasted_iota(jnp.int32, (8, T), 0)
    doc = jnp.broadcast_to(doc_ref[...].astype(F32)[None, :], (8, T))

    def log_sigmoid(f):
        return jnp.minimum(f, 0.0) - jnp.log1p(jnp.exp(-jnp.abs(f)))

    cumf, cumb = log_sigmoid(row(fg_ref, 0)), log_sigmoid(row(fg_ref, 1))
    sh = 1
    while sh < T:
        cumf = cumf + jnp.where(lane >= sh, roll_lanes(cumf, sh), 0.0)
        cumb = cumb + jnp.where(lane < T - sh, roll_lanes(cumb, T - sh), 0.0)
        sh *= 2
    af, ab = row(ig_ref, 0) - cumf, row(ig_ref, 1) - cumb
    mf, mb = af, ab
    sh = 1
    while sh < T:
        same_f = (lane >= sh) & (roll_lanes(doc, sh) == doc)
        same_b = (lane < T - sh) & (roll_lanes(doc, T - sh) == doc)
        mf = jnp.where(same_f, jnp.maximum(mf, roll_lanes(mf, sh)), mf)
        mb = jnp.where(same_b, jnp.maximum(mb, roll_lanes(mb, T - sh)), mb)
        sh *= 2
    doc0, docl = doc[:, 0:1], doc[:, T - 1 : T]
    mxf, mxb = mf[:, T - 1 : T], mb[:, 0:1]
    totf, totb = cumf[:, T - 1 : T], cumb[:, 0:1]
    wf = jnp.where(doc == docl, jnp.exp(af - mxf), 0.0)
    wbk = jnp.where(doc == doc0, jnp.exp(ab - mxb), 0.0)
    arow[0] = af
    arow[1] = ab
    arow[2] = doc
    stack = jnp.where(
        rowi == 0, mf,
        jnp.where(rowi == 1, mb, jnp.where(rowi == 2, doc, jnp.where(rowi == 3, wf, wbk))),
    )
    cols[...] = stack.T
    r8 = lax.broadcasted_iota(jnp.int32, (8, 128), 0)
    scal = jnp.zeros((8, 128), F32)
    for i, val in enumerate((totf + mxf, totb + mxb, totf, totb, doc0, docl)):
        scal = jnp.where(r8 == i, jnp.broadcast_to(val, (8, 128)), scal)
    sc_pair[c] = scal
    d_sc = cp.remote(sc_pair.at[c], sc_pair.at[c], partner)
    d_sc.start()

    stage("wd_block")
    d_wd.wait_recv()
    ei = lax.broadcasted_iota(jnp.int32, (64, 128), 0)
    ej = lax.broadcasted_iota(jnp.int32, (64, 128), 1)
    put_own = jnp.where(ej == ei + 64 * c, 1.0, 0.0).astype(BF16)
    put_par = jnp.where(ej == ei + 64 * other, 1.0, 0.0).astype(BF16)
    mine = wa[:, pl.ds(pl.multiple_of(1024 * c, 1024), 1024)]
    tn = (((0,), (0,)), ((), ()))
    wd[z, y, c] = (
        lax.dot_general(mine, put_own, tn, preferred_element_type=F32)
        + lax.dot_general(wb[...], put_par, tn, preferred_element_type=F32)
    ).astype(BF16)
    b1.start()

    stage("state")
    l_k.wait()
    l_v.wait()
    keys = k[...].astype(F32)
    d_st = []
    for d in range(2):
        weighted = (keys * cols[:, 3 + d : 4 + d]).astype(BF16)
        st = lax.dot_general(
            v[...], weighted, (((0,), (0,)), ((), ())), preferred_element_type=F32
        ).astype(BF16)
        norm = jnp.sum(weighted.astype(F32), axis=0, keepdims=True)
        tail = jnp.broadcast_to(norm, (16, DK)).astype(BF16)
        for h in range(2):
            st_own[d, h, 0:256, :] = st[256 * h : 256 * h + 256]
            st_own[d, h, 256:SROWS, :] = tail
        d_st.append(cp.remote(st_own.at[d], st_par.at[d], partner))
        d_st[d].start()

    stage("pair_wait")
    def pick(ref, i):
        return ref[i : i + 1, 0:1]

    def pair_terms(s0, s1, d):
        early, late = (s0, s1) if d == 0 else (s1, s0)
        e_last = early[5 - d : 6 - d, 0:1]
        l_first, l_last = late[4 + d : 5 + d, 0:1], late[5 - d : 6 - d, 0:1]
        linked = (l_first == e_last) & (l_first == l_last)
        e_top = early[d : d + 1, 0:1] + late[2 + d : 3 + d, 0:1]
        l_top = late[d : d + 1, 0:1]
        top = jnp.where(linked, jnp.maximum(l_top, e_top), l_top)
        f_early = jnp.where(linked, jnp.exp(jnp.minimum(e_top - top, 0.0)), 0.0)
        f_late = jnp.exp(l_top - top)
        total = early[2 + d : 3 + d, 0:1] + late[2 + d : 3 + d, 0:1]
        return top, total, f_early, f_late, l_last

    d_sc.wait_recv()
    s0, s1 = sc_pair[0], sc_pair[1]
    cq = []
    cs = []
    for d in range(2):
        pos = c if d == 0 else other
        _, _, f_early, f_late, _ = pair_terms(s0, s1, d)
        f_own = jnp.where(pos == 0, f_early, f_late)
        f_par = jnp.where(pos == 0, f_late, f_early)
        d_st[d].wait_recv()
        q_send[d] = (f_own * st_own[d, c].astype(F32) + f_par * st_par[d, c].astype(F32)).astype(BF16)
        to = chip_up if d == 0 else chip_dn
        cs.append(cp.remote(sc_pair, sc_recv.at[d, 0], to))
        cq.append(cp.remote(q_send.at[d], q_recv.at[d, 0, c], to))
        cs[-1].start()
        cq[-1].start()

    stage("intra0")
    l_q.wait()

    def intra(r0, size):
        qb = q[r0 : r0 + size, :]
        mfc, mbc, dc = (cols[r0 : r0 + size, i : i + 1] for i in range(3))
        score = (
            lax.dot_general(qb, k[...], (((1,), (1,)), ((), ())), preferred_element_type=F32)
            * SCALE
        )
        for d in range(2):
            lo, hi = (0, r0 + size) if d == 0 else (r0, T)
            ti = r0 + lax.broadcasted_iota(jnp.int32, (size, hi - lo), 0)
            si = lo + lax.broadcasted_iota(jnp.int32, (size, hi - lo), 1)
            keep = ((si <= ti) if d == 0 else (si >= ti)) & (arow[2, 0:1, lo:hi] == dc)
            e = jnp.exp(jnp.minimum(arow[d, 0:1, lo:hi] - (mfc if d == 0 else mbc), 0.0))
            w = jnp.where(keep, score[:, lo:hi] * e, 0.0)
            dens[r0 : r0 + size, d : d + 1] = jnp.sum(w, axis=1, keepdims=True)
            num = jnp.dot(w.astype(BF16), v[lo:hi, :], preferred_element_type=F32)
            (numf if d == 0 else numb)[r0 : r0 + size, :] = num

    intra(0, 256)
    stage("pieces")
    for w in wp:
        w.wait_recv()
    c1.start()
    b1.relay()
    stage("intra1")
    intra(256, 256)
    stage("wr_relay")
    wr.relay()
    stage("intra2")
    intra(512, 256)

    stage("c1_relay")
    c1.relay()
    stage("carry_near")
    rq, rs, dq = [], [], []
    for d in range(2):
        to = chip_up if d == 0 else chip_dn
        rs.append(cp.remote(sc_recv.at[d, 0], sc_recv.at[d, 1], to))
        rq.append(cp.remote(q_recv.at[d, 0, c], q_recv.at[d, 1, c], to))
        dq.append(cp.remote(q_recv.at[d, 0, c], q_recv.at[d, 0, c], partner))
        cs[d].wait_recv()
        rs[d].start()
        cq[d].wait_recv()
        rq[d].start()
        dq[d].start()
    a1.relay()
    stage("c1_wait")
    c1.near()
    c1.far()
    c2.start()
    stage("b1_wait")
    b1.near()
    b1.far()
    stage("carry_far")
    dq2 = []
    for d in range(2):
        rs[d].wait_recv()
        rq[d].wait_recv()
        dq2.append(cp.remote(q_recv.at[d, 1, c], q_recv.at[d, 1, c], partner))
        dq2[d].start()
    fw = [
        cp.remote(wu.at[z, :, c], wu.at[z, :, c], partner),
        cp.remote(wd.at[:, y, c], wd.at[:, y, c], partner),
    ]

    def second_phase():
        stage("c2_relay")
        c2.relay()
        a1.near()
        a1.far()
        a2.start()
        b2.start()
        for f in fw:
            f.start()
        stage("emit_rest")

    stage("carry_combine")
    scal_in = []
    for d in range(2):
        pos = c if d == 0 else other
        chip = n if d == 0 else 15 - n
        own_s = sc_pair[c]
        par_s = sc_pair[other]
        first = own_s[4 + d : 5 + d, 0:1]
        t1, tot1, _, _, last1 = pair_terms(sc_recv[d, 0, 0], sc_recv[d, 0, 1], d)
        t2, _, _, _, last2 = pair_terms(sc_recv[d, 1, 0], sc_recv[d, 1, 1], d)
        l0 = (par_s[5 - d : 6 - d, 0:1] == first) & (pos == 1)
        l1 = (last1 == first) & (chip >= 1)
        l2 = (last2 == first) & (chip >= 2)
        shift = jnp.where(pos == 1, par_s[2 + d : 3 + d, 0:1], 0.0)
        e0 = jnp.where(l0, par_s[d : d + 1, 0:1], FAR_LOW)
        e1 = jnp.where(l1, t1 + shift, FAR_LOW)
        e2 = jnp.where(l2, t2 + tot1 + shift, FAR_LOW)
        top = jnp.maximum(e0, jnp.maximum(e1, e2))
        g0 = jnp.where(l0, jnp.exp(e0 - top), 0.0)
        g1 = jnp.where(l1, jnp.exp(e1 - top), 0.0)
        g2 = jnp.where(l2, jnp.exp(e2 - top), 0.0)
        late = jnp.where(pos == 1, 1.0, 0.0)
        linked = late * jnp.where(l0, 1.0, 0.0) + (1.0 - late) * jnp.where(l1, 1.0, 0.0)
        dq[d].wait_recv()
        dq2[d].wait_recv()
        for h in range(2):
            cin[d, h] = (
                g0 * st_par[d, h].astype(F32)
                + g1 * q_recv[d, 0, h].astype(F32)
                + g2 * q_recv[d, 1, h].astype(F32)
            ).astype(BF16)
        scal_in.append((top, linked, first))

    stage("emit")
    l_og.wait()
    ca = []
    lo, hi = pl.ds(0, HALF), pl.ds(HALF, HALF)
    for step, to in enumerate((xf, xp, xm, x)):
        r0 = pl.multiple_of(to * ROWS, 64)
        rows = pl.ds(r0, ROWS)
        qb = q[rows, :]
        qw = qb.astype(F32)
        dc = cols[rows, 2:3]
        memory = None
        for d in range(2):
            top, linked, first = scal_in[d]
            m_loc = cols[rows, d : d + 1]
            usable = jnp.where(dc == first, linked, 0.0) > 0.5
            m = jnp.where(usable, jnp.maximum(m_loc, top), m_loc)
            keep = jnp.exp(m_loc - m)
            inter = jnp.where(usable, jnp.exp(jnp.minimum(top - m, 0.0)), 0.0) * SCALE
            nt = (((1,), (1,)), ((), ()))
            qc = jnp.concatenate(
                [
                    lax.dot_general(qb, cin[d, h, 0:256, :], nt, preferred_element_type=F32)
                    for h in range(2)
                ],
                axis=1,
            )
            norm = cin[d, 0, 256:257, :].astype(F32)
            num = keep * (numf if d == 0 else numb)[rows, :] + inter * qc
            den = keep * dens[rows, d : d + 1] + inter * jnp.sum(qw * norm, axis=1, keepdims=True)
            h_dir = num / jnp.maximum(jnp.abs(den), 1.0)
            memory = h_dir if memory is None else memory + h_dir
        normed = memory * lax.rsqrt(jnp.mean(memory * memory, axis=1, keepdims=True) + EPS)
        gate = 1.0 / (1.0 + jnp.exp(-og[rows, :].astype(F32)))
        readout = (normed * gain_ref[...] * gate).astype(BF16)
        if step == 3:
            ro[x] = readout
        else:
            ro_out[step] = readout
        if step == 0:
            ca0 = [
                cp.remote(ro_out.at[0, lo], ro_st.at[0], {"x": xp}),
                cp.remote(ro_out.at[0, hi], ro_st.at[1], {"x": xm}),
            ]
            for cc in ca0:
                cc.start()
            second_phase()
        elif step < 3:
            ca.append(cp.remote(ro_out.at[step], ro.at[x], {"x": to}))
            ca[-1].start()
    stage("a2a_relay")
    ca += [
        cp.remote(ro_st.at[0], ro.at[xm, lo], {"x": xp}),
        cp.remote(ro_st.at[1], ro.at[xp, hi], {"x": xm}),
    ]
    for i in range(2):
        ca0[i].wait_recv()
        ca[2 + i].start()

    stage("wout_fwd")
    wr.near()
    wr.far()
    fo = [cp.remote(wox.at[pl.ds(1, 3), c], wox.at[pl.ds(1, 3), c], partner)]
    fo[0].start()
    c2.near()
    c2.far()
    fo.append(cp.remote(wop.at[c, pl.ds(1, 3)], wop.at[c, pl.ds(1, 3)], partner))
    fo[1].start()
    stage("a2a_wait")
    l_re.wait()
    for l in l_wp:
        l.wait()
    for f in fo:
        f.wait_recv()
    for cc in ca:
        cc.wait_recv()

    stage("wout")
    mixed[...] = resid[...].astype(F32)

    @pl.loop(0, 4)
    def _(t):
        cs_ = pl.ds(pl.multiple_of(t * 512, 512), 512)
        tot = mixed[:, cs_]
        side = pl.ds(pl.multiple_of(lax.rem(t, 2) * 512, 512), 512)
        for j in range(4):
            head = ro.at[lax.rem(x + j, 4)]
            w0 = wox[j, :, :, :, cs_].reshape(256, 512)
            w1 = wop[lax.div(t, 2), j, :, :, side].reshape(256, 512)
            one = jnp.dot(head[:, 0:256], w0, preferred_element_type=F32) + jnp.dot(
                head[:, 256:512], w1, preferred_element_type=F32
            )
            tot = tot + one.astype(BF16).astype(F32)
        mixed[:, cs_] = tot

    mx = mixed[...]
    factor = lax.rsqrt(jnp.mean(mx * mx, axis=1, keepdims=True) + EPS)
    nrm[0] = (mx * factor * ngain_ref[...]).astype(BF16)

    h01 = lambda j, h: nrm.at[j, pl.ds(HALF * h, HALF)]
    ag = Ring(
        cp, {"x": xp}, {"x": xm},
        lambda h: h01(0, h),
        lambda h: h01(1 + h, 0),
        lambda h: h01(2 - h, 1),
        h01(1, 0), h01(1, 1), h01(3, 0), h01(3, 1),
    )
    ag.start()
    stage("a2_relay")
    a2.relay()
    stage("b2_relay")
    b2.relay()
    stage("ag_relay")
    ag.relay()

    stage("a2b2_near")
    def forward(refs):
        for r in refs:
            fw.append(cp.remote(r, r, partner))
            fw[-1].start()

    zp, zm, zf = lax.rem(z + 1, 4), lax.rem(z + 3, 4), lax.rem(z + 2, 4)
    yp, ym, yf = lax.rem(y + 1, 4), lax.rem(y + 3, 4), lax.rem(y + 2, 4)
    a2.near()
    forward([wu.at[zp, :, c], wu.at[zm, :, c]])
    b2.near()
    forward([wd.at[:, yp, c], wd.at[:, ym, c]])
    stage("a2_far")
    a2.far()
    forward([wu.at[zf, :, c]])
    for i in (0, 2, 3, 6):
        fw[i].wait_recv()

    def up(j):
        rows = nrm[j]

        @pl.loop(0, 4)
        def _(t):
            cs_ = pl.ds(pl.multiple_of(t * 512, 512), 512)
            w = wu[:, :, :, :, cs_].reshape(D, 512)
            pre = jnp.maximum(jnp.dot(rows, w, preferred_element_type=F32), 0.0)
            hid[j, :, cs_] = (pre * pre).astype(BF16)

    def down(j, first, last, sink):
        @pl.loop(first, last)
        def _(t):
            cs_ = pl.ds(pl.multiple_of(t * 512, 512), 512)
            w = jnp.concatenate([wd[t, i].reshape(D, 128) for i in range(4)], axis=1)
            sink(cs_, jnp.dot(hid[j], w, preferred_element_type=F32))

    def add_own(cs_, val):
        mixed[:, cs_] += val

    def to_part(j):
        def sink(cs_, val):
            part[j, :, cs_] = val.astype(BF16)

        return sink

    def to_acc(cs_, val):
        acc2[:, cs_] = val

    stage("up1")
    up(1)
    stage("up0")
    up(0)
    stage("b2_far")
    b2.far()
    forward([wd.at[:, yf, c]])
    for i in (1, 4, 5, 7):
        fw[i].wait_recv()
    stage("down1")
    down(1, 0, 4, to_part(0))
    rs1 = [
        cp.remote(part.at[0, hi], rs_in.at[0, hi], {"x": xp}),
        cp.remote(part.at[0, lo], rs_in.at[1, lo], {"x": xm}),
    ]
    for r in rs1:
        r.start()
    stage("down0")
    down(0, 0, 4, add_own)
    l_mx = cp.local(mixed, own_out)
    l_mx.start()
    stage("ag_far")
    ag.far()
    stage("up3")
    up(3)
    stage("down3")
    rs2, rs3 = [], []
    for i in range(2):
        down(3, 2 * i, 2 * i + 2, to_part(1))
        wide = pl.ds(1024 * i, 1024)
        rs2.append(cp.remote(part.at[1, lo, wide], add_in.at[0, :, wide], {"x": xp}))
        rs2.append(cp.remote(part.at[1, hi, wide], add_in.at[1, :, wide], {"x": xm}))
        rs3.append(cp.remote(part.at[2, hi, wide], rs_in.at[0, lo, wide], {"x": xp}))
        rs3.append(cp.remote(part.at[2, lo, wide], rs_in.at[1, hi, wide], {"x": xm}))
        rs2[-2].start()
        rs2[-1].start()
    stage("ff2")
    ag.near()
    up(2)
    down(2, 0, 4, to_acc)
    for i in range(2):
        stage(f"rs_add{i}")
        lanes = slice(1024 * i, 1024 * i + 1024)
        for side in range(2):
            rs2[2 * i + side].wait_recv()
            rows = slice(HALF, ROWS) if side == 0 else slice(0, HALF)
            part[2, rows, lanes] = (
                acc2[rows, lanes] + add_in[side, :, lanes].astype(F32)
            ).astype(BF16)
            rs3[2 * i + side].start()
    stage("rs_wait")
    for r in (*rs1, *rs3):
        r.wait_recv()
    l_mx.wait()
    stage("drain")
    for r in cp.all:
        r.wait_send()
    stage()


def shards(
    queries, keys, values, out_gate, input_gates, forget_gates, doc_ids,
    head_gain, w_out, resid, norm_gain, w_up, w_down,
):
    vmem = pl.BlockSpec(memory_space=pltpu.VMEM)
    hbm = pl.BlockSpec(memory_space=pl.ANY)
    own, sums = pl.pallas_call(
        kernel,
        out_shape=(
            jax.ShapeDtypeStruct((ROWS, D), F32),
            jax.ShapeDtypeStruct((2, ROWS, D), BF16),
        ),
        in_specs=[vmem] * 5 + [hbm] * 8,
        out_specs=(hbm, hbm),
        scratch_shapes=[
            pltpu.VMEM((4, 4, 2, 64, D), BF16),
            pltpu.VMEM((4, 4, 2, 1024, 128), BF16),
            pltpu.VMEM((4, 2, 8, 16, D), BF16),
            pltpu.VMEM((2, 4, 16, 16, 1024), BF16),
            pltpu.VMEM((64, D), BF16),
            pltpu.VMEM((64, 1024), BF16),
            pltpu.VMEM((T, DK), BF16),
            pltpu.VMEM((T, DK), BF16),
            pltpu.VMEM((T, DV), BF16),
            pltpu.VMEM((T, DV), BF16),
            pltpu.VMEM((ROWS, D), BF16),
            pltpu.VMEM((3, 8, T), F32),
            pltpu.VMEM((T, 8), F32),
            pltpu.VMEM((T, DV), F32),
            pltpu.VMEM((T, DV), F32),
            pltpu.VMEM((T, 8), F32),
            pltpu.VMEM((2, 2, SROWS, DK), BF16),
            pltpu.VMEM((2, 2, SROWS, DK), BF16),
            pltpu.VMEM((2, 8, 128), F32),
            pltpu.VMEM((2, SROWS, DK), BF16),
            pltpu.VMEM((2, 2, 2, SROWS, DK), BF16),
            pltpu.VMEM((2, 2, 2, 8, 128), F32),
            pltpu.VMEM((2, 2, SROWS, DK), BF16),
            pltpu.VMEM((3, ROWS, DV), BF16),
            pltpu.VMEM((2, HALF, DV), BF16),
            pltpu.VMEM((4, ROWS, DV), BF16),
            pltpu.VMEM((ROWS, D), F32),
            pltpu.VMEM((4, ROWS, D), BF16),
            pltpu.VMEM((4, ROWS, D), BF16),
            pltpu.VMEM((3, ROWS, D), BF16),
            pltpu.VMEM((ROWS, D), F32),
            pltpu.VMEM((2, HALF, D), BF16),
            pltpu.SemaphoreType.DMA((N_SEMS,)),
            pltpu.SemaphoreType.DMA((N_SEMS,)),
            pltpu.SemaphoreType.DMA((13,)),
        ],
        compiler_params=pltpu.CompilerParams(
            collective_id=0, has_side_effects=True, vmem_limit_bytes=66 * 1024 * 1000
        ),
        name="layer",
    )(
        input_gates, forget_gates, doc_ids, head_gain.reshape(1, DV),
        norm_gain.reshape(1, D), queries, keys, values, out_gate, w_out.reshape(32, 16, D), resid, w_up,
        w_down.T,
    )
    return (own + sums[0].astype(F32) + sums[1].astype(F32)).astype(BF16)


def solution(mesh):
    split = Mesh(mesh.devices.reshape(4, 4, 2, mesh.shape["tp"]), ("z", "y", "c", "x"))
    sp = ("z", "y", "c")
    return jax.shard_map(
        shards,
        mesh=split,
        in_specs=(
            P(sp, "x"), P(sp, "x"), P(sp, "x"), P(sp, "x"),
            P(None, "x", sp), P(None, "x", sp), P(sp), P("x"), P("x", None),
            P((*sp, "x"), None), P(), P(sp, "x"), P("x", sp),
        ),
        out_specs=P((*sp, "x"), None),
        check_vma=False,
    )
```

```python
import contextlib

import jax
import jax.numpy as jnp
from jax import lax
from jax.experimental import pallas as pl
from jax.experimental.pallas import tpu as pltpu
from jax.sharding import Mesh
from jax.sharding import PartitionSpec as P

MESH = pl.DeviceIdType.MESH
F32 = jnp.float32
BF16 = jnp.bfloat16
EPS = 1e-06
FAR_LOW = -1e30

T = 768
ROWS = 192
HALF = 96
DK = 256
DV = 512
D = 2048
SROWS = 272
SCALE = DK ** (-0.5)
N_SEMS = (37, 62, 14)


class Stages:
    def __init__(self):
        self.scopes = contextlib.ExitStack()

    def __call__(self, name=None):
        self.scopes.close()
        if name:
            self.scopes.enter_context(jax.named_scope(name))


class Copies:
    def __init__(self, send, recv, loc):
        self.send, self.recv, self.loc = send, recv, loc
        self.sends = self.recvs = self.locals = 0
        self.drain = []

    def new_send(self):
        self.sends += 1
        return self.send.at[self.sends - 1]

    def new_recv(self):
        self.recvs += 1
        return self.recv.at[self.recvs - 1]

    def remote(self, src, dst, dev, send=None, recv=None):
        alone = send is None
        c = pltpu.make_async_remote_copy(
            src_ref=src,
            dst_ref=dst,
            send_sem=self.new_send() if alone else send,
            recv_sem=self.new_recv() if recv is None else recv,
            device_id=dev,
            device_id_type=MESH,
        )
        if alone:
            self.drain.append(c)
        return c

    def waiter(self, ref, send, recv):
        return pltpu.make_async_remote_copy(
            src_ref=ref,
            dst_ref=ref,
            send_sem=send,
            recv_sem=recv,
            device_id={"c": 1 - lax.axis_index("c")},
            device_id_type=MESH,
        )

    def drain_later(self, ref, send, recv):
        self.drain.append(self.waiter(ref, send, recv))

    def local(self, src, dst):
        self.locals += 1
        return pltpu.make_async_copy(src, dst, self.loc.at[self.locals - 1])


class Ring:
    def __init__(
        self, cp, plus, minus, own, put_plus, put_minus, near0, near1, far0, far1, block, three
    ):
        send = cp.new_send()
        self.first, self.second, self.third = (cp.new_recv() for _ in range(3))

        def group(srcs, dsts, dev, recv):
            return [cp.remote(s, d, dev, send, recv) for s, d in zip(srcs, dsts, strict=True)]

        self.out0 = group(own(0), put_plus(0), plus, self.first)
        self.out0 += group(own(1), put_minus(1), minus, self.first)
        self.out1 = group(own(1), put_plus(1), plus, self.second)
        self.out1 += group(own(0), put_minus(0), minus, self.second)
        self.on = group(near0, far0, plus, self.third) + group(near1, far1, minus, self.third)
        self.waits = [cp.waiter(block, send, r) for r in (self.first, self.second, self.third)]
        cp.drain_later(three, send, self.first)

    def start0(self):
        for c in self.out0:
            c.start()

    def start1(self):
        for c in self.out1:
            c.start()

    def start(self):
        self.start0()
        self.start1()

    def relay(self):
        self.waits[0].wait_recv()
        for c in self.on:
            c.start()

    def near(self):
        self.waits[1].wait_recv()

    def far(self):
        self.waits[2].wait_recv()


def slot_ring(cp, plus, minus, p, slots, block, three):
    up, down = lax.rem(p + 1, 4), lax.rem(p + 3, 4)
    at = lambda pos, h: [f(pos, h) for f in slots]
    own = lambda h: at(p, h)
    return Ring(
        cp, plus, minus, own, own, own, at(down, 0), at(up, 1), at(down, 0), at(up, 1), block, three
    )


def roll_lanes(x, shift):
    return pltpu.roll(x, shift % T, 1)


def kernel(
    ig_ref, fg_ref, doc_ref, gain_ref, ngain_ref,
    q_h, k_h, v_h, og_h, wout_h, resid_h, wup_h, wdn_h,
    own_out, rs_in,
    wu, wd, wox, wop, wa, wb, q, k, v, og, resid,
    arow, cols, numf, numb, dens,
    st_own, st_par, sc_pair, q_send, q_recv, sc_recv, cin,
    ro_out, ro_st, ro, mixed, nrm, hid, part, acc2, add_in,
    send_sem, recv_sem, loc_sem,
):
    z, y, c, x = (lax.axis_index(a) for a in ("z", "y", "c", "x"))
    other = 1 - c
    n = z * 4 + y
    n_up, n_dn = lax.rem(n + 1, 16), lax.rem(n + 15, 16)
    chip_up = {"z": lax.div(n_up, 4), "y": lax.rem(n_up, 4)}
    chip_dn = {"z": lax.div(n_dn, 4), "y": lax.rem(n_dn, 4)}
    partner = {"c": other}
    xp, xm, xf = lax.rem(x + 1, 4), lax.rem(x + 3, 4), lax.rem(x + 2, 4)
    cp = Copies(send_sem, recv_sem, loc_sem)
    stage = Stages()
    stage("loads")

    l_wd = cp.local(wdn_h, wa)
    l_wu = cp.local(wup_h, wu.at[z, y, c])
    l_wo = [cp.local(wout_h.at[pl.ds(12 * i, 12)], wox.at[0, i]) for i in range(2)]
    l_k = cp.local(k_h, k)
    l_v = cp.local(v_h, v)
    l_q = cp.local(q_h, q)
    l_og = cp.local(og_h, og)
    l_wp = [
        cp.local(wout_h.at[pl.ds(24, 8), :, pl.ds(512 * i, 512)], wop.at[i // 2, 0, :, i % 2])
        for i in range(4)
    ]
    l_re = cp.local(resid_h, resid)
    for l in (l_wd, l_wu, *l_wo, l_k, l_v, l_q, l_og, *l_wp, l_re):
        l.start()

    stage("barrier")
    barrier = pltpu.get_barrier_semaphore()
    peers = (
        partner, {"y": lax.rem(y + 1, 4)}, {"y": lax.rem(y + 3, 4)}, {"z": lax.rem(z + 1, 4)},
        {"z": lax.rem(z + 3, 4)}, {"x": xp}, {"x": xm}, {"x": xf}, chip_up, chip_dn,
    )
    for dev in peers:
        pl.semaphore_signal(barrier, inc=1, device_id=dev, device_id_type=MESH)
    pl.semaphore_wait(barrier, len(peers))

    stage("first_sends")
    zp, zm, zf = lax.rem(z + 1, 4), lax.rem(z + 3, 4), lax.rem(z + 2, 4)
    yp, ym, yf = lax.rem(y + 1, 4), lax.rem(y + 3, 4), lax.rem(y + 2, 4)
    over_y, over_z = ({"y": yp}, {"y": ym}), ({"z": zp}, {"z": zm})
    up_half = lambda a, b, h: wu.at[a, b, c, pl.ds(32 * h, 32)]
    dn_half = lambda a, b, h: wd.at[a, b, c, pl.ds(512 * h, 512)]
    three = pl.ds(0, 3)
    a1 = slot_ring(
        cp, *over_y, y, [lambda p, h: up_half(z, p, h)], wu.at[z, y, c], wu.at[z, three, c]
    )
    a2o = slot_ring(
        cp, *over_z, z, [lambda p, h: up_half(p, y, h)], wu.at[z, y, c], wu.at[z, three, c]
    )
    a2 = slot_ring(
        cp, *over_z, z, [lambda p, h, o=o: up_half(p, o, h) for o in (yp, ym, yf)],
        wu.at[z, three, c], wu.at[three, three, c],
    )
    b1 = slot_ring(
        cp, *over_z, z, [lambda p, h: dn_half(p, y, h)], wd.at[z, y, c], wd.at[z, three, c]
    )
    b2o = slot_ring(
        cp, *over_y, y, [lambda p, h: dn_half(z, p, h)], wd.at[z, y, c], wd.at[z, three, c]
    )
    b2 = slot_ring(
        cp, *over_y, y, [lambda p, h, o=o: dn_half(o, p, h) for o in (zp, zm, zf)],
        wd.at[z, three, c], wd.at[three, three, c],
    )

    wx = lambda j, h: wox.at[j, c, pl.ds(6 * h, 6)]
    wr = Ring(
        cp, {"x": xp}, {"x": xm},
        lambda h: [wx(0, h)], lambda h: [wx(3, h)], lambda h: [wx(1, h)],
        [wx(3, 0)], [wx(1, 1)], [wx(2, 0)], [wx(2, 1)], wox.at[0, c], wox.at[three, c],
    )
    a_pos, b_pos = jnp.where(c == 0, z, y), jnp.where(c == 0, y, z)
    piece = lambda a, b: (2 * a + lax.div(b, 2), lax.rem(b, 2))
    p_row, p_col = piece(a_pos, b_pos)
    cols_c = pl.ds(pl.multiple_of(1024 * c + 512 * p_col, 512), 512)
    wp_send, wp_recv = cp.new_send(), cp.new_recv()
    wp = [
        cp.remote(
            wout_h.at[24 + p_row, :, cols_c], wop.at[c, j, p_row, p_col], {"x": to}, wp_send, wp_recv
        )
        for to, j in ((xp, 3), (xm, 1), (xf, 2))
    ]
    wp_all = cp.waiter(wop.at[c, three, 0, 0], wp_send, wp_recv)
    cp.drain.append(wp_all)

    def dev_b(step):
        return {
            "z": jnp.where(c == 0, z, lax.rem(z + step, 4)),
            "y": jnp.where(c == 0, lax.rem(y + step, 4), y),
        }

    def dev_a(step):
        return {
            "z": jnp.where(c == 0, lax.rem(z + step, 4), z),
            "y": jnp.where(c == 0, y, lax.rem(y + step, 4)),
        }

    heads = pl.ds(1, 3)
    c1 = slot_ring(
        cp, dev_b(1), dev_b(3), b_pos,
        [lambda p, h: wop.at[(c, heads, *piece(a_pos, p), slice(None), pl.ds(256 * h, 256))]],
        wop.at[c, heads, 0, 0], wop.at[c, heads, three, 0],
    )
    c2 = slot_ring(
        cp, dev_a(1), dev_a(3), a_pos,
        [lambda p, h: wop.at[c, heads, pl.ds(2 * p, 2), :, :, pl.ds(256 * h, 256)]],
        wop.at[c, heads, pl.ds(0, 2)], wop.at[c, heads, pl.ds(0, 6)],
    )

    for w in wp:
        w.start()
    l_wd.wait()
    d_wd = cp.remote(wa.at[:, pl.ds(pl.multiple_of(1024 * other, 1024), 1024)], wb, partner)
    d_wd.start()
    l_wu.wait()
    a1.start()
    for l in l_wo:
        l.wait()
    wr.start()

    stage("gates")
    def row(ref, i):
        return jnp.broadcast_to(ref[i], (8, T))

    lane = lax.broadcasted_iota(jnp.int32, (8, T), 1)
    rowi = lax.broadcasted_iota(jnp.int32, (8, T), 0)
    doc = jnp.broadcast_to(doc_ref[...].astype(F32)[None, :], (8, T))

    def log_sigmoid(f):
        return jnp.minimum(f, 0.0) - jnp.log1p(jnp.exp(-jnp.abs(f)))

    cumf, cumb = log_sigmoid(row(fg_ref, 0)), log_sigmoid(row(fg_ref, 1))
    sh = 1
    while sh < T:
        cumf = cumf + jnp.where(lane >= sh, roll_lanes(cumf, sh), 0.0)
        cumb = cumb + jnp.where(lane < T - sh, roll_lanes(cumb, T - sh), 0.0)
        sh *= 2
    af, ab = row(ig_ref, 0) - cumf, row(ig_ref, 1) - cumb
    mf, mb = af, ab
    sh = 1
    while sh < T:
        same_f = (lane >= sh) & (roll_lanes(doc, sh) == doc)
        same_b = (lane < T - sh) & (roll_lanes(doc, T - sh) == doc)
        mf = jnp.where(same_f, jnp.maximum(mf, roll_lanes(mf, sh)), mf)
        mb = jnp.where(same_b, jnp.maximum(mb, roll_lanes(mb, T - sh)), mb)
        sh *= 2
    doc0, docl = doc[:, 0:1], doc[:, T - 1 : T]
    mxf, mxb = mf[:, T - 1 : T], mb[:, 0:1]
    totf, totb = cumf[:, T - 1 : T], cumb[:, 0:1]
    wf = jnp.where(doc == docl, jnp.exp(af - mxf), 0.0)
    wbk = jnp.where(doc == doc0, jnp.exp(ab - mxb), 0.0)
    arow[0] = af
    arow[1] = ab
    arow[2] = doc
    stack = jnp.where(
        rowi == 0, mf,
        jnp.where(rowi == 1, mb, jnp.where(rowi == 2, doc, jnp.where(rowi == 3, wf, wbk))),
    )
    cols[...] = stack.T
    r8 = lax.broadcasted_iota(jnp.int32, (8, 128), 0)
    scal = jnp.zeros((8, 128), F32)
    for i, val in enumerate((totf + mxf, totb + mxb, totf, totb, doc0, docl)):
        scal = jnp.where(r8 == i, jnp.broadcast_to(val, (8, 128)), scal)
    sc_pair[c] = scal
    d_sc = cp.remote(sc_pair.at[c], sc_pair.at[c], partner)
    d_sc.start()

    stage("wd_block")
    d_wd.wait_recv()
    ei = lax.broadcasted_iota(jnp.int32, (64, 128), 0)
    ej = lax.broadcasted_iota(jnp.int32, (64, 128), 1)
    put_own = jnp.where(ej == ei + 64 * c, 1.0, 0.0).astype(BF16)
    put_par = jnp.where(ej == ei + 64 * other, 1.0, 0.0).astype(BF16)
    mine = wa[:, pl.ds(pl.multiple_of(1024 * c, 1024), 1024)]
    tn = (((0,), (0,)), ((), ()))
    wd[z, y, c] = (
        lax.dot_general(mine, put_own, tn, preferred_element_type=F32)
        + lax.dot_general(wb[...], put_par, tn, preferred_element_type=F32)
    ).astype(BF16)
    b1.start()

    stage("state")
    l_k.wait()
    l_v.wait()
    keys = k[...].astype(F32)
    d_st = []
    for d in range(2):
        weighted = (keys * cols[:, 3 + d : 4 + d]).astype(BF16)
        st = lax.dot_general(
            v[...], weighted, (((0,), (0,)), ((), ())), preferred_element_type=F32
        ).astype(BF16)
        norm = jnp.sum(weighted.astype(F32), axis=0, keepdims=True)
        tail = jnp.broadcast_to(norm, (16, DK)).astype(BF16)
        for h in range(2):
            st_own[d, h, 0:256, :] = st[256 * h : 256 * h + 256]
            st_own[d, h, 256:SROWS, :] = tail
        d_st.append(cp.remote(st_own.at[d], st_par.at[d], partner))
        d_st[d].start()

    stage("pair_wait")
    def pick(ref, i):
        return ref[i : i + 1, 0:1]

    def pair_terms(s0, s1, d):
        early, late = (s0, s1) if d == 0 else (s1, s0)
        e_last = early[5 - d : 6 - d, 0:1]
        l_first, l_last = late[4 + d : 5 + d, 0:1], late[5 - d : 6 - d, 0:1]
        linked = (l_first == e_last) & (l_first == l_last)
        e_top = early[d : d + 1, 0:1] + late[2 + d : 3 + d, 0:1]
        l_top = late[d : d + 1, 0:1]
        top = jnp.where(linked, jnp.maximum(l_top, e_top), l_top)
        f_early = jnp.where(linked, jnp.exp(jnp.minimum(e_top - top, 0.0)), 0.0)
        f_late = jnp.exp(l_top - top)
        total = early[2 + d : 3 + d, 0:1] + late[2 + d : 3 + d, 0:1]
        return top, total, f_early, f_late, l_last

    d_sc.wait_recv()
    s0, s1 = sc_pair[0], sc_pair[1]
    cq = []
    cs = []
    for d in range(2):
        pos = c if d == 0 else other
        _, _, f_early, f_late, _ = pair_terms(s0, s1, d)
        f_own = jnp.where(pos == 0, f_early, f_late)
        f_par = jnp.where(pos == 0, f_late, f_early)
        d_st[d].wait_recv()
        q_send[d] = (f_own * st_own[d, c].astype(F32) + f_par * st_par[d, c].astype(F32)).astype(BF16)
        to = chip_up if d == 0 else chip_dn
        cs.append(cp.remote(sc_pair, sc_recv.at[d, 0], to))
        cq.append(cp.remote(q_send.at[d], q_recv.at[d, 0, c], to))
        cs[-1].start()
        cq[-1].start()

    stage("intra0")
    l_q.wait()

    def intra(r0, size):
        qb = q[r0 : r0 + size, :]
        mfc, mbc, dc = (cols[r0 : r0 + size, i : i + 1] for i in range(3))
        score = (
            lax.dot_general(qb, k[...], (((1,), (1,)), ((), ())), preferred_element_type=F32)
            * SCALE
        )
        for d in range(2):
            lo, hi = (0, r0 + size) if d == 0 else (r0, T)
            ti = r0 + lax.broadcasted_iota(jnp.int32, (size, hi - lo), 0)
            si = lo + lax.broadcasted_iota(jnp.int32, (size, hi - lo), 1)
            keep = ((si <= ti) if d == 0 else (si >= ti)) & (arow[2, 0:1, lo:hi] == dc)
            e = jnp.exp(jnp.minimum(arow[d, 0:1, lo:hi] - (mfc if d == 0 else mbc), 0.0))
            w = jnp.where(keep, score[:, lo:hi] * e, 0.0)
            dens[r0 : r0 + size, d : d + 1] = jnp.sum(w, axis=1, keepdims=True)
            num = jnp.dot(w.astype(BF16), v[lo:hi, :], preferred_element_type=F32)
            (numf if d == 0 else numb)[r0 : r0 + size, :] = num

    intra(0, 256)
    stage("pieces")
    wp_all.wait_recv()
    c1.start()
    b1.relay()
    b2o.start0()
    stage("intra1")
    intra(256, 256)
    stage("intra2")
    intra(512, 256)
    stage("c1_relay")
    c1.relay()
    a2o.start0()
    stage("carry_near")
    rq, rs, dq = [], [], []
    for d in range(2):
        to = chip_up if d == 0 else chip_dn
        rs.append(cp.remote(sc_recv.at[d, 0], sc_recv.at[d, 1], to))
        rq.append(cp.remote(q_recv.at[d, 0, c], q_recv.at[d, 1, c], to))
        dq.append(cp.remote(q_recv.at[d, 0, c], q_recv.at[d, 0, c], partner))
        cs[d].wait_recv()
        rs[d].start()
        cq[d].wait_recv()
        rq[d].start()
        dq[d].start()
    b2o.start1()
    a2o.start1()
    stage("wr_relay")
    wr.relay()
    stage("c1_wait")
    c1.near()
    c1.far()
    c2.start()
    a1.relay()
    b1.near()
    b1.far()
    stage("carry_far")
    dq2 = []
    for d in range(2):
        rs[d].wait_recv()
        rq[d].wait_recv()
        dq2.append(cp.remote(q_recv.at[d, 1, c], q_recv.at[d, 1, c], partner))
        dq2[d].start()
    fw_send, fw_up, fw_dn = cp.new_send(), cp.new_recv(), cp.new_recv()
    fw = [
        cp.remote(wu.at[z, :, c], wu.at[z, :, c], partner, fw_send, fw_up),
        cp.remote(wd.at[:, y, c], wd.at[:, y, c], partner, fw_send, fw_dn),
    ]

    def second_phase():
        stage("c2_relay")
        c2.relay()
        a2o.relay()
        b2o.relay()
        b2.start()
        stage("emit_rest")

    stage("carry_combine")
    scal_in = []
    for d in range(2):
        pos = c if d == 0 else other
        chip = n if d == 0 else 15 - n
        own_s = sc_pair[c]
        par_s = sc_pair[other]
        first = own_s[4 + d : 5 + d, 0:1]
        t1, tot1, _, _, last1 = pair_terms(sc_recv[d, 0, 0], sc_recv[d, 0, 1], d)
        t2, _, _, _, last2 = pair_terms(sc_recv[d, 1, 0], sc_recv[d, 1, 1], d)
        l0 = (par_s[5 - d : 6 - d, 0:1] == first) & (pos == 1)
        l1 = (last1 == first) & (chip >= 1)
        l2 = (last2 == first) & (chip >= 2)
        shift = jnp.where(pos == 1, par_s[2 + d : 3 + d, 0:1], 0.0)
        e0 = jnp.where(l0, par_s[d : d + 1, 0:1], FAR_LOW)
        e1 = jnp.where(l1, t1 + shift, FAR_LOW)
        e2 = jnp.where(l2, t2 + tot1 + shift, FAR_LOW)
        top = jnp.maximum(e0, jnp.maximum(e1, e2))
        g0 = jnp.where(l0, jnp.exp(e0 - top), 0.0)
        g1 = jnp.where(l1, jnp.exp(e1 - top), 0.0)
        g2 = jnp.where(l2, jnp.exp(e2 - top), 0.0)
        late = jnp.where(pos == 1, 1.0, 0.0)
        linked = late * jnp.where(l0, 1.0, 0.0) + (1.0 - late) * jnp.where(l1, 1.0, 0.0)
        dq[d].wait_recv()
        dq2[d].wait_recv()
        for h in range(2):
            cin[d, h] = (
                g0 * st_par[d, h].astype(F32)
                + g1 * q_recv[d, 0, h].astype(F32)
                + g2 * q_recv[d, 1, h].astype(F32)
            ).astype(BF16)
        scal_in.append((top, linked, first))

    stage("emit")
    l_og.wait()
    ca = []
    lo, hi = pl.ds(0, HALF), pl.ds(HALF, HALF)
    for step, to in enumerate((xf, xp, xm, x)):
        r0 = pl.multiple_of(to * ROWS, 64)
        rows = pl.ds(r0, ROWS)
        qb = q[rows, :]
        qw = qb.astype(F32)
        dc = cols[rows, 2:3]
        memory = None
        for d in range(2):
            top, linked, first = scal_in[d]
            m_loc = cols[rows, d : d + 1]
            usable = jnp.where(dc == first, linked, 0.0) > 0.5
            m = jnp.where(usable, jnp.maximum(m_loc, top), m_loc)
            keep = jnp.exp(m_loc - m)
            inter = jnp.where(usable, jnp.exp(jnp.minimum(top - m, 0.0)), 0.0) * SCALE
            nt = (((1,), (1,)), ((), ()))
            qc = jnp.concatenate(
                [
                    lax.dot_general(qb, cin[d, h, 0:256, :], nt, preferred_element_type=F32)
                    for h in range(2)
                ],
                axis=1,
            )
            norm = cin[d, 0, 256:257, :].astype(F32)
            num = keep * (numf if d == 0 else numb)[rows, :] + inter * qc
            den = keep * dens[rows, d : d + 1] + inter * jnp.sum(qw * norm, axis=1, keepdims=True)
            h_dir = num / jnp.maximum(jnp.abs(den), 1.0)
            memory = h_dir if memory is None else memory + h_dir
        normed = memory * lax.rsqrt(jnp.mean(memory * memory, axis=1, keepdims=True) + EPS)
        gate = 1.0 / (1.0 + jnp.exp(-og[rows, :].astype(F32)))
        readout = (normed * gain_ref[...] * gate).astype(BF16)
        if step == 3:
            ro[x] = readout
        else:
            ro_out[step] = readout
        if step == 0:
            ca0 = [
                cp.remote(ro_out.at[0, lo], ro_st.at[0], {"x": xp}),
                cp.remote(ro_out.at[0, hi], ro_st.at[1], {"x": xm}),
            ]
            for cc in ca0:
                cc.start()
        elif step < 3:
            ca.append(cp.remote(ro_out.at[step], ro.at[x], {"x": to}))
            ca[-1].start()
            if step == 1:
                second_phase()
    stage("a1_wait")
    a1.near()
    a1.far()
    a2.start()
    stage("a2a_relay")
    ca += [
        cp.remote(ro_st.at[0], ro.at[xm, lo], {"x": xp}),
        cp.remote(ro_st.at[1], ro.at[xp, hi], {"x": xm}),
    ]
    for i in range(2):
        ca0[i].wait_recv()
        ca[2 + i].start()

    stage("wout_fwd")
    wr.near()
    wr.far()
    fo = [cp.remote(wox.at[pl.ds(1, 3), c], wox.at[pl.ds(1, 3), c], partner)]
    fo[0].start()
    c2.near()
    c2.far()
    fo.append(cp.remote(wop.at[c, pl.ds(1, 3)], wop.at[c, pl.ds(1, 3)], partner))
    fo[1].start()
    for f in fw:
        f.start()
    stage("a2a_wait")
    l_re.wait()
    for l in l_wp:
        l.wait()
    for f in fo:
        f.wait_recv()
    for cc in ca:
        cc.wait_recv()

    stage("wout")
    mixed[...] = resid[...].astype(F32)

    @pl.loop(0, 4)
    def _(t):
        cs_ = pl.ds(pl.multiple_of(t * 512, 512), 512)
        tot = mixed[:, cs_]
        for j in range(4):
            head = ro.at[lax.rem(x + j, 4)]
            w0 = wox[j, :, :, :, cs_].reshape(384, 512)
            w1 = wop[lax.div(t, 2), j, :, lax.rem(t, 2)].reshape(128, 512)
            one = jnp.dot(head[:, 0:384], w0, preferred_element_type=F32) + jnp.dot(
                head[:, 384:512], w1, preferred_element_type=F32
            )
            tot = tot + one.astype(BF16).astype(F32)
        mixed[:, cs_] = tot

    mx = mixed[...]
    factor = lax.rsqrt(jnp.mean(mx * mx, axis=1, keepdims=True) + EPS)
    nrm[0] = (mx * factor * ngain_ref[...]).astype(BF16)

    h01 = lambda j, h: nrm.at[j, pl.ds(HALF * h, HALF)]
    ag = Ring(
        cp, {"x": xp}, {"x": xm},
        lambda h: [h01(0, h)],
        lambda h: [h01(1 + h, 0)],
        lambda h: [h01(2 - h, 1)],
        [h01(1, 0)], [h01(1, 1)], [h01(3, 0)], [h01(3, 1)], nrm.at[0], nrm.at[three],
    )
    ag.start()
    stage("a2_relay")
    a2.relay()
    stage("b2_relay")
    b2.relay()
    stage("a2b2_near")
    def forward(refs, recv):
        for r in refs:
            cp.remote(r, r, partner, fw_send, recv).start()

    up_all = cp.waiter(wu.at[:, :, 0], fw_send, fw_up)
    dn_all = cp.waiter(wd.at[:, :, 0], fw_send, fw_dn)
    cp.drain_later(wu, fw_send, fw_up)
    a2o.near()
    a2.near()
    forward([wu.at[zp, :, c], wu.at[zm, :, c]], fw_up)
    stage("b2_near")
    b2o.near()
    b2.near()
    forward([wd.at[:, yp, c], wd.at[:, ym, c]], fw_dn)
    stage("ag_relay")
    ag.relay()
    stage("a2_far")
    a2o.far()
    a2.far()
    forward([wu.at[zf, :, c]], fw_up)
    up_all.wait_recv()

    def up(j):
        rows = nrm[j]

        @pl.loop(0, 4)
        def _(t):
            cs_ = pl.ds(pl.multiple_of(t * 512, 512), 512)
            w = wu[:, :, :, :, cs_].reshape(D, 512)
            pre = jnp.maximum(jnp.dot(rows, w, preferred_element_type=F32), 0.0)
            hid[j, :, cs_] = (pre * pre).astype(BF16)

    def down(j, first, last, sink):
        @pl.loop(first, last)
        def _(t):
            cs_ = pl.ds(pl.multiple_of(t * 512, 512), 512)
            w = jnp.concatenate([wd[t, i].reshape(D, 128) for i in range(4)], axis=1)
            sink(cs_, jnp.dot(hid[j], w, preferred_element_type=F32))

    def add_own(cs_, val):
        mixed[:, cs_] += val

    def to_part(j):
        def sink(cs_, val):
            part[j, :, cs_] = val.astype(BF16)

        return sink

    def to_acc(cs_, val):
        acc2[:, cs_] = val

    stage("up1")
    up(1)
    stage("up0")
    up(0)
    stage("b2_far")
    b2o.far()
    b2.far()
    forward([wd.at[:, yf, c]], fw_dn)
    dn_all.wait_recv()
    stage("down1")
    down(1, 0, 4, to_part(0))
    rs_send, rs_recv = cp.new_send(), cp.new_recv()
    cp.drain_later(nrm.at[three], rs_send, rs_recv)
    rs1 = [
        cp.remote(part.at[0, hi], rs_in.at[0, hi], {"x": xp}, rs_send, rs_recv),
        cp.remote(part.at[0, lo], rs_in.at[1, lo], {"x": xm}, rs_send, rs_recv),
    ]
    for r in rs1:
        r.start()
    stage("down0")
    down(0, 0, 4, add_own)
    l_mx = cp.local(mixed, own_out)
    l_mx.start()
    stage("ag_far")
    ag.far()
    stage("up3")
    up(3)
    stage("down3")
    rs2, rs3 = [], []
    for i in range(2):
        down(3, 2 * i, 2 * i + 2, to_part(1))
        wide = pl.ds(1024 * i, 1024)
        rs2.append(cp.remote(part.at[1, lo, wide], add_in.at[0, :, wide], {"x": xp}, rs_send))
        rs2.append(cp.remote(part.at[1, hi, wide], add_in.at[1, :, wide], {"x": xm}, rs_send))
        for part_rows, side, to in ((hi, 0, xp), (lo, 1, xm)):
            rs_rows = lo if side == 0 else hi
            rs3.append(
                cp.remote(
                    part.at[2, part_rows, wide], rs_in.at[side, rs_rows, wide], {"x": to},
                    rs_send, rs_recv,
                )
            )
        rs2[-2].start()
        rs2[-1].start()
    stage("ff2")
    ag.near()
    up(2)
    down(2, 0, 4, to_acc)
    for i in range(2):
        stage(f"rs_add{i}")
        lanes = slice(1024 * i, 1024 * i + 1024)
        for side in range(2):
            rs2[2 * i + side].wait_recv()
            rows = slice(HALF, ROWS) if side == 0 else slice(0, HALF)
            part[2, rows, lanes] = (
                acc2[rows, lanes] + add_in[side, :, lanes].astype(F32)
            ).astype(BF16)
            rs3[2 * i + side].start()
    stage("rs_wait")
    cp.waiter(rs_in, rs_send, rs_recv).wait_recv()
    l_mx.wait()
    stage("drain")
    assert (cp.sends, cp.recvs, cp.locals) == N_SEMS, (cp.sends, cp.recvs, cp.locals)
    for r in cp.drain:
        r.wait_send()
    stage()


def shards(
    queries, keys, values, out_gate, input_gates, forget_gates, doc_ids,
    head_gain, w_out, resid, norm_gain, w_up, w_down,
):
    vmem = pl.BlockSpec(memory_space=pltpu.VMEM)
    hbm = pl.BlockSpec(memory_space=pl.ANY)
    own, sums = pl.pallas_call(
        kernel,
        out_shape=(
            jax.ShapeDtypeStruct((ROWS, D), F32),
            jax.ShapeDtypeStruct((2, ROWS, D), BF16),
        ),
        in_specs=[vmem] * 5 + [hbm] * 8,
        out_specs=(hbm, hbm),
        scratch_shapes=[
            pltpu.VMEM((4, 4, 2, 64, D), BF16),
            pltpu.VMEM((4, 4, 2, 1024, 128), BF16),
            pltpu.VMEM((4, 2, 12, 16, D), BF16),
            pltpu.VMEM((2, 4, 8, 2, 16, 512), BF16),
            pltpu.VMEM((64, D), BF16),
            pltpu.VMEM((64, 1024), BF16),
            pltpu.VMEM((T, DK), BF16),
            pltpu.VMEM((T, DK), BF16),
            pltpu.VMEM((T, DV), BF16),
            pltpu.VMEM((T, DV), BF16),
            pltpu.VMEM((ROWS, D), BF16),
            pltpu.VMEM((3, 8, T), F32),
            pltpu.VMEM((T, 8), F32),
            pltpu.VMEM((T, DV), F32),
            pltpu.VMEM((T, DV), F32),
            pltpu.VMEM((T, 8), F32),
            pltpu.VMEM((2, 2, SROWS, DK), BF16),
            pltpu.VMEM((2, 2, SROWS, DK), BF16),
            pltpu.VMEM((2, 8, 128), F32),
            pltpu.VMEM((2, SROWS, DK), BF16),
            pltpu.VMEM((2, 2, 2, SROWS, DK), BF16),
            pltpu.VMEM((2, 2, 2, 8, 128), F32),
            pltpu.VMEM((2, 2, SROWS, DK), BF16),
            pltpu.VMEM((3, ROWS, DV), BF16),
            pltpu.VMEM((2, HALF, DV), BF16),
            pltpu.VMEM((4, ROWS, DV), BF16),
            pltpu.VMEM((ROWS, D), F32),
            pltpu.VMEM((4, ROWS, D), BF16),
            pltpu.VMEM((4, ROWS, D), BF16),
            pltpu.VMEM((3, ROWS, D), BF16),
            pltpu.VMEM((ROWS, D), F32),
            pltpu.VMEM((2, HALF, D), BF16),
            *(pltpu.SemaphoreType.DMA((k,)) for k in N_SEMS),
        ],
        compiler_params=pltpu.CompilerParams(
            collective_id=0, has_side_effects=True, vmem_limit_bytes=66 * 1024 * 1000
        ),
        name="layer",
    )(
        input_gates, forget_gates, doc_ids, head_gain.reshape(1, DV),
        norm_gain.reshape(1, D), queries, keys, values, out_gate, w_out.reshape(32, 16, D), resid, w_up,
        w_down.T,
    )
    return (own + sums[0].astype(F32) + sums[1].astype(F32)).astype(BF16)


def solution(mesh):
    split = Mesh(mesh.devices.reshape(4, 4, 2, mesh.shape["tp"]), ("z", "y", "c", "x"))
    sp = ("z", "y", "c")
    return jax.shard_map(
        shards,
        mesh=split,
        in_specs=(
            P(sp, "x"), P(sp, "x"), P(sp, "x"), P(sp, "x"),
            P(None, "x", sp), P(None, "x", sp), P(sp), P("x"), P("x", None),
            P((*sp, "x"), None), P(), P(sp, "x"), P("x", sp),
        ),
        out_specs=P((*sp, "x"), None),
        check_vma=False,
    )
```

```python
import contextlib

import jax
import jax.numpy as jnp
from jax import lax
from jax.experimental import pallas as pl
from jax.experimental.pallas import tpu as pltpu
from jax.sharding import Mesh
from jax.sharding import PartitionSpec as P

MESH = pl.DeviceIdType.MESH
F32 = jnp.float32
BF16 = jnp.bfloat16
EPS = 1e-06
FAR_LOW = -1e30

T = 768
ROWS = 192
HALF = 96
DK = 256
DV = 512
D = 2048
SROWS = 272
SCALE = DK ** (-0.5)
KP = 3
WX = 16 - 2 * KP
N_SEMS = (36, 63, 47)


class Stages:
    def __init__(self):
        self.scopes = contextlib.ExitStack()

    def __call__(self, name=None):
        self.scopes.close()
        if name:
            self.scopes.enter_context(jax.named_scope(name))


class Copies:
    def __init__(self, send, recv, loc):
        self.send, self.recv, self.loc = send, recv, loc
        self.sends = self.recvs = self.locals = 0
        self.drain = []

    def new_send(self):
        self.sends += 1
        return self.send.at[self.sends - 1]

    def new_recv(self):
        self.recvs += 1
        return self.recv.at[self.recvs - 1]

    def remote(self, src, dst, dev, send=None, recv=None):
        alone = send is None
        c = pltpu.make_async_remote_copy(
            src_ref=src,
            dst_ref=dst,
            send_sem=self.new_send() if alone else send,
            recv_sem=self.new_recv() if recv is None else recv,
            device_id=dev,
            device_id_type=MESH,
        )
        if alone:
            self.drain.append(c)
        return c

    def waiter(self, ref, send, recv):
        return pltpu.make_async_remote_copy(
            src_ref=ref,
            dst_ref=ref,
            send_sem=send,
            recv_sem=recv,
            device_id={"c": 1 - lax.axis_index("c")},
            device_id_type=MESH,
        )

    def drain_later(self, ref, send, recv):
        self.drain.append(self.waiter(ref, send, recv))

    def local(self, src, dst):
        self.locals += 1
        return pltpu.make_async_copy(src, dst, self.loc.at[self.locals - 1])


class Ring:
    def __init__(
        self, cp, plus, minus, own, put_plus, put_minus, near0, near1, far0, far1, block, three
    ):
        send = cp.new_send()
        self.first, self.second, self.third = (cp.new_recv() for _ in range(3))

        def group(srcs, dsts, dev, recv):
            return [cp.remote(s, d, dev, send, recv) for s, d in zip(srcs, dsts, strict=True)]

        self.out0 = group(own(0), put_plus(0), plus, self.first)
        self.out0 += group(own(1), put_minus(1), minus, self.first)
        self.out1 = group(own(1), put_plus(1), plus, self.second)
        self.out1 += group(own(0), put_minus(0), minus, self.second)
        self.on = group(near0, far0, plus, self.third) + group(near1, far1, minus, self.third)
        self.waits = [cp.waiter(block, send, r) for r in (self.first, self.second, self.third)]
        cp.drain_later(three, send, self.first)

    def start0(self):
        for c in self.out0:
            c.start()

    def start1(self):
        for c in self.out1:
            c.start()

    def start(self):
        self.start0()
        self.start1()

    def relay(self):
        self.waits[0].wait_recv()
        for c in self.on:
            c.start()

    def near(self):
        self.waits[1].wait_recv()

    def far(self):
        self.waits[2].wait_recv()


def slot_ring(cp, plus, minus, p, slots, block, three):
    up, down = lax.rem(p + 1, 4), lax.rem(p + 3, 4)
    at = lambda pos, h: [f(pos, h) for f in slots]
    own = lambda h: at(p, h)
    return Ring(
        cp, plus, minus, own, own, own, at(down, 0), at(up, 1), at(down, 0), at(up, 1), block, three
    )


def roll_lanes(x, shift):
    return pltpu.roll(x, shift % T, 1)


def kernel(
    ig_h, fg_h, doc_h, gain_h, ngain_h,
    q_h, k_h, v_h, og_h, wout_h, resid_h, wup_h, wdn_h,
    own_out, rs_in,
    ig_ref, fg_ref, doc_ref, gain_ref, ngain_ref,
    wu, wd, wox, wop, wa, wb, q, k, v, og, resid,
    arow, cols, numf, numb, dens,
    st_own, st_par, sc_pair, q_send, q_recv, sc_recv, cin,
    ro_out, ro_st, ro, mixed, nrm, hid, part, acc2, add_in,
    send_sem, recv_sem, loc_sem,
):
    z, y, c, x = (lax.axis_index(a) for a in ("z", "y", "c", "x"))
    other = 1 - c
    n = z * 4 + y
    n_up, n_dn = lax.rem(n + 1, 16), lax.rem(n + 15, 16)
    chip_up = {"z": lax.div(n_up, 4), "y": lax.rem(n_up, 4)}
    chip_dn = {"z": lax.div(n_dn, 4), "y": lax.rem(n_dn, 4)}
    partner = {"c": other}
    xp, xm, xf = lax.rem(x + 1, 4), lax.rem(x + 3, 4), lax.rem(x + 2, 4)
    cp = Copies(send_sem, recv_sem, loc_sem)
    stage = Stages()
    stage("loads")

    l_wd = cp.local(wdn_h, wa)
    l_wu = cp.local(wup_h, wu.at[z, y, c])
    l_wo = [cp.local(wout_h.at[pl.ds(WX * i, WX)], wox.at[0, i]) for i in range(2)]
    l_k = cp.local(k_h, k)
    l_v = cp.local(v_h, v)
    l_q = cp.local(q_h, q)
    l_og = cp.local(og_h, og)
    l_wp = [
        cp.local(
            wout_h.at[pl.ds(2 * WX + KP * i, KP), :, pl.ds(1024 * j + 256 * b, 256)],
            wop.at[j, 0, i, b],
        )
        for i in range(4)
        for j in range(2)
        for b in range(4)
    ]
    l_re = cp.local(resid_h, resid)
    l_gate = [cp.local(a, b) for a, b in ((ig_h, ig_ref), (fg_h, fg_ref), (doc_h, doc_ref))]
    l_gain = [cp.local(gain_h, gain_ref), cp.local(ngain_h, ngain_ref)]
    loads = (l_wu, *l_gate, l_wd, *l_wo, l_k, l_v, l_q, l_og, *l_gain, *l_wp, l_re)

    stage("barrier")
    barrier = pltpu.get_barrier_semaphore()
    peers = (
        partner, {"y": lax.rem(y + 1, 4)}, {"y": lax.rem(y + 3, 4)}, {"z": lax.rem(z + 1, 4)},
        {"z": lax.rem(z + 3, 4)}, {"x": xp}, {"x": xm}, {"x": xf}, chip_up, chip_dn,
    )
    for dev in peers:
        pl.semaphore_signal(barrier, inc=1, device_id=dev, device_id_type=MESH)
    for l in loads:
        l.start()
    pl.semaphore_wait(barrier, len(peers))

    stage("first_sends")
    zp, zm, zf = lax.rem(z + 1, 4), lax.rem(z + 3, 4), lax.rem(z + 2, 4)
    yp, ym, yf = lax.rem(y + 1, 4), lax.rem(y + 3, 4), lax.rem(y + 2, 4)
    over_y, over_z = ({"y": yp}, {"y": ym}), ({"z": zp}, {"z": zm})
    up_half = lambda a, b, h: wu.at[a, b, c, pl.ds(32 * h, 32)]
    dn_half = lambda a, b, h: wd.at[a, b, c, pl.ds(512 * h, 512)]
    three = pl.ds(0, 3)
    a1 = slot_ring(
        cp, *over_y, y, [lambda p, h: up_half(z, p, h)], wu.at[z, y, c], wu.at[z, three, c]
    )
    a2o = slot_ring(
        cp, *over_z, z, [lambda p, h: up_half(p, y, h)], wu.at[z, y, c], wu.at[z, three, c]
    )
    a2 = slot_ring(
        cp, *over_z, z, [lambda p, h, o=o: up_half(p, o, h) for o in (yp, ym, yf)],
        wu.at[z, three, c], wu.at[three, three, c],
    )
    b1 = slot_ring(
        cp, *over_z, z, [lambda p, h: dn_half(p, y, h)], wd.at[z, y, c], wd.at[z, three, c]
    )
    b2o = slot_ring(
        cp, *over_y, y, [lambda p, h: dn_half(z, p, h)], wd.at[z, y, c], wd.at[z, three, c]
    )
    b2 = slot_ring(
        cp, *over_y, y, [lambda p, h, o=o: dn_half(o, p, h) for o in (zp, zm, zf)],
        wd.at[z, three, c], wd.at[three, three, c],
    )

    wx = lambda j, h: wox.at[j, c, pl.ds(WX // 2 * h, WX // 2)]
    wr = Ring(
        cp, {"x": xp}, {"x": xm},
        lambda h: [wx(0, h)], lambda h: [wx(3, h)], lambda h: [wx(1, h)],
        [wx(3, 0)], [wx(1, 1)], [wx(2, 0)], [wx(2, 1)], wox.at[0, c], wox.at[three, c],
    )
    a_pos, b_pos = jnp.where(c == 0, z, y), jnp.where(c == 0, y, z)
    cols_c = pl.ds(pl.multiple_of(1024 * c + 256 * b_pos, 256), 256)
    wp_send, wp_recv = cp.new_send(), cp.new_recv()
    wp = [
        cp.remote(
            wout_h.at[pl.ds(2 * WX + KP * a_pos, KP), :, cols_c], wop.at[c, j, a_pos, b_pos],
            {"x": to}, wp_send, wp_recv,
        )
        for to, j in ((xp, 3), (xm, 1), (xf, 2))
    ]
    wp_all = cp.waiter(wop.at[c, three, 0, 0], wp_send, wp_recv)
    cp.drain.append(wp_all)

    def dev_b(step):
        return {
            "z": jnp.where(c == 0, z, lax.rem(z + step, 4)),
            "y": jnp.where(c == 0, lax.rem(y + step, 4), y),
        }

    def dev_a(step):
        return {
            "z": jnp.where(c == 0, lax.rem(z + step, 4), z),
            "y": jnp.where(c == 0, y, lax.rem(y + step, 4)),
        }

    heads = pl.ds(1, 3)
    c1 = slot_ring(
        cp, dev_b(1), dev_b(3), b_pos,
        [lambda p, h: wop.at[c, heads, a_pos, p, :, :, pl.ds(128 * h, 128)]],
        wop.at[c, heads, 0, 0], wop.at[c, heads, 0, three],
    )
    c2 = slot_ring(
        cp, dev_a(1), dev_a(3), a_pos,
        [lambda p, h: wop.at[c, heads, p, :, :, :, pl.ds(128 * h, 128)]],
        wop.at[c, heads, 0], wop.at[c, heads, three],
    )

    for w in wp:
        w.start()
    l_wu.wait()
    a1.start0()
    a2o.start0()
    l_wd.wait()
    d_wd = cp.remote(wa.at[:, pl.ds(pl.multiple_of(1024 * other, 1024), 1024)], wb, partner)
    d_wd.start()
    for l in l_wo:
        l.wait()
    wr.start()

    stage("gates")
    for l in l_gate:
        l.wait()
    def row(ref, i):
        return jnp.broadcast_to(ref[i], (8, T))

    lane = lax.broadcasted_iota(jnp.int32, (8, T), 1)
    rowi = lax.broadcasted_iota(jnp.int32, (8, T), 0)
    doc = jnp.broadcast_to(doc_ref[...].astype(F32)[None, :], (8, T))

    def log_sigmoid(f):
        return jnp.minimum(f, 0.0) - jnp.log1p(jnp.exp(-jnp.abs(f)))

    cumf, cumb = log_sigmoid(row(fg_ref, 0)), log_sigmoid(row(fg_ref, 1))
    sh = 1
    while sh < T:
        cumf = cumf + jnp.where(lane >= sh, roll_lanes(cumf, sh), 0.0)
        cumb = cumb + jnp.where(lane < T - sh, roll_lanes(cumb, T - sh), 0.0)
        sh *= 2
    af, ab = row(ig_ref, 0) - cumf, row(ig_ref, 1) - cumb
    mf, mb = af, ab
    sh = 1
    while sh < T:
        same_f = (lane >= sh) & (roll_lanes(doc, sh) == doc)
        same_b = (lane < T - sh) & (roll_lanes(doc, T - sh) == doc)
        mf = jnp.where(same_f, jnp.maximum(mf, roll_lanes(mf, sh)), mf)
        mb = jnp.where(same_b, jnp.maximum(mb, roll_lanes(mb, T - sh)), mb)
        sh *= 2
    doc0, docl = doc[:, 0:1], doc[:, T - 1 : T]
    mxf, mxb = mf[:, T - 1 : T], mb[:, 0:1]
    totf, totb = cumf[:, T - 1 : T], cumb[:, 0:1]
    wf = jnp.where(doc == docl, jnp.exp(af - mxf), 0.0)
    wbk = jnp.where(doc == doc0, jnp.exp(ab - mxb), 0.0)
    arow[0] = af
    arow[1] = ab
    arow[2] = doc
    stack = jnp.where(
        rowi == 0, mf,
        jnp.where(rowi == 1, mb, jnp.where(rowi == 2, doc, jnp.where(rowi == 3, wf, wbk))),
    )
    cols[...] = stack.T
    r8 = lax.broadcasted_iota(jnp.int32, (8, 128), 0)
    scal = jnp.zeros((8, 128), F32)
    for i, val in enumerate((totf + mxf, totb + mxb, totf, totb, doc0, docl)):
        scal = jnp.where(r8 == i, jnp.broadcast_to(val, (8, 128)), scal)
    sc_pair[c] = scal
    d_sc = cp.remote(sc_pair.at[c], sc_pair.at[c], partner)
    d_sc.start()

    stage("state")
    l_k.wait()
    l_v.wait()
    keys = k[...].astype(F32)
    d_st = []
    for d in range(2):
        weighted = (keys * cols[:, 3 + d : 4 + d]).astype(BF16)
        st = lax.dot_general(
            v[...], weighted, (((0,), (0,)), ((), ())), preferred_element_type=F32
        ).astype(BF16)
        norm = jnp.sum(weighted.astype(F32), axis=0, keepdims=True)
        tail = jnp.broadcast_to(norm, (16, DK)).astype(BF16)
        for h in range(2):
            st_own[d, h, 0:256, :] = st[256 * h : 256 * h + 256]
            st_own[d, h, 256:SROWS, :] = tail
        d_st.append(cp.remote(st_own.at[d], st_par.at[d], partner))
        d_st[d].start()

    stage("wd_block")
    d_wd.wait_recv()
    ei = lax.broadcasted_iota(jnp.int32, (64, 128), 0)
    ej = lax.broadcasted_iota(jnp.int32, (64, 128), 1)
    put_own = jnp.where(ej == ei + 64 * c, 1.0, 0.0).astype(BF16)
    put_par = jnp.where(ej == ei + 64 * other, 1.0, 0.0).astype(BF16)
    mine = wa[:, pl.ds(pl.multiple_of(1024 * c, 1024), 1024)]
    tn = (((0,), (0,)), ((), ()))
    wd[z, y, c] = (
        lax.dot_general(mine, put_own, tn, preferred_element_type=F32)
        + lax.dot_general(wb[...], put_par, tn, preferred_element_type=F32)
    ).astype(BF16)
    b1.start0()

    stage("pair_wait")
    def pick(ref, i):
        return ref[i : i + 1, 0:1]

    def pair_terms(s0, s1, d):
        early, late = (s0, s1) if d == 0 else (s1, s0)
        e_last = early[5 - d : 6 - d, 0:1]
        l_first, l_last = late[4 + d : 5 + d, 0:1], late[5 - d : 6 - d, 0:1]
        linked = (l_first == e_last) & (l_first == l_last)
        e_top = early[d : d + 1, 0:1] + late[2 + d : 3 + d, 0:1]
        l_top = late[d : d + 1, 0:1]
        top = jnp.where(linked, jnp.maximum(l_top, e_top), l_top)
        f_early = jnp.where(linked, jnp.exp(jnp.minimum(e_top - top, 0.0)), 0.0)
        f_late = jnp.exp(l_top - top)
        total = early[2 + d : 3 + d, 0:1] + late[2 + d : 3 + d, 0:1]
        return top, total, f_early, f_late, l_last

    d_sc.wait_recv()
    s0, s1 = sc_pair[0], sc_pair[1]
    cq = []
    cs = []
    for d in range(2):
        pos = c if d == 0 else other
        _, _, f_early, f_late, _ = pair_terms(s0, s1, d)
        f_own = jnp.where(pos == 0, f_early, f_late)
        f_par = jnp.where(pos == 0, f_late, f_early)
        d_st[d].wait_recv()
        q_send[d] = (f_own * st_own[d, c].astype(F32) + f_par * st_par[d, c].astype(F32)).astype(BF16)
        to = chip_up if d == 0 else chip_dn
        cs.append(cp.remote(sc_pair, sc_recv.at[d, 0], to))
        cq.append(cp.remote(q_send.at[d], q_recv.at[d, 0, c], to))
        cs[-1].start()
        cq[-1].start()

    stage("intra0")
    l_q.wait()

    def intra(r0, size):
        qb = q[r0 : r0 + size, :]
        mfc, mbc, dc = (cols[r0 : r0 + size, i : i + 1] for i in range(3))
        score = (
            lax.dot_general(qb, k[...], (((1,), (1,)), ((), ())), preferred_element_type=F32)
            * SCALE
        )
        for d in range(2):
            lo, hi = (0, r0 + size) if d == 0 else (r0, T)
            ti = r0 + lax.broadcasted_iota(jnp.int32, (size, hi - lo), 0)
            si = lo + lax.broadcasted_iota(jnp.int32, (size, hi - lo), 1)
            keep = ((si <= ti) if d == 0 else (si >= ti)) & (arow[2, 0:1, lo:hi] == dc)
            e = jnp.exp(jnp.minimum(arow[d, 0:1, lo:hi] - (mfc if d == 0 else mbc), 0.0))
            w = jnp.where(keep, score[:, lo:hi] * e, 0.0)
            dens[r0 : r0 + size, d : d + 1] = jnp.sum(w, axis=1, keepdims=True)
            num = jnp.dot(w.astype(BF16), v[lo:hi, :], preferred_element_type=F32)
            (numf if d == 0 else numb)[r0 : r0 + size, :] = num

    intra(0, 256)
    stage("pieces")
    wp_all.wait_recv()
    c1.start()
    b1.start1()
    stage("intra1")
    intra(256, 256)
    stage("intra2")
    intra(512, 256)

    stage("c1_relay")
    c1.relay()
    stage("carry_near")
    rq, rs, dq = [], [], []
    for d in range(2):
        to = chip_up if d == 0 else chip_dn
        rs.append(cp.remote(sc_recv.at[d, 0], sc_recv.at[d, 1], to))
        rq.append(cp.remote(q_recv.at[d, 0, c], q_recv.at[d, 1, c], to))
        dq.append(cp.remote(q_recv.at[d, 0, c], q_recv.at[d, 0, c], partner))
        cs[d].wait_recv()
        rs[d].start()
        cq[d].wait_recv()
        rq[d].start()
        dq[d].start()
    stage("b1_relay")
    b1.relay()
    stage("wr_relay")
    wr.relay()
    stage("c1_wait")
    c1.near()
    c1.far()
    c2.start()
    a1.start1()
    a2o.start1()
    a1.relay()

    stage("carry_far")
    dq2 = []
    for d in range(2):
        rs[d].wait_recv()
        rq[d].wait_recv()
        dq2.append(cp.remote(q_recv.at[d, 1, c], q_recv.at[d, 1, c], partner))
        dq2[d].start()
    fw_send, fo_send = cp.new_send(), cp.new_send()
    fw_up, fw_up2, fw_dn, fw_dn2, fo_recv = (cp.new_recv() for _ in range(5))

    def forward(refs, recv, send=fw_send):
        for r in refs:
            cp.remote(r, r, partner, send, recv).start()

    def second_phase():
        stage("c2_relay")
        c2.relay()
        b2o.start()
        a2o.relay()
        wr.near()
        forward([wox.at[j, c] for j in (1, 3)], fo_recv, fo_send)
        stage("emit_rest")

    stage("carry_combine")
    scal_in = []
    for d in range(2):
        pos = c if d == 0 else other
        chip = n if d == 0 else 15 - n
        own_s = sc_pair[c]
        par_s = sc_pair[other]
        first = own_s[4 + d : 5 + d, 0:1]
        t1, tot1, _, _, last1 = pair_terms(sc_recv[d, 0, 0], sc_recv[d, 0, 1], d)
        t2, _, _, _, last2 = pair_terms(sc_recv[d, 1, 0], sc_recv[d, 1, 1], d)
        l0 = (par_s[5 - d : 6 - d, 0:1] == first) & (pos == 1)
        l1 = (last1 == first) & (chip >= 1)
        l2 = (last2 == first) & (chip >= 2)
        shift = jnp.where(pos == 1, par_s[2 + d : 3 + d, 0:1], 0.0)
        e0 = jnp.where(l0, par_s[d : d + 1, 0:1], FAR_LOW)
        e1 = jnp.where(l1, t1 + shift, FAR_LOW)
        e2 = jnp.where(l2, t2 + tot1 + shift, FAR_LOW)
        top = jnp.maximum(e0, jnp.maximum(e1, e2))
        g0 = jnp.where(l0, jnp.exp(e0 - top), 0.0)
        g1 = jnp.where(l1, jnp.exp(e1 - top), 0.0)
        g2 = jnp.where(l2, jnp.exp(e2 - top), 0.0)
        late = jnp.where(pos == 1, 1.0, 0.0)
        linked = late * jnp.where(l0, 1.0, 0.0) + (1.0 - late) * jnp.where(l1, 1.0, 0.0)
        dq[d].wait_recv()
        dq2[d].wait_recv()
        for h in range(2):
            cin[d, h] = (
                g0 * st_par[d, h].astype(F32)
                + g1 * q_recv[d, 0, h].astype(F32)
                + g2 * q_recv[d, 1, h].astype(F32)
            ).astype(BF16)
        scal_in.append((top, linked, first))

    stage("emit")
    for l in (l_og, *l_gain):
        l.wait()
    ca = []
    lo, hi = pl.ds(0, HALF), pl.ds(HALF, HALF)
    for step, to in enumerate((xf, xp, xm, x)):
        r0 = pl.multiple_of(to * ROWS, 64)
        rows = pl.ds(r0, ROWS)
        qb = q[rows, :]
        qw = qb.astype(F32)
        dc = cols[rows, 2:3]
        memory = None
        for d in range(2):
            top, linked, first = scal_in[d]
            m_loc = cols[rows, d : d + 1]
            usable = jnp.where(dc == first, linked, 0.0) > 0.5
            m = jnp.where(usable, jnp.maximum(m_loc, top), m_loc)
            keep = jnp.exp(m_loc - m)
            inter = jnp.where(usable, jnp.exp(jnp.minimum(top - m, 0.0)), 0.0) * SCALE
            nt = (((1,), (1,)), ((), ()))
            qc = jnp.concatenate(
                [
                    lax.dot_general(qb, cin[d, h, 0:256, :], nt, preferred_element_type=F32)
                    for h in range(2)
                ],
                axis=1,
            )
            norm = cin[d, 0, 256:257, :].astype(F32)
            num = keep * (numf if d == 0 else numb)[rows, :] + inter * qc
            den = keep * dens[rows, d : d + 1] + inter * jnp.sum(qw * norm, axis=1, keepdims=True)
            h_dir = num / jnp.maximum(jnp.abs(den), 1.0)
            memory = h_dir if memory is None else memory + h_dir
        normed = memory * lax.rsqrt(jnp.mean(memory * memory, axis=1, keepdims=True) + EPS)
        gate = 1.0 / (1.0 + jnp.exp(-og[rows, :].astype(F32)))
        readout = (normed * gain_ref[...] * gate).astype(BF16)
        if step == 3:
            ro[x] = readout
        else:
            ro_out[step] = readout
        if step == 0:
            ca0 = [
                cp.remote(ro_out.at[0, lo], ro_st.at[0], {"x": xp}),
                cp.remote(ro_out.at[0, hi], ro_st.at[1], {"x": xm}),
            ]
            for cc in ca0:
                cc.start()
            second_phase()
        elif step < 3:
            ca.append(cp.remote(ro_out.at[step], ro.at[x], {"x": to}))
            ca[-1].start()
    stage("a1_wait")
    b1.near()
    b1.far()
    b2.start()
    a1.near()
    a1.far()
    a2.start()
    stage("a2a_relay")
    ca += [
        cp.remote(ro_st.at[0], ro.at[xm, lo], {"x": xp}),
        cp.remote(ro_st.at[1], ro.at[xp, hi], {"x": xm}),
    ]
    for i in range(2):
        ca0[i].wait_recv()
        ca[2 + i].start()

    stage("wout_fwd")
    wr.far()
    forward([wox.at[2, c]], fo_recv, fo_send)
    c2.near()
    c2.far()
    forward([wop.at[c, heads]], fo_recv, fo_send)
    b2o.relay()
    stage("a2a_wait")
    l_re.wait()
    for l in l_wp:
        l.wait()
    stage("wout")

    def project(j):
        head = ro.at[lax.rem(x + j, 4)]
        base = resid if j == 0 else mixed
        for t in range(4):
            cs_ = slice(512 * t, 512 * t + 512)
            w0 = wox[j, :, :, :, cs_].reshape(512 - 64 * KP, 512)
            at = [wop[t // 2, j, :, 2 * (t % 2) + i].reshape(64 * KP, 256) for i in range(2)]
            one = jnp.dot(head[:, 0 : 512 - 64 * KP], w0, preferred_element_type=F32) + jnp.dot(
                head[:, 512 - 64 * KP : 512],
                jnp.concatenate(at, axis=1),
                preferred_element_type=F32,
            )
            mixed[:, cs_] = base[:, cs_].astype(F32) + one.astype(BF16).astype(F32)

    project(0)
    stage("fo_wait")
    fo_all = cp.waiter(nrm, fo_send, fo_recv)
    fo_all.wait_recv()
    cp.drain.append(fo_all)
    stage("near_wait")
    ca[0].wait_recv()
    project(3)
    ca[1].wait_recv()
    project(1)
    stage("far_wait")
    ca[2].wait_recv()
    ca[3].wait_recv()
    stage("far_project")
    project(2)

    mx = mixed[...]
    factor = lax.rsqrt(jnp.mean(mx * mx, axis=1, keepdims=True) + EPS)
    nrm[0] = (mx * factor * ngain_ref[...]).astype(BF16)

    h01 = lambda j, h: nrm.at[j, pl.ds(HALF * h, HALF)]
    ag = Ring(
        cp, {"x": xp}, {"x": xm},
        lambda h: [h01(0, h)],
        lambda h: [h01(1 + h, 0)],
        lambda h: [h01(2 - h, 1)],
        [h01(1, 0)], [h01(1, 1)], [h01(3, 0)], [h01(3, 1)], nrm.at[0], nrm.at[three],
    )
    ag.start()
    up_most = cp.waiter(wu.at[three, :, 0], fw_send, fw_up)
    up_last = cp.waiter(wu.at[0, :, 0], fw_send, fw_up2)
    dn_most = cp.waiter(wd.at[three, :, 0], fw_send, fw_dn)
    dn_last = cp.waiter(wd.at[0, :, 0], fw_send, fw_dn2)
    cp.drain_later(wu, fw_send, fw_up)

    def up(j, zs, start=None, final=True):
        @pl.loop(0, 4)
        def _(t):
            cs_ = pl.ds(pl.multiple_of(t * 512, 512), 512)
            if zs is None:
                pre = jnp.dot(
                    nrm[j], wu[:, :, :, :, cs_].reshape(D, 512), preferred_element_type=F32
                )
            else:
                pre = start[:, cs_] if start is not None else None
                for zz in zs:
                    one = jnp.dot(
                        nrm[j, :, pl.ds(pl.multiple_of(512 * zz, 512), 512)],
                        wu[zz, :, :, :, cs_].reshape(512, 512),
                        preferred_element_type=F32,
                    )
                    pre = one if pre is None else pre + one
            if final:
                pre = jnp.maximum(pre, 0.0)
                hid[j, :, cs_] = (pre * pre).astype(BF16)
            else:
                acc2[:, cs_] = pre

    def down(j, first, last, sink):
        @pl.loop(first, last)
        def _(t):
            cs_ = pl.ds(pl.multiple_of(t * 512, 512), 512)
            w = jnp.concatenate([wd[t, i].reshape(D, 128) for i in range(4)], axis=1)
            sink(cs_, jnp.dot(hid[j], w, preferred_element_type=F32))

    def add_own(cs_, val):
        mixed[:, cs_] += val

    def to_part(j):
        def sink(cs_, val):
            part[j, :, cs_] = val.astype(BF16)

        return sink

    def to_acc(cs_, val):
        acc2[:, cs_] = val

    rs_send, rs_recv = cp.new_send(), cp.new_recv()
    cp.drain_later(nrm.at[three], rs_send, rs_recv)

    def first_sums(yy):
        w = jnp.concatenate([wd[i, yy].reshape(D, 128) for i in range(4)], axis=1)
        val = jnp.dot(hid[1], w, preferred_element_type=F32).astype(BF16)
        for i in range(4):
            strip = pl.ds(pl.multiple_of((4 * i + yy) * 128, 128), 128)
            part[0, :, strip] = val[:, 128 * i : 128 * i + 128]
        for i in range(4):
            strip = pl.ds(pl.multiple_of((4 * i + yy) * 128, 128), 128)
            for rows, side, to in ((hi, 0, xp), (lo, 1, xm)):
                cp.remote(
                    part.at[0, rows, strip], rs_in.at[side, rows, strip], {"x": to}, rs_send, rs_recv
                ).start()

    up_other, dn_other = (yp, ym, yf), (zp, zm, zf)
    lower, upper = [pl.ds(32 * h, 32) for h in range(2)], [pl.ds(512 * h, 512) for h in range(2)]

    def up_part(row, h):
        return [wu.at[row, o, c, lower[h]] for o in up_other]

    def dn_part(col, h):
        return [wd.at[o, col, c, upper[h]] for o in dn_other]

    stage("own_rows")
    forward([wu.at[z, :, c]], fw_up)
    forward([wd.at[:, y, c]], fw_dn)
    a2o.near()
    a2o.far()
    forward([wu.at[zp, y, c], wu.at[zm, y, c]], fw_up)
    forward([wu.at[zf, y, c]], fw_up2)
    stage("a2_relay")
    a2.relay()
    forward(up_part(zm, 0) + up_part(zp, 1), fw_up)
    stage("b2_relay")
    b2o.near()
    b2.relay()
    forward([wd.at[z, yp, c], wd.at[z, ym, c]], fw_dn)
    forward(dn_part(ym, 0) + dn_part(yp, 1), fw_dn)
    stage("a2_near")
    a2.near()
    forward(up_part(zm, 1) + up_part(zp, 0), fw_up)
    stage("b2_near")
    b2.near()
    forward(dn_part(ym, 1) + dn_part(yp, 0), fw_dn)
    stage("ag_relay")
    ag.relay()
    stage("up1_most")
    up_most.wait_recv()
    up(1, (z, zp, zm), final=False)
    stage("a2_far")
    a2.far()
    forward(up_part(zf, 0) + up_part(zf, 1), fw_up2)
    up_last.wait_recv()
    stage("up1_last")
    up(1, (zf,), start=acc2)
    stage("down1_most")
    dn_most.wait_recv()
    for yy in (y, yp, ym):
        first_sums(yy)
    stage("b2_far")
    b2o.far()
    b2.far()
    forward([wd.at[:, yf, c]], fw_dn2)
    stage("up0")
    up(0, None)
    stage("down1_last")
    dn_last.wait_recv()
    first_sums(yf)
    stage("ag_far")
    ag.far()
    stage("up3")
    up(3, None)
    stage("down3")
    rs2, rs3 = [], []
    for i in range(2):
        down(3, 2 * i, 2 * i + 2, to_part(1))
        wide = pl.ds(1024 * i, 1024)
        rs2.append(cp.remote(part.at[1, lo, wide], add_in.at[0, :, wide], {"x": xp}, rs_send))
        rs2.append(cp.remote(part.at[1, hi, wide], add_in.at[1, :, wide], {"x": xm}, rs_send))
        for part_rows, side, to in ((hi, 0, xp), (lo, 1, xm)):
            rs_rows = lo if side == 0 else hi
            rs3.append(
                cp.remote(
                    part.at[2, part_rows, wide], rs_in.at[side, rs_rows, wide], {"x": to},
                    rs_send, rs_recv,
                )
            )
        rs2[-2].start()
        rs2[-1].start()
    stage("ff2")
    ag.near()
    up(2, None)
    down(2, 0, 4, to_acc)
    for i in range(2):
        stage(f"rs_add{i}")
        lanes = slice(1024 * i, 1024 * i + 1024)
        for side in range(2):
            rs2[2 * i + side].wait_recv()
            rows = slice(HALF, ROWS) if side == 0 else slice(0, HALF)
            part[2, rows, lanes] = (
                acc2[rows, lanes] + add_in[side, :, lanes].astype(F32)
            ).astype(BF16)
            rs3[2 * i + side].start()
    stage("down0")
    down(0, 0, 4, add_own)
    l_mx = cp.local(mixed, own_out)
    l_mx.start()
    stage("rs_wait")
    cp.waiter(rs_in, rs_send, rs_recv).wait_recv()
    l_mx.wait()
    stage("drain")
    assert (cp.sends, cp.recvs, cp.locals) == N_SEMS, (cp.sends, cp.recvs, cp.locals)
    for r in cp.drain:
        r.wait_send()
    stage()


def shards(
    queries, keys, values, out_gate, input_gates, forget_gates, doc_ids,
    head_gain, w_out, resid, norm_gain, w_up, w_down,
):
    hbm = pl.BlockSpec(memory_space=pl.ANY)
    own, sums = pl.pallas_call(
        kernel,
        out_shape=(
            jax.ShapeDtypeStruct((ROWS, D), F32),
            jax.ShapeDtypeStruct((2, ROWS, D), BF16),
        ),
        in_specs=[hbm] * 13,
        out_specs=(hbm, hbm),
        scratch_shapes=[
            pltpu.VMEM((2, 1, T), F32),
            pltpu.VMEM((2, 1, T), F32),
            pltpu.VMEM((T,), jnp.int32),
            pltpu.VMEM((1, DV), F32),
            pltpu.VMEM((1, D), F32),
            pltpu.VMEM((4, 4, 2, 64, D), BF16),
            pltpu.VMEM((4, 4, 2, 1024, 128), BF16),
            pltpu.VMEM((4, 2, WX, 16, D), BF16),
            pltpu.VMEM((2, 4, 4, 4, KP, 16, 256), BF16),
            pltpu.VMEM((64, D), BF16),
            pltpu.VMEM((64, 1024), BF16),
            pltpu.VMEM((T, DK), BF16),
            pltpu.VMEM((T, DK), BF16),
            pltpu.VMEM((T, DV), BF16),
            pltpu.VMEM((T, DV), BF16),
            pltpu.VMEM((ROWS, D), BF16),
            pltpu.VMEM((3, 8, T), F32),
            pltpu.VMEM((T, 8), F32),
            pltpu.VMEM((T, DV), F32),
            pltpu.VMEM((T, DV), F32),
            pltpu.VMEM((T, 8), F32),
            pltpu.VMEM((2, 2, SROWS, DK), BF16),
            pltpu.VMEM((2, 2, SROWS, DK), BF16),
            pltpu.VMEM((2, 8, 128), F32),
            pltpu.VMEM((2, SROWS, DK), BF16),
            pltpu.VMEM((2, 2, 2, SROWS, DK), BF16),
            pltpu.VMEM((2, 2, 2, 8, 128), F32),
            pltpu.VMEM((2, 2, SROWS, DK), BF16),
            pltpu.VMEM((3, ROWS, DV), BF16),
            pltpu.VMEM((2, HALF, DV), BF16),
            pltpu.VMEM((4, ROWS, DV), BF16),
            pltpu.VMEM((ROWS, D), F32),
            pltpu.VMEM((4, ROWS, D), BF16),
            pltpu.VMEM((4, ROWS, D), BF16),
            pltpu.VMEM((3, ROWS, D), BF16),
            pltpu.VMEM((ROWS, D), F32),
            pltpu.VMEM((2, HALF, D), BF16),
            *(pltpu.SemaphoreType.DMA((k,)) for k in N_SEMS),
        ],
        compiler_params=pltpu.CompilerParams(
            collective_id=0, has_side_effects=True, vmem_limit_bytes=66 * 1024 * 1000
        ),
        name="layer",
    )(
        input_gates, forget_gates, doc_ids, head_gain.reshape(1, DV),
        norm_gain.reshape(1, D), queries, keys, values, out_gate, w_out.reshape(32, 16, D), resid, w_up,
        w_down.T,
    )
    return (own + sums[0].astype(F32) + sums[1].astype(F32)).astype(BF16)


def solution(mesh):
    split = Mesh(mesh.devices.reshape(4, 4, 2, mesh.shape["tp"]), ("z", "y", "c", "x"))
    sp = ("z", "y", "c")
    return jax.shard_map(
        shards,
        mesh=split,
        in_specs=(
            P(sp, "x"), P(sp, "x"), P(sp, "x"), P(sp, "x"),
            P(None, "x", sp), P(None, "x", sp), P(sp), P("x"), P("x", None),
            P((*sp, "x"), None), P(), P(sp, "x"), P("x", sp),
        ),
        out_specs=P((*sp, "x"), None),
        check_vma=False,
    )
```

```python
import contextlib

import jax
import jax.numpy as jnp
from jax import lax
from jax.experimental import pallas as pl
from jax.experimental.pallas import tpu as pltpu
from jax.sharding import Mesh
from jax.sharding import PartitionSpec as P

MESH = pl.DeviceIdType.MESH
F32 = jnp.float32
BF16 = jnp.bfloat16
EPS = 1e-06
FAR_LOW = -1e30

T = 768
ROWS = 192
HALF = 96
DK = 256
DV = 512
D = 2048
SROWS = 272
SCALE = DK ** (-0.5)
KP = 3
WX = 16 - 2 * KP
N_SEMS = (20, 60, 16)


class Stages:
    def __init__(self):
        self.scopes = contextlib.ExitStack()

    def __call__(self, name=None):
        self.scopes.close()
        if name:
            self.scopes.enter_context(jax.named_scope(name))


class Copies:
    def __init__(self, send, recv, loc):
        self.send, self.recv, self.loc = send, recv, loc
        self.sends = self.recvs = self.locals = 0
        self.drain = []

    def new_send(self):
        self.sends += 1
        return self.send.at[self.sends - 1]

    def new_recv(self):
        self.recvs += 1
        return self.recv.at[self.recvs - 1]

    def remote(self, src, dst, dev, send=None, recv=None):
        alone = send is None
        c = pltpu.make_async_remote_copy(
            src_ref=src,
            dst_ref=dst,
            send_sem=self.new_send() if alone else send,
            recv_sem=self.new_recv() if recv is None else recv,
            device_id=dev,
            device_id_type=MESH,
        )
        if alone:
            self.drain.append(c)
        return c

    def waiter(self, ref, send, recv):
        return pltpu.make_async_remote_copy(
            src_ref=ref,
            dst_ref=ref,
            send_sem=send,
            recv_sem=recv,
            device_id={"c": 1 - lax.axis_index("c")},
            device_id_type=MESH,
        )

    def drain_later(self, ref, send, recv):
        self.drain.append(self.waiter(ref, send, recv))

    def local(self, src, dst, again=False):
        self.locals += not again
        return pltpu.make_async_copy(src, dst, self.loc.at[self.locals - 1])


class Ring:
    def __init__(
        self, cp, plus, minus, own, put_plus, put_minus, near0, near1, far0, far1, block, three
    ):
        send = cp.new_send()
        self.first, self.second, self.third = (cp.new_recv() for _ in range(3))

        def group(srcs, dsts, dev, recv):
            return [cp.remote(s, d, dev, send, recv) for s, d in zip(srcs, dsts, strict=True)]

        self.out0 = group(own(0), put_plus(0), plus, self.first)
        self.out0 += group(own(1), put_minus(1), minus, self.first)
        self.out1 = group(own(1), put_plus(1), plus, self.second)
        self.out1 += group(own(0), put_minus(0), minus, self.second)
        self.on = group(near0, far0, plus, self.third) + group(near1, far1, minus, self.third)
        self.waits = [cp.waiter(block, send, r) for r in (self.first, self.second, self.third)]
        cp.drain_later(three, send, self.first)

    def start0(self):
        for c in self.out0:
            c.start()

    def start1(self):
        for c in self.out1:
            c.start()

    def start(self):
        self.start0()
        self.start1()

    def relay(self):
        self.waits[0].wait_recv()
        for c in self.on:
            c.start()

    def near(self):
        self.waits[1].wait_recv()

    def far(self):
        self.waits[2].wait_recv()


def slot_ring(cp, plus, minus, p, slots, block, three):
    up, down = lax.rem(p + 1, 4), lax.rem(p + 3, 4)
    at = lambda pos, h: [f(pos, h) for f in slots]
    own = lambda h: at(p, h)
    return Ring(
        cp, plus, minus, own, own, own, at(down, 0), at(up, 1), at(down, 0), at(up, 1), block, three
    )


def roll_lanes(x, shift):
    return pltpu.roll(x, shift % T, 1)


def kernel(
    ig_h, fg_h, doc_h, gain_h, ngain_h,
    q_h, k_h, v_h, og_h, wout_h, resid_h, wup_h, wdn_h,
    own_out, rs_in,
    ig_ref, fg_ref, doc_ref, gain_ref, ngain_ref,
    wu, wd, wox, wop, wa, wb, q, k, v, og, resid,
    arow, cols, numf, numb, dens,
    st_own, st_par, sc_pair, q_send, q_recv, sc_recv, cin,
    ro_out, ro_st, ro, mixed, nrm, hid, part, acc2, add_in,
    send_sem, recv_sem, loc_sem,
):
    z, y, c, x = (lax.axis_index(a) for a in ("z", "y", "c", "x"))
    other = 1 - c
    n = z * 4 + y
    n_up, n_dn = lax.rem(n + 1, 16), lax.rem(n + 15, 16)
    chip_up = {"z": lax.div(n_up, 4), "y": lax.rem(n_up, 4)}
    chip_dn = {"z": lax.div(n_dn, 4), "y": lax.rem(n_dn, 4)}
    partner = {"c": other}
    xp, xm, xf = lax.rem(x + 1, 4), lax.rem(x + 3, 4), lax.rem(x + 2, 4)
    cp = Copies(send_sem, recv_sem, loc_sem)
    stage = Stages()
    stage("loads")

    l_wd = cp.local(wdn_h, wa)
    l_wu = cp.local(wup_h, wu.at[z, y, c])
    l_wo = [cp.local(wout_h.at[pl.ds(WX * i, WX)], wox.at[0, i]) for i in range(2)]
    l_k = cp.local(k_h, k)
    l_v = cp.local(v_h, v)
    l_q = cp.local(q_h, q)
    l_og = cp.local(og_h, og)
    l_wp = [
        cp.local(
            wout_h.at[pl.ds(2 * WX + KP * i, KP), :, pl.ds(1024 * j + 256 * b, 256)],
            wop.at[j, 0, i, b],
            i + j + b > 0,
        )
        for i in range(4)
        for j in range(2)
        for b in range(4)
    ]
    l_wp_all = cp.local(wop.at[:, 0], wop.at[:, 0], True)
    l_re = cp.local(resid_h, resid)
    l_gate = [cp.local(a, b) for a, b in ((ig_h, ig_ref), (fg_h, fg_ref), (doc_h, doc_ref))]
    l_gain = [cp.local(gain_h, gain_ref), cp.local(ngain_h, ngain_ref)]
    loads = (l_wu, *l_gate, l_wd, *l_wo, l_k, l_v, l_q, l_og, *l_gain, *l_wp, l_re)

    stage("barrier")
    barrier = pltpu.get_barrier_semaphore()
    peers = (
        partner, {"y": lax.rem(y + 1, 4)}, {"y": lax.rem(y + 3, 4)}, {"z": lax.rem(z + 1, 4)},
        {"z": lax.rem(z + 3, 4)}, {"x": xp}, {"x": xm}, {"x": xf}, chip_up, chip_dn,
    )
    for dev in peers:
        pl.semaphore_signal(barrier, inc=1, device_id=dev, device_id_type=MESH)
    for l in loads:
        l.start()
    pl.semaphore_wait(barrier, len(peers))

    stage("first_sends")
    zp, zm, zf = lax.rem(z + 1, 4), lax.rem(z + 3, 4), lax.rem(z + 2, 4)
    yp, ym, yf = lax.rem(y + 1, 4), lax.rem(y + 3, 4), lax.rem(y + 2, 4)
    over_y, over_z = ({"y": yp}, {"y": ym}), ({"z": zp}, {"z": zm})
    up_half = lambda a, b, h: wu.at[a, b, c, pl.ds(32 * h, 32)]
    dn_half = lambda a, b, h: wd.at[a, b, c, pl.ds(512 * h, 512)]
    three = pl.ds(0, 3)
    a1 = slot_ring(
        cp, *over_y, y, [lambda p, h: up_half(z, p, h)], wu.at[z, y, c], wu.at[z, three, c]
    )
    a2o = slot_ring(
        cp, *over_z, z, [lambda p, h: up_half(p, y, h)], wu.at[z, y, c], wu.at[z, three, c]
    )
    a2 = slot_ring(
        cp, *over_z, z, [lambda p, h, o=o: up_half(p, o, h) for o in (yp, ym, yf)],
        wu.at[z, three, c], wu.at[three, three, c],
    )
    b1 = slot_ring(
        cp, *over_z, z, [lambda p, h: dn_half(p, y, h)], wd.at[z, y, c], wd.at[z, three, c]
    )
    b2o = slot_ring(
        cp, *over_y, y, [lambda p, h: dn_half(z, p, h)], wd.at[z, y, c], wd.at[z, three, c]
    )
    b2 = slot_ring(
        cp, *over_y, y, [lambda p, h, o=o: dn_half(o, p, h) for o in (zp, zm, zf)],
        wd.at[z, three, c], wd.at[three, three, c],
    )

    wx = lambda j, h: wox.at[j, c, pl.ds(WX // 2 * h, WX // 2)]
    wr = Ring(
        cp, {"x": xp}, {"x": xm},
        lambda h: [wx(0, h)], lambda h: [wx(3, h)], lambda h: [wx(1, h)],
        [wx(3, 0)], [wx(1, 1)], [wx(2, 0)], [wx(2, 1)], wox.at[0, c], wox.at[three, c],
    )
    a_pos, b_pos = jnp.where(c == 0, z, y), jnp.where(c == 0, y, z)
    cols_c = pl.ds(pl.multiple_of(1024 * c + 256 * b_pos, 256), 256)
    wp_send, wp_recv = cp.new_send(), cp.new_recv()
    wp = [
        cp.remote(
            wout_h.at[pl.ds(2 * WX + KP * a_pos, KP), :, cols_c], wop.at[c, j, a_pos, b_pos],
            {"x": to}, wp_send, wp_recv,
        )
        for to, j in ((xp, 3), (xm, 1), (xf, 2))
    ]
    wp_all = cp.waiter(wop.at[c, three, 0, 0], wp_send, wp_recv)
    cp.drain.append(wp_all)

    def dev_b(step):
        return {
            "z": jnp.where(c == 0, z, lax.rem(z + step, 4)),
            "y": jnp.where(c == 0, lax.rem(y + step, 4), y),
        }

    def dev_a(step):
        return {
            "z": jnp.where(c == 0, lax.rem(z + step, 4), z),
            "y": jnp.where(c == 0, y, lax.rem(y + step, 4)),
        }

    heads = pl.ds(1, 3)
    c1 = slot_ring(
        cp, dev_b(1), dev_b(3), b_pos,
        [lambda p, h: wop.at[c, heads, a_pos, p, :, :, pl.ds(128 * h, 128)]],
        wop.at[c, heads, 0, 0], wop.at[c, heads, 0, three],
    )
    c2 = slot_ring(
        cp, dev_a(1), dev_a(3), a_pos,
        [lambda p, h: wop.at[c, heads, p, :, :, :, pl.ds(128 * h, 128)]],
        wop.at[c, heads, 0], wop.at[c, heads, three],
    )

    for w in wp:
        w.start()
    l_wu.wait()
    a1.start0()
    a2o.start0()
    l_wd.wait()
    d_wd = cp.remote(wa.at[:, pl.ds(pl.multiple_of(1024 * other, 1024), 1024)], wb, partner)
    d_wd.start()
    for l in l_wo:
        l.wait()
    wr.start()

    stage("gates")
    for l in l_gate:
        l.wait()
    def row(ref, i):
        return jnp.broadcast_to(ref[i], (8, T))

    lane = lax.broadcasted_iota(jnp.int32, (8, T), 1)
    rowi = lax.broadcasted_iota(jnp.int32, (8, T), 0)
    doc = jnp.broadcast_to(doc_ref[...].astype(F32)[None, :], (8, T))

    def log_sigmoid(f):
        return jnp.minimum(f, 0.0) - jnp.log1p(jnp.exp(-jnp.abs(f)))

    cumf, cumb = log_sigmoid(row(fg_ref, 0)), log_sigmoid(row(fg_ref, 1))
    sh = 1
    while sh < T:
        cumf = cumf + jnp.where(lane >= sh, roll_lanes(cumf, sh), 0.0)
        cumb = cumb + jnp.where(lane < T - sh, roll_lanes(cumb, T - sh), 0.0)
        sh *= 2
    af, ab = row(ig_ref, 0) - cumf, row(ig_ref, 1) - cumb
    mf, mb = af, ab
    sh = 1
    while sh < T:
        same_f = (lane >= sh) & (roll_lanes(doc, sh) == doc)
        same_b = (lane < T - sh) & (roll_lanes(doc, T - sh) == doc)
        mf = jnp.where(same_f, jnp.maximum(mf, roll_lanes(mf, sh)), mf)
        mb = jnp.where(same_b, jnp.maximum(mb, roll_lanes(mb, T - sh)), mb)
        sh *= 2
    doc0, docl = doc[:, 0:1], doc[:, T - 1 : T]
    mxf, mxb = mf[:, T - 1 : T], mb[:, 0:1]
    totf, totb = cumf[:, T - 1 : T], cumb[:, 0:1]
    wf = jnp.where(doc == docl, jnp.exp(af - mxf), 0.0)
    wbk = jnp.where(doc == doc0, jnp.exp(ab - mxb), 0.0)
    arow[0] = af
    arow[1] = ab
    arow[2] = doc
    stack = jnp.where(
        rowi == 0, mf,
        jnp.where(rowi == 1, mb, jnp.where(rowi == 2, doc, jnp.where(rowi == 3, wf, wbk))),
    )
    cols[...] = stack.T
    r8 = lax.broadcasted_iota(jnp.int32, (8, 128), 0)
    scal = jnp.zeros((8, 128), F32)
    for i, val in enumerate((totf + mxf, totb + mxb, totf, totb, doc0, docl)):
        scal = jnp.where(r8 == i, jnp.broadcast_to(val, (8, 128)), scal)
    sc_pair[c] = scal
    d_sc = cp.remote(sc_pair.at[c], sc_pair.at[c], partner)
    d_sc.start()

    stage("state")
    l_k.wait()
    l_v.wait()
    keys = k[...].astype(F32)
    d_st = []
    st_send, q_sends, sc_sends, ro_send = (cp.new_send() for _ in range(4))
    for d in range(2):
        weighted = (keys * cols[:, 3 + d : 4 + d]).astype(BF16)
        st = lax.dot_general(
            v[...], weighted, (((0,), (0,)), ((), ())), preferred_element_type=F32
        ).astype(BF16)
        norm = jnp.sum(weighted.astype(F32), axis=0, keepdims=True)
        tail = jnp.broadcast_to(norm, (16, DK)).astype(BF16)
        for h in range(2):
            st_own[d, h, 0:256, :] = st[256 * h : 256 * h + 256]
            st_own[d, h, 256:SROWS, :] = tail
        d_st.append(cp.remote(st_own.at[d], st_par.at[d], partner, st_send))
        d_st[d].start()

    stage("wd_block")
    d_wd.wait_recv()
    ei = lax.broadcasted_iota(jnp.int32, (64, 128), 0)
    ej = lax.broadcasted_iota(jnp.int32, (64, 128), 1)
    put_own = jnp.where(ej == ei + 64 * c, 1.0, 0.0).astype(BF16)
    put_par = jnp.where(ej == ei + 64 * other, 1.0, 0.0).astype(BF16)
    mine = wa[:, pl.ds(pl.multiple_of(1024 * c, 1024), 1024)]
    tn = (((0,), (0,)), ((), ()))
    wd[z, y, c] = (
        lax.dot_general(mine, put_own, tn, preferred_element_type=F32)
        + lax.dot_general(wb[...], put_par, tn, preferred_element_type=F32)
    ).astype(BF16)
    b1.start0()

    stage("pair_wait")
    def pick(ref, i):
        return ref[i : i + 1, 0:1]

    def pair_terms(s0, s1, d):
        early, late = (s0, s1) if d == 0 else (s1, s0)
        e_last = early[5 - d : 6 - d, 0:1]
        l_first, l_last = late[4 + d : 5 + d, 0:1], late[5 - d : 6 - d, 0:1]
        linked = (l_first == e_last) & (l_first == l_last)
        e_top = early[d : d + 1, 0:1] + late[2 + d : 3 + d, 0:1]
        l_top = late[d : d + 1, 0:1]
        top = jnp.where(linked, jnp.maximum(l_top, e_top), l_top)
        f_early = jnp.where(linked, jnp.exp(jnp.minimum(e_top - top, 0.0)), 0.0)
        f_late = jnp.exp(l_top - top)
        total = early[2 + d : 3 + d, 0:1] + late[2 + d : 3 + d, 0:1]
        return top, total, f_early, f_late, l_last

    d_sc.wait_recv()
    s0, s1 = sc_pair[0], sc_pair[1]
    cq = []
    cs = []
    for d in range(2):
        pos = c if d == 0 else other
        _, _, f_early, f_late, _ = pair_terms(s0, s1, d)
        f_own = jnp.where(pos == 0, f_early, f_late)
        f_par = jnp.where(pos == 0, f_late, f_early)
        d_st[d].wait_recv()
        q_send[d] = (f_own * st_own[d, c].astype(F32) + f_par * st_par[d, c].astype(F32)).astype(BF16)
        to = chip_up if d == 0 else chip_dn
        cs.append(cp.remote(sc_pair, sc_recv.at[d, 0], to, sc_sends))
        cq.append(cp.remote(q_send.at[d], q_recv.at[d, 0, c], to, q_sends))
        cs[-1].start()
        cq[-1].start()

    stage("intra0")
    l_q.wait()

    def intra(r0, size):
        qb = q[r0 : r0 + size, :]
        mfc, mbc, dc = (cols[r0 : r0 + size, i : i + 1] for i in range(3))
        score = (
            lax.dot_general(qb, k[...], (((1,), (1,)), ((), ())), preferred_element_type=F32)
            * SCALE
        )
        for d in range(2):
            lo, hi = (0, r0 + size) if d == 0 else (r0, T)
            ti = r0 + lax.broadcasted_iota(jnp.int32, (size, hi - lo), 0)
            si = lo + lax.broadcasted_iota(jnp.int32, (size, hi - lo), 1)
            keep = ((si <= ti) if d == 0 else (si >= ti)) & (arow[2, 0:1, lo:hi] == dc)
            e = jnp.exp(jnp.minimum(arow[d, 0:1, lo:hi] - (mfc if d == 0 else mbc), 0.0))
            w = jnp.where(keep, score[:, lo:hi] * e, 0.0)
            dens[r0 : r0 + size, d : d + 1] = jnp.sum(w, axis=1, keepdims=True)
            num = jnp.dot(w.astype(BF16), v[lo:hi, :], preferred_element_type=F32)
            (numf if d == 0 else numb)[r0 : r0 + size, :] = num

    intra(0, 256)
    stage("pieces")
    wp_all.wait_recv()
    c1.start()
    b1.start1()
    stage("intra1")
    intra(256, 256)
    stage("intra2")
    intra(512, 256)

    stage("c1_relay")
    c1.relay()
    stage("carry_near")
    rq, rs, dq, dq_recv = [], [], [], cp.new_recv()
    for d in range(2):
        to = chip_up if d == 0 else chip_dn
        rs.append(cp.remote(sc_recv.at[d, 0], sc_recv.at[d, 1], to, sc_sends))
        rq.append(cp.remote(q_recv.at[d, 0, c], q_recv.at[d, 1, c], to, q_sends))
        dq.append(cp.remote(q_recv.at[d, 0, c], q_recv.at[d, 0, c], partner, q_sends, dq_recv))
        cs[d].wait_recv()
        rs[d].start()
        cq[d].wait_recv()
        rq[d].start()
        dq[d].start()
    stage("b1_relay")
    b1.relay()
    stage("wr_relay")
    wr.relay()
    stage("c1_wait")
    c1.near()
    c1.far()
    c2.start()
    a1.start1()
    a1.relay()
    fo_send, fo_recv = cp.new_send(), cp.new_recv()
    cp.remote(
        wop.at[c, heads, a_pos], wop.at[c, heads, a_pos], partner, fo_send, fo_recv
    ).start()

    stage("carry_far")
    dq2 = []
    for d in range(2):
        rs[d].wait_recv()
        rq[d].wait_recv()
        dq2.append(cp.remote(q_recv.at[d, 1, c], q_recv.at[d, 1, c], partner, q_sends, dq_recv))
        dq2[d].start()
    fw_send = cp.new_send()
    fw_up, fw_up2, fw_dn, fw_dn2 = (cp.new_recv() for _ in range(4))

    def forward(refs, recv, send=fw_send):
        for r in refs:
            cp.remote(r, r, partner, send, recv).start()

    def second_phase():
        stage("c2_relay")
        c2.relay()
        a2o.start1()
        b2o.start()
        a2o.relay()
        wr.near()
        forward([wox.at[j, c] for j in (1, 3)], fo_recv, fo_send)
        stage("emit_rest")

    stage("carry_combine")
    scal_in = []
    for d in range(2):
        pos = c if d == 0 else other
        chip = n if d == 0 else 15 - n
        own_s = sc_pair[c]
        par_s = sc_pair[other]
        first = own_s[4 + d : 5 + d, 0:1]
        t1, tot1, _, _, last1 = pair_terms(sc_recv[d, 0, 0], sc_recv[d, 0, 1], d)
        t2, _, _, _, last2 = pair_terms(sc_recv[d, 1, 0], sc_recv[d, 1, 1], d)
        l0 = (par_s[5 - d : 6 - d, 0:1] == first) & (pos == 1)
        l1 = (last1 == first) & (chip >= 1)
        l2 = (last2 == first) & (chip >= 2)
        shift = jnp.where(pos == 1, par_s[2 + d : 3 + d, 0:1], 0.0)
        e0 = jnp.where(l0, par_s[d : d + 1, 0:1], FAR_LOW)
        e1 = jnp.where(l1, t1 + shift, FAR_LOW)
        e2 = jnp.where(l2, t2 + tot1 + shift, FAR_LOW)
        top = jnp.maximum(e0, jnp.maximum(e1, e2))
        g0 = jnp.where(l0, jnp.exp(e0 - top), 0.0)
        g1 = jnp.where(l1, jnp.exp(e1 - top), 0.0)
        g2 = jnp.where(l2, jnp.exp(e2 - top), 0.0)
        late = jnp.where(pos == 1, 1.0, 0.0)
        linked = late * jnp.where(l0, 1.0, 0.0) + (1.0 - late) * jnp.where(l1, 1.0, 0.0)
        if d == 0:
            cp.waiter(q_recv.at[:, :, 0], q_sends, dq_recv).wait_recv()
        for h in range(2):
            cin[d, h] = (
                g0 * st_par[d, h].astype(F32)
                + g1 * q_recv[d, 0, h].astype(F32)
                + g2 * q_recv[d, 1, h].astype(F32)
            ).astype(BF16)
        scal_in.append((top, linked, first))

    stage("emit")
    for l in (l_og, *l_gain):
        l.wait()
    ca = []
    lo, hi = pl.ds(0, HALF), pl.ds(HALF, HALF)
    for step, to in enumerate((xf, xp, xm, x)):
        r0 = pl.multiple_of(to * ROWS, 64)
        rows = pl.ds(r0, ROWS)
        qb = q[rows, :]
        qw = qb.astype(F32)
        dc = cols[rows, 2:3]
        memory = None
        for d in range(2):
            top, linked, first = scal_in[d]
            m_loc = cols[rows, d : d + 1]
            usable = jnp.where(dc == first, linked, 0.0) > 0.5
            m = jnp.where(usable, jnp.maximum(m_loc, top), m_loc)
            keep = jnp.exp(m_loc - m)
            inter = jnp.where(usable, jnp.exp(jnp.minimum(top - m, 0.0)), 0.0) * SCALE
            nt = (((1,), (1,)), ((), ()))
            qc = jnp.concatenate(
                [
                    lax.dot_general(qb, cin[d, h, 0:256, :], nt, preferred_element_type=F32)
                    for h in range(2)
                ],
                axis=1,
            )
            norm = cin[d, 0, 256:257, :].astype(F32)
            num = keep * (numf if d == 0 else numb)[rows, :] + inter * qc
            den = keep * dens[rows, d : d + 1] + inter * jnp.sum(qw * norm, axis=1, keepdims=True)
            h_dir = num / jnp.maximum(jnp.abs(den), 1.0)
            memory = h_dir if memory is None else memory + h_dir
        normed = memory * lax.rsqrt(jnp.mean(memory * memory, axis=1, keepdims=True) + EPS)
        gate = 1.0 / (1.0 + jnp.exp(-og[rows, :].astype(F32)))
        readout = (normed * gain_ref[...] * gate).astype(BF16)
        if step == 3:
            ro[x] = readout
        else:
            ro_out[step] = readout
        if step == 0:
            ca0 = [
                cp.remote(ro_out.at[0, lo], ro_st.at[0], {"x": xp}, ro_send),
                cp.remote(ro_out.at[0, hi], ro_st.at[1], {"x": xm}, ro_send),
            ]
            for cc in ca0:
                cc.start()
        elif step < 3:
            ca.append(cp.remote(ro_out.at[step], ro.at[x], {"x": to}, ro_send))
            ca[-1].start()
            if step == 1:
                second_phase()
    stage("a1_wait")
    b1.near()
    b1.far()
    b2.start()
    a1.near()
    a1.far()
    a2.start()
    stage("a2a_relay")
    ca += [
        cp.remote(ro_st.at[0], ro.at[xm, lo], {"x": xp}, ro_send),
        cp.remote(ro_st.at[1], ro.at[xp, hi], {"x": xm}, ro_send),
    ]
    for i in range(2):
        ca0[i].wait_recv()
        ca[2 + i].start()

    stage("wout_fwd")
    c2.near()
    forward([wop.at[c, heads, lax.rem(a_pos + i, 4)] for i in (1, 3)], fo_recv, fo_send)
    wr.far()
    forward([wox.at[2, c]], fo_recv, fo_send)
    stage("c2_far")
    c2.far()
    forward([wop.at[c, heads, lax.rem(a_pos + 2, 4)]], fo_recv, fo_send)
    b2o.relay()
    stage("a2a_wait")
    l_re.wait()
    l_wp_all.wait()
    stage("wout")

    def project(j):
        head = ro.at[lax.rem(x + j, 4)]
        base = resid if j == 0 else mixed
        for t in range(4):
            cs_ = slice(512 * t, 512 * t + 512)
            w0 = wox[j, :, :, :, cs_].reshape(512 - 64 * KP, 512)
            at = [wop[t // 2, j, :, 2 * (t % 2) + i].reshape(64 * KP, 256) for i in range(2)]
            one = jnp.dot(head[:, 0 : 512 - 64 * KP], w0, preferred_element_type=F32) + jnp.dot(
                head[:, 512 - 64 * KP : 512],
                jnp.concatenate(at, axis=1),
                preferred_element_type=F32,
            )
            mixed[:, cs_] = base[:, cs_].astype(F32) + one.astype(BF16).astype(F32)

    project(0)
    stage("fo_wait")
    fo_all = cp.waiter(nrm, fo_send, fo_recv)
    fo_all.wait_recv()
    cp.drain.append(fo_all)
    stage("near_wait")
    ca[0].wait_recv()
    project(3)
    ca[1].wait_recv()
    project(1)
    stage("far_wait")
    ca[2].wait_recv()
    ca[3].wait_recv()
    stage("far_project")
    project(2)

    mx = mixed[...]
    factor = lax.rsqrt(jnp.mean(mx * mx, axis=1, keepdims=True) + EPS)
    nrm[0] = (mx * factor * ngain_ref[...]).astype(BF16)

    h01 = lambda j, h: nrm.at[j, pl.ds(HALF * h, HALF)]
    ag = Ring(
        cp, {"x": xp}, {"x": xm},
        lambda h: [h01(0, h)],
        lambda h: [h01(1 + h, 0)],
        lambda h: [h01(2 - h, 1)],
        [h01(1, 0)], [h01(1, 1)], [h01(3, 0)], [h01(3, 1)], nrm.at[0], nrm.at[three],
    )
    ag.start()
    up_most = cp.waiter(wu.at[three, :, 0], fw_send, fw_up)
    up_last = cp.waiter(wu.at[0, :, 0], fw_send, fw_up2)
    dn_most = cp.waiter(wd.at[three, :, 0], fw_send, fw_dn)
    dn_last = cp.waiter(wd.at[0, :, 0], fw_send, fw_dn2)
    cp.drain_later(wu, fw_send, fw_up)

    def up(j, zs, start=None, final=True):
        @pl.loop(0, 4)
        def _(t):
            cs_ = pl.ds(pl.multiple_of(t * 512, 512), 512)
            if zs is None:
                pre = jnp.dot(
                    nrm[j], wu[:, :, :, :, cs_].reshape(D, 512), preferred_element_type=F32
                )
            else:
                pre = start[:, cs_] if start is not None else None
                for zz in zs:
                    one = jnp.dot(
                        nrm[j, :, pl.ds(pl.multiple_of(512 * zz, 512), 512)],
                        wu[zz, :, :, :, cs_].reshape(512, 512),
                        preferred_element_type=F32,
                    )
                    pre = one if pre is None else pre + one
            if final:
                pre = jnp.maximum(pre, 0.0)
                hid[j, :, cs_] = (pre * pre).astype(BF16)
            else:
                acc2[:, cs_] = pre

    def down(j, first, last, sink):
        @pl.loop(first, last)
        def _(t):
            cs_ = pl.ds(pl.multiple_of(t * 512, 512), 512)
            w = jnp.concatenate([wd[t, i].reshape(D, 128) for i in range(4)], axis=1)
            sink(cs_, jnp.dot(hid[j], w, preferred_element_type=F32))

    def add_own(cs_, val):
        mixed[:, cs_] += val

    def to_part(j):
        def sink(cs_, val):
            part[j, :, cs_] = val.astype(BF16)

        return sink

    def to_acc(cs_, val):
        acc2[:, cs_] = val

    rs_send, rs_recv = cp.new_send(), cp.new_recv()
    cp.drain_later(nrm.at[three], rs_send, rs_recv)

    def first_sums(yy):
        w = jnp.concatenate([wd[i, yy].reshape(D, 128) for i in range(4)], axis=1)
        val = jnp.dot(hid[1], w, preferred_element_type=F32).astype(BF16)
        for i in range(4):
            strip = pl.ds(pl.multiple_of((4 * i + yy) * 128, 128), 128)
            part[0, :, strip] = val[:, 128 * i : 128 * i + 128]
        for i in range(4):
            strip = pl.ds(pl.multiple_of((4 * i + yy) * 128, 128), 128)
            for rows, side, to in ((hi, 0, xp), (lo, 1, xm)):
                cp.remote(
                    part.at[0, rows, strip], rs_in.at[side, rows, strip], {"x": to}, rs_send, rs_recv
                ).start()

    up_other, dn_other = (yp, ym, yf), (zp, zm, zf)
    lower, upper = [pl.ds(32 * h, 32) for h in range(2)], [pl.ds(512 * h, 512) for h in range(2)]

    def up_part(row, h):
        return [wu.at[row, o, c, lower[h]] for o in up_other]

    def dn_part(col, h):
        return [wd.at[o, col, c, upper[h]] for o in dn_other]

    stage("own_rows")
    forward([wu.at[z, :, c]], fw_up)
    forward([wd.at[:, y, c]], fw_dn)
    a2o.near()
    a2o.far()
    forward([wu.at[zp, y, c], wu.at[zm, y, c]], fw_up)
    forward([wu.at[zf, y, c]], fw_up2)
    stage("a2_relay")
    a2.relay()
    forward(up_part(zm, 0) + up_part(zp, 1), fw_up)
    stage("b2_relay")
    b2o.near()
    b2.relay()
    forward([wd.at[z, yp, c], wd.at[z, ym, c]], fw_dn)
    forward(dn_part(ym, 0) + dn_part(yp, 1), fw_dn)
    stage("a2_near")
    a2.near()
    forward(up_part(zm, 1) + up_part(zp, 0), fw_up)
    stage("b2_near")
    b2.near()
    forward(dn_part(ym, 1) + dn_part(yp, 0), fw_dn)
    stage("ag_relay")
    ag.relay()
    stage("up1_most")
    up_most.wait_recv()
    up(1, (z, zp, zm), final=False)
    stage("a2_far")
    a2.far()
    forward(up_part(zf, 0) + up_part(zf, 1), fw_up2)
    up_last.wait_recv()
    stage("up1_last")
    up(1, (zf,), start=acc2)
    stage("down1_most")
    dn_most.wait_recv()
    for yy in (y, yp, ym):
        first_sums(yy)
    stage("b2_far")
    b2o.far()
    b2.far()
    forward([wd.at[:, yf, c]], fw_dn2)
    stage("ag_far")
    ag.far()
    stage("up3")
    up(3, None)
    stage("down1_last")
    dn_last.wait_recv()
    first_sums(yf)
    stage("down3")
    rs2, rs3 = [], []
    for i in range(2):
        down(3, 2 * i, 2 * i + 2, to_part(1))
        wide = pl.ds(1024 * i, 1024)
        rs2.append(cp.remote(part.at[1, lo, wide], add_in.at[0, :, wide], {"x": xp}, rs_send))
        rs2.append(cp.remote(part.at[1, hi, wide], add_in.at[1, :, wide], {"x": xm}, rs_send))
        for part_rows, side, to in ((hi, 0, xp), (lo, 1, xm)):
            rs_rows = lo if side == 0 else hi
            rs3.append(
                cp.remote(
                    part.at[2, part_rows, wide], rs_in.at[side, rs_rows, wide], {"x": to},
                    rs_send, rs_recv,
                )
            )
        rs2[-2].start()
        rs2[-1].start()
    stage("ff2")
    ag.near()
    up(2, None)
    down(2, 0, 4, to_acc)
    for i in range(2):
        stage(f"rs_add{i}")
        lanes = slice(1024 * i, 1024 * i + 1024)
        for side in range(2):
            rs2[2 * i + side].wait_recv()
            rows = slice(HALF, ROWS) if side == 0 else slice(0, HALF)
            part[2, rows, lanes] = (
                acc2[rows, lanes] + add_in[side, :, lanes].astype(F32)
            ).astype(BF16)
            rs3[2 * i + side].start()
    stage("up0")
    up(0, None)
    stage("down0")
    down(0, 0, 4, add_own)
    l_mx = cp.local(mixed, own_out)
    l_mx.start()
    stage("rs_wait")
    cp.waiter(rs_in, rs_send, rs_recv).wait_recv()
    cp.drain_later(st_own, st_send, rs_recv)
    cp.drain_later(q_recv, q_sends, rs_recv)
    cp.drain_later(sc_recv, sc_sends, rs_recv)
    cp.drain_later(ro, ro_send, rs_recv)
    l_mx.wait()
    stage("drain")
    assert (cp.sends, cp.recvs, cp.locals) == N_SEMS, (cp.sends, cp.recvs, cp.locals)
    for r in cp.drain:
        r.wait_send()
    stage()


def shards(
    queries, keys, values, out_gate, input_gates, forget_gates, doc_ids,
    head_gain, w_out, resid, norm_gain, w_up, w_down,
):
    hbm = pl.BlockSpec(memory_space=pl.ANY)
    own, sums = pl.pallas_call(
        kernel,
        out_shape=(
            jax.ShapeDtypeStruct((ROWS, D), F32),
            jax.ShapeDtypeStruct((2, ROWS, D), BF16),
        ),
        in_specs=[hbm] * 13,
        out_specs=(hbm, hbm),
        scratch_shapes=[
            pltpu.VMEM((2, 1, T), F32),
            pltpu.VMEM((2, 1, T), F32),
            pltpu.VMEM((T,), jnp.int32),
            pltpu.VMEM((1, DV), F32),
            pltpu.VMEM((1, D), F32),
            pltpu.VMEM((4, 4, 2, 64, D), BF16),
            pltpu.VMEM((4, 4, 2, 1024, 128), BF16),
            pltpu.VMEM((4, 2, WX, 16, D), BF16),
            pltpu.VMEM((2, 4, 4, 4, KP, 16, 256), BF16),
            pltpu.VMEM((64, D), BF16),
            pltpu.VMEM((64, 1024), BF16),
            pltpu.VMEM((T, DK), BF16),
            pltpu.VMEM((T, DK), BF16),
            pltpu.VMEM((T, DV), BF16),
            pltpu.VMEM((T, DV), BF16),
            pltpu.VMEM((ROWS, D), BF16),
            pltpu.VMEM((3, 8, T), F32),
            pltpu.VMEM((T, 8), F32),
            pltpu.VMEM((T, DV), F32),
            pltpu.VMEM((T, DV), F32),
            pltpu.VMEM((T, 8), F32),
            pltpu.VMEM((2, 2, SROWS, DK), BF16),
            pltpu.VMEM((2, 2, SROWS, DK), BF16),
            pltpu.VMEM((2, 8, 128), F32),
            pltpu.VMEM((2, SROWS, DK), BF16),
            pltpu.VMEM((2, 2, 2, SROWS, DK), BF16),
            pltpu.VMEM((2, 2, 2, 8, 128), F32),
            pltpu.VMEM((2, 2, SROWS, DK), BF16),
            pltpu.VMEM((3, ROWS, DV), BF16),
            pltpu.VMEM((2, HALF, DV), BF16),
            pltpu.VMEM((4, ROWS, DV), BF16),
            pltpu.VMEM((ROWS, D), F32),
            pltpu.VMEM((4, ROWS, D), BF16),
            pltpu.VMEM((4, ROWS, D), BF16),
            pltpu.VMEM((3, ROWS, D), BF16),
            pltpu.VMEM((ROWS, D), F32),
            pltpu.VMEM((2, HALF, D), BF16),
            *(pltpu.SemaphoreType.DMA((k,)) for k in N_SEMS),
        ],
        compiler_params=pltpu.CompilerParams(
            collective_id=0, has_side_effects=True, vmem_limit_bytes=66 * 1024 * 1000
        ),
        name="layer",
    )(
        input_gates, forget_gates, doc_ids, head_gain.reshape(1, DV),
        norm_gain.reshape(1, D), queries, keys, values, out_gate, w_out.reshape(32, 16, D), resid, w_up,
        w_down.T,
    )
    return (own + sums[0].astype(F32) + sums[1].astype(F32)).astype(BF16)


def solution(mesh):
    split = Mesh(mesh.devices.reshape(4, 4, 2, mesh.shape["tp"]), ("z", "y", "c", "x"))
    sp = ("z", "y", "c")
    return jax.shard_map(
        shards,
        mesh=split,
        in_specs=(
            P(sp, "x"), P(sp, "x"), P(sp, "x"), P(sp, "x"),
            P(None, "x", sp), P(None, "x", sp), P(sp), P("x"), P("x", None),
            P((*sp, "x"), None), P(), P(sp, "x"), P("x", sp),
        ),
        out_specs=P((*sp, "x"), None),
        check_vma=False,
    )
```

```python
import contextlib

import jax
import jax.numpy as jnp
from jax import lax
from jax.experimental import pallas as pl
from jax.experimental.pallas import tpu as pltpu
from jax.sharding import Mesh
from jax.sharding import PartitionSpec as P

MESH = pl.DeviceIdType.MESH
F32 = jnp.float32
BF16 = jnp.bfloat16
EPS = 1e-06
FAR_LOW = -1e30

T = 768
ROWS = 192
HALF = 96
DK = 256
DV = 512
D = 2048
SROWS = 272
SCALE = DK ** (-0.5)
KP = 3
WX = 16 - 2 * KP
N_SEMS = (20, 60, 16)


class Stages:
    def __init__(self):
        self.scopes = contextlib.ExitStack()

    def __call__(self, name=None):
        self.scopes.close()
        if name:
            self.scopes.enter_context(jax.named_scope(name))


class Copies:
    def __init__(self, send, recv, loc):
        self.send, self.recv, self.loc = send, recv, loc
        self.sends = self.recvs = self.locals = 0
        self.drain = []

    def new_send(self):
        self.sends += 1
        return self.send.at[self.sends - 1]

    def new_recv(self):
        self.recvs += 1
        return self.recv.at[self.recvs - 1]

    def remote(self, src, dst, dev, send=None, recv=None):
        alone = send is None
        c = pltpu.make_async_remote_copy(
            src_ref=src,
            dst_ref=dst,
            send_sem=self.new_send() if alone else send,
            recv_sem=self.new_recv() if recv is None else recv,
            device_id=dev,
            device_id_type=MESH,
        )
        if alone:
            self.drain.append(c)
        return c

    def waiter(self, ref, send, recv):
        return pltpu.make_async_remote_copy(
            src_ref=ref,
            dst_ref=ref,
            send_sem=send,
            recv_sem=recv,
            device_id={"c": 1 - lax.axis_index("c")},
            device_id_type=MESH,
        )

    def drain_later(self, ref, send, recv):
        self.drain.append(self.waiter(ref, send, recv))

    def local(self, src, dst, again=False):
        self.locals += not again
        return pltpu.make_async_copy(src, dst, self.loc.at[self.locals - 1])


class Ring:
    def __init__(
        self, cp, plus, minus, own, put_plus, put_minus, near0, near1, far0, far1, block, three
    ):
        send = cp.new_send()
        self.first, self.second, self.third = (cp.new_recv() for _ in range(3))

        def group(srcs, dsts, dev, recv):
            return [cp.remote(s, d, dev, send, recv) for s, d in zip(srcs, dsts, strict=True)]

        self.out0 = group(own(0), put_plus(0), plus, self.first)
        self.out0 += group(own(1), put_minus(1), minus, self.first)
        self.out1 = group(own(1), put_plus(1), plus, self.second)
        self.out1 += group(own(0), put_minus(0), minus, self.second)
        self.on = group(near0, far0, plus, self.third) + group(near1, far1, minus, self.third)
        self.waits = [cp.waiter(block, send, r) for r in (self.first, self.second, self.third)]
        cp.drain_later(three, send, self.first)

    def start0(self):
        for c in self.out0:
            c.start()

    def start1(self):
        for c in self.out1:
            c.start()

    def start(self):
        self.start0()
        self.start1()

    def relay(self):
        self.waits[0].wait_recv()
        for c in self.on:
            c.start()

    def near(self):
        self.waits[1].wait_recv()

    def far(self):
        self.waits[2].wait_recv()


def slot_ring(cp, plus, minus, p, slots, block, three):
    up, down = lax.rem(p + 1, 4), lax.rem(p + 3, 4)
    at = lambda pos, h: [f(pos, h) for f in slots]
    own = lambda h: at(p, h)
    return Ring(
        cp, plus, minus, own, own, own, at(down, 0), at(up, 1), at(down, 0), at(up, 1), block, three
    )


def roll_lanes(x, shift):
    return pltpu.roll(x, shift % T, 1)


def kernel(
    ig_h, fg_h, doc_h, gain_h, ngain_h,
    q_h, k_h, v_h, og_h, wout_h, resid_h, wup_h, wdn_h,
    own_out, rs_in,
    ig_ref, fg_ref, doc_ref, gain_ref, ngain_ref,
    wu, wd, wox, wop, wa, wb, q, k, v, og, resid,
    arow, cols, numf, numb, dens,
    st_own, st_par, sc_pair, q_send, q_recv, sc_recv, cin,
    ro_out, ro_st, ro, mixed, nrm, hid, part, acc2, add_in,
    send_sem, recv_sem, loc_sem,
):
    z, y, c, x = (lax.axis_index(a) for a in ("z", "y", "c", "x"))
    other = 1 - c
    n = z * 4 + y
    n_up, n_dn = lax.rem(n + 1, 16), lax.rem(n + 15, 16)
    chip_up = {"z": lax.div(n_up, 4), "y": lax.rem(n_up, 4)}
    chip_dn = {"z": lax.div(n_dn, 4), "y": lax.rem(n_dn, 4)}
    partner = {"c": other}
    xp, xm, xf = lax.rem(x + 1, 4), lax.rem(x + 3, 4), lax.rem(x + 2, 4)
    cp = Copies(send_sem, recv_sem, loc_sem)
    stage = Stages()
    stage("loads")

    l_wd = cp.local(wdn_h, wa)
    l_wu = cp.local(wup_h, wu.at[z, y, c])
    l_wo = [cp.local(wout_h.at[pl.ds(WX * i, WX)], wox.at[0, i]) for i in range(2)]
    l_k = cp.local(k_h, k)
    l_v = cp.local(v_h, v)
    l_q = cp.local(q_h, q)
    l_og = cp.local(og_h, og)
    l_wp = [
        cp.local(
            wout_h.at[pl.ds(2 * WX + KP * i, KP), :, pl.ds(1024 * j + 256 * b, 256)],
            wop.at[j, 0, i, b],
            i + j + b > 0,
        )
        for i in range(4)
        for j in range(2)
        for b in range(4)
    ]
    l_wp_all = cp.local(wop.at[:, 0], wop.at[:, 0], True)
    l_re = cp.local(resid_h, resid)
    l_gate = [cp.local(a, b) for a, b in ((ig_h, ig_ref), (fg_h, fg_ref), (doc_h, doc_ref))]
    l_gain = [cp.local(gain_h, gain_ref), cp.local(ngain_h, ngain_ref)]
    loads = (l_wu, *l_gate, l_wd, *l_wo, l_k, l_v, l_q, l_og, *l_gain, *l_wp, l_re)

    stage("barrier")
    barrier = pltpu.get_barrier_semaphore()
    peers = (
        partner, {"y": lax.rem(y + 1, 4)}, {"y": lax.rem(y + 3, 4)}, {"z": lax.rem(z + 1, 4)},
        {"z": lax.rem(z + 3, 4)}, {"x": xp}, {"x": xm}, {"x": xf}, chip_up, chip_dn,
    )
    for dev in peers:
        pl.semaphore_signal(barrier, inc=1, device_id=dev, device_id_type=MESH)
    for l in loads:
        l.start()
    pl.semaphore_wait(barrier, len(peers))

    stage("first_sends")
    zp, zm, zf = lax.rem(z + 1, 4), lax.rem(z + 3, 4), lax.rem(z + 2, 4)
    yp, ym, yf = lax.rem(y + 1, 4), lax.rem(y + 3, 4), lax.rem(y + 2, 4)
    over_y, over_z = ({"y": yp}, {"y": ym}), ({"z": zp}, {"z": zm})
    up_half = lambda a, b, h: wu.at[a, b, c, pl.ds(32 * h, 32)]
    dn_half = lambda a, b, h: wd.at[a, b, c, pl.ds(512 * h, 512)]
    three = pl.ds(0, 3)
    a1 = slot_ring(
        cp, *over_y, y, [lambda p, h: up_half(z, p, h)], wu.at[z, y, c], wu.at[z, three, c]
    )
    a2o = slot_ring(
        cp, *over_z, z, [lambda p, h: up_half(p, y, h)], wu.at[z, y, c], wu.at[z, three, c]
    )
    a2 = slot_ring(
        cp, *over_z, z, [lambda p, h, o=o: up_half(p, o, h) for o in (yp, ym, yf)],
        wu.at[z, three, c], wu.at[three, three, c],
    )
    b1 = slot_ring(
        cp, *over_z, z, [lambda p, h: dn_half(p, y, h)], wd.at[z, y, c], wd.at[z, three, c]
    )
    b2o = slot_ring(
        cp, *over_y, y, [lambda p, h: dn_half(z, p, h)], wd.at[z, y, c], wd.at[z, three, c]
    )
    b2 = slot_ring(
        cp, *over_y, y, [lambda p, h, o=o: dn_half(o, p, h) for o in (zp, zm, zf)],
        wd.at[z, three, c], wd.at[three, three, c],
    )

    wx = lambda j, h: wox.at[j, c, pl.ds(WX // 2 * h, WX // 2)]
    wr = Ring(
        cp, {"x": xp}, {"x": xm},
        lambda h: [wx(0, h)], lambda h: [wx(3, h)], lambda h: [wx(1, h)],
        [wx(3, 0)], [wx(1, 1)], [wx(2, 0)], [wx(2, 1)], wox.at[0, c], wox.at[three, c],
    )
    a_pos, b_pos = jnp.where(c == 0, z, y), jnp.where(c == 0, y, z)
    cols_c = pl.ds(pl.multiple_of(1024 * c + 256 * b_pos, 256), 256)
    wp_send, wp_recv = cp.new_send(), cp.new_recv()
    wp = [
        cp.remote(
            wout_h.at[pl.ds(2 * WX + KP * a_pos, KP), :, cols_c], wop.at[c, j, a_pos, b_pos],
            {"x": to}, wp_send, wp_recv,
        )
        for to, j in ((xp, 3), (xm, 1), (xf, 2))
    ]
    wp_all = cp.waiter(wop.at[c, three, 0, 0], wp_send, wp_recv)
    cp.drain.append(wp_all)

    def dev_b(step):
        return {
            "z": jnp.where(c == 0, z, lax.rem(z + step, 4)),
            "y": jnp.where(c == 0, lax.rem(y + step, 4), y),
        }

    def dev_a(step):
        return {
            "z": jnp.where(c == 0, lax.rem(z + step, 4), z),
            "y": jnp.where(c == 0, y, lax.rem(y + step, 4)),
        }

    heads = pl.ds(1, 3)
    c1 = slot_ring(
        cp, dev_b(1), dev_b(3), b_pos,
        [lambda p, h: wop.at[c, heads, a_pos, p, :, :, pl.ds(128 * h, 128)]],
        wop.at[c, heads, 0, 0], wop.at[c, heads, 0, three],
    )
    c2 = slot_ring(
        cp, dev_a(1), dev_a(3), a_pos,
        [lambda p, h: wop.at[c, heads, p, :, :, :, pl.ds(128 * h, 128)]],
        wop.at[c, heads, 0], wop.at[c, heads, three],
    )

    for w in wp:
        w.start()
    l_wu.wait()
    a1.start0()
    a2o.start0()
    l_wd.wait()
    d_wd = cp.remote(wa.at[:, pl.ds(pl.multiple_of(1024 * other, 1024), 1024)], wb, partner)
    d_wd.start()
    for l in l_wo:
        l.wait()
    wr.start()

    stage("gates")
    for l in l_gate:
        l.wait()
    def row(ref, i):
        return jnp.broadcast_to(ref[i], (8, T))

    lane = lax.broadcasted_iota(jnp.int32, (8, T), 1)
    rowi = lax.broadcasted_iota(jnp.int32, (8, T), 0)
    doc = jnp.broadcast_to(doc_ref[...].astype(F32)[None, :], (8, T))

    def log_sigmoid(f):
        return jnp.minimum(f, 0.0) - jnp.log1p(jnp.exp(-jnp.abs(f)))

    cumf, cumb = log_sigmoid(row(fg_ref, 0)), log_sigmoid(row(fg_ref, 1))
    sh = 1
    while sh < T:
        cumf = cumf + jnp.where(lane >= sh, roll_lanes(cumf, sh), 0.0)
        cumb = cumb + jnp.where(lane < T - sh, roll_lanes(cumb, T - sh), 0.0)
        sh *= 2
    af, ab = row(ig_ref, 0) - cumf, row(ig_ref, 1) - cumb
    mf, mb = af, ab
    sh = 1
    while sh < T:
        same_f = (lane >= sh) & (roll_lanes(doc, sh) == doc)
        same_b = (lane < T - sh) & (roll_lanes(doc, T - sh) == doc)
        mf = jnp.where(same_f, jnp.maximum(mf, roll_lanes(mf, sh)), mf)
        mb = jnp.where(same_b, jnp.maximum(mb, roll_lanes(mb, T - sh)), mb)
        sh *= 2
    doc0, docl = doc[:, 0:1], doc[:, T - 1 : T]
    mxf, mxb = mf[:, T - 1 : T], mb[:, 0:1]
    totf, totb = cumf[:, T - 1 : T], cumb[:, 0:1]
    wf = jnp.where(doc == docl, jnp.exp(af - mxf), 0.0)
    wbk = jnp.where(doc == doc0, jnp.exp(ab - mxb), 0.0)
    arow[0] = af
    arow[1] = ab
    arow[2] = doc
    stack = jnp.where(
        rowi == 0, mf,
        jnp.where(rowi == 1, mb, jnp.where(rowi == 2, doc, jnp.where(rowi == 3, wf, wbk))),
    )
    cols[...] = stack.T
    r8 = lax.broadcasted_iota(jnp.int32, (8, 128), 0)
    scal = jnp.zeros((8, 128), F32)
    for i, val in enumerate((totf + mxf, totb + mxb, totf, totb, doc0, docl)):
        scal = jnp.where(r8 == i, jnp.broadcast_to(val, (8, 128)), scal)
    sc_pair[c] = scal
    d_sc = cp.remote(sc_pair.at[c], sc_pair.at[c], partner)
    d_sc.start()

    stage("state")
    l_k.wait()
    l_v.wait()
    keys = k[...].astype(F32)
    d_st = []
    st_send, q_sends, sc_sends, ro_send = (cp.new_send() for _ in range(4))
    for d in range(2):
        weighted = (keys * cols[:, 3 + d : 4 + d]).astype(BF16)
        st = lax.dot_general(
            v[...], weighted, (((0,), (0,)), ((), ())), preferred_element_type=F32
        ).astype(BF16)
        norm = jnp.sum(weighted.astype(F32), axis=0, keepdims=True)
        tail = jnp.broadcast_to(norm, (16, DK)).astype(BF16)
        for h in range(2):
            st_own[d, h, 0:256, :] = st[256 * h : 256 * h + 256]
            st_own[d, h, 256:SROWS, :] = tail
        d_st.append(cp.remote(st_own.at[d], st_par.at[d], partner, st_send))
        d_st[d].start()

    stage("wd_block")
    d_wd.wait_recv()
    ei = lax.broadcasted_iota(jnp.int32, (64, 128), 0)
    ej = lax.broadcasted_iota(jnp.int32, (64, 128), 1)
    put_own = jnp.where(ej == ei + 64 * c, 1.0, 0.0).astype(BF16)
    put_par = jnp.where(ej == ei + 64 * other, 1.0, 0.0).astype(BF16)
    mine = wa[:, pl.ds(pl.multiple_of(1024 * c, 1024), 1024)]
    tn = (((0,), (0,)), ((), ()))
    wd[z, y, c] = (
        lax.dot_general(mine, put_own, tn, preferred_element_type=F32)
        + lax.dot_general(wb[...], put_par, tn, preferred_element_type=F32)
    ).astype(BF16)
    b1.start0()

    stage("pair_wait")
    def pick(ref, i):
        return ref[i : i + 1, 0:1]

    def pair_terms(s0, s1, d):
        early, late = (s0, s1) if d == 0 else (s1, s0)
        e_last = early[5 - d : 6 - d, 0:1]
        l_first, l_last = late[4 + d : 5 + d, 0:1], late[5 - d : 6 - d, 0:1]
        linked = (l_first == e_last) & (l_first == l_last)
        e_top = early[d : d + 1, 0:1] + late[2 + d : 3 + d, 0:1]
        l_top = late[d : d + 1, 0:1]
        top = jnp.where(linked, jnp.maximum(l_top, e_top), l_top)
        f_early = jnp.where(linked, jnp.exp(jnp.minimum(e_top - top, 0.0)), 0.0)
        f_late = jnp.exp(l_top - top)
        total = early[2 + d : 3 + d, 0:1] + late[2 + d : 3 + d, 0:1]
        return top, total, f_early, f_late, l_last

    d_sc.wait_recv()
    s0, s1 = sc_pair[0], sc_pair[1]
    cq = []
    cs = []
    for d in range(2):
        pos = c if d == 0 else other
        _, _, f_early, f_late, _ = pair_terms(s0, s1, d)
        f_own = jnp.where(pos == 0, f_early, f_late)
        f_par = jnp.where(pos == 0, f_late, f_early)
        d_st[d].wait_recv()
        q_send[d] = (f_own * st_own[d, c].astype(F32) + f_par * st_par[d, c].astype(F32)).astype(BF16)
        to = chip_up if d == 0 else chip_dn
        cs.append(cp.remote(sc_pair, sc_recv.at[d, 0], to, sc_sends))
        cq.append(cp.remote(q_send.at[d], q_recv.at[d, 0, c], to, q_sends))
        cs[-1].start()
        cq[-1].start()

    stage("intra0")
    l_q.wait()

    def intra(r0, size):
        qb = q[r0 : r0 + size, :]
        mfc, mbc, dc = (cols[r0 : r0 + size, i : i + 1] for i in range(3))
        score = (
            lax.dot_general(qb, k[...], (((1,), (1,)), ((), ())), preferred_element_type=F32)
            * SCALE
        )
        for d in range(2):
            lo, hi = (0, r0 + size) if d == 0 else (r0, T)
            ti = r0 + lax.broadcasted_iota(jnp.int32, (size, hi - lo), 0)
            si = lo + lax.broadcasted_iota(jnp.int32, (size, hi - lo), 1)
            keep = ((si <= ti) if d == 0 else (si >= ti)) & (arow[2, 0:1, lo:hi] == dc)
            e = jnp.exp(jnp.minimum(arow[d, 0:1, lo:hi] - (mfc if d == 0 else mbc), 0.0))
            w = jnp.where(keep, score[:, lo:hi] * e, 0.0)
            dens[r0 : r0 + size, d : d + 1] = jnp.sum(w, axis=1, keepdims=True)
            num = jnp.dot(w.astype(BF16), v[lo:hi, :], preferred_element_type=F32)
            (numf if d == 0 else numb)[r0 : r0 + size, :] = num

    intra(0, 256)
    stage("pieces")
    wp_all.wait_recv()
    c1.start()
    stage("intra1")
    intra(256, 256)
    stage("intra2")
    intra(512, 256)

    stage("c1_relay")
    c1.relay()
    stage("carry_near")
    rq, rs, dq, dq_recv = [], [], [], cp.new_recv()
    for d in range(2):
        to = chip_up if d == 0 else chip_dn
        rs.append(cp.remote(sc_recv.at[d, 0], sc_recv.at[d, 1], to, sc_sends))
        rq.append(cp.remote(q_recv.at[d, 0, c], q_recv.at[d, 1, c], to, q_sends))
        dq.append(cp.remote(q_recv.at[d, 0, c], q_recv.at[d, 0, c], partner, q_sends, dq_recv))
        cs[d].wait_recv()
        rs[d].start()
        cq[d].wait_recv()
        rq[d].start()
        dq[d].start()
    stage("b1_relay")
    b1.start1()
    b1.relay()
    stage("wr_relay")
    wr.relay()
    stage("c1_wait")
    c1.near()
    c1.far()
    c2.start()
    a1.start1()
    a1.relay()
    fo_send, fo_recv = cp.new_send(), cp.new_recv()
    cp.remote(
        wop.at[c, heads, a_pos], wop.at[c, heads, a_pos], partner, fo_send, fo_recv
    ).start()

    stage("carry_far")
    dq2 = []
    for d in range(2):
        rs[d].wait_recv()
        rq[d].wait_recv()
        dq2.append(cp.remote(q_recv.at[d, 1, c], q_recv.at[d, 1, c], partner, q_sends, dq_recv))
        dq2[d].start()
    fw_send = cp.new_send()
    fw_up, fw_up2, fw_dn, fw_dn2 = (cp.new_recv() for _ in range(4))

    def forward(refs, recv, send=fw_send):
        for r in refs:
            cp.remote(r, r, partner, send, recv).start()

    def second_phase():
        stage("c2_relay")
        c2.relay()
        a2o.start1()
        b2o.start()
        a2o.relay()
        wr.near()
        forward([wox.at[j, c] for j in (1, 3)], fo_recv, fo_send)
        stage("emit_rest")

    stage("carry_combine")
    scal_in = []
    for d in range(2):
        pos = c if d == 0 else other
        chip = n if d == 0 else 15 - n
        own_s = sc_pair[c]
        par_s = sc_pair[other]
        first = own_s[4 + d : 5 + d, 0:1]
        t1, tot1, _, _, last1 = pair_terms(sc_recv[d, 0, 0], sc_recv[d, 0, 1], d)
        t2, _, _, _, last2 = pair_terms(sc_recv[d, 1, 0], sc_recv[d, 1, 1], d)
        l0 = (par_s[5 - d : 6 - d, 0:1] == first) & (pos == 1)
        l1 = (last1 == first) & (chip >= 1)
        l2 = (last2 == first) & (chip >= 2)
        shift = jnp.where(pos == 1, par_s[2 + d : 3 + d, 0:1], 0.0)
        e0 = jnp.where(l0, par_s[d : d + 1, 0:1], FAR_LOW)
        e1 = jnp.where(l1, t1 + shift, FAR_LOW)
        e2 = jnp.where(l2, t2 + tot1 + shift, FAR_LOW)
        top = jnp.maximum(e0, jnp.maximum(e1, e2))
        g0 = jnp.where(l0, jnp.exp(e0 - top), 0.0)
        g1 = jnp.where(l1, jnp.exp(e1 - top), 0.0)
        g2 = jnp.where(l2, jnp.exp(e2 - top), 0.0)
        late = jnp.where(pos == 1, 1.0, 0.0)
        linked = late * jnp.where(l0, 1.0, 0.0) + (1.0 - late) * jnp.where(l1, 1.0, 0.0)
        if d == 0:
            cp.waiter(q_recv.at[:, :, 0], q_sends, dq_recv).wait_recv()
        for h in range(2):
            cin[d, h] = (
                g0 * st_par[d, h].astype(F32)
                + g1 * q_recv[d, 0, h].astype(F32)
                + g2 * q_recv[d, 1, h].astype(F32)
            ).astype(BF16)
        scal_in.append((top, linked, first))

    stage("emit")
    for l in (l_og, *l_gain):
        l.wait()
    ca = []
    lo, hi = pl.ds(0, HALF), pl.ds(HALF, HALF)
    for step, to in enumerate((xf, xp, xm, x)):
        r0 = pl.multiple_of(to * ROWS, 64)
        rows = pl.ds(r0, ROWS)
        qb = q[rows, :]
        qw = qb.astype(F32)
        dc = cols[rows, 2:3]
        memory = None
        for d in range(2):
            top, linked, first = scal_in[d]
            m_loc = cols[rows, d : d + 1]
            usable = jnp.where(dc == first, linked, 0.0) > 0.5
            m = jnp.where(usable, jnp.maximum(m_loc, top), m_loc)
            keep = jnp.exp(m_loc - m)
            inter = jnp.where(usable, jnp.exp(jnp.minimum(top - m, 0.0)), 0.0) * SCALE
            nt = (((1,), (1,)), ((), ()))
            qc = jnp.concatenate(
                [
                    lax.dot_general(qb, cin[d, h, 0:256, :], nt, preferred_element_type=F32)
                    for h in range(2)
                ],
                axis=1,
            )
            norm = cin[d, 0, 256:257, :].astype(F32)
            num = keep * (numf if d == 0 else numb)[rows, :] + inter * qc
            den = keep * dens[rows, d : d + 1] + inter * jnp.sum(qw * norm, axis=1, keepdims=True)
            h_dir = num / jnp.maximum(jnp.abs(den), 1.0)
            memory = h_dir if memory is None else memory + h_dir
        normed = memory * lax.rsqrt(jnp.mean(memory * memory, axis=1, keepdims=True) + EPS)
        gate = 1.0 / (1.0 + jnp.exp(-og[rows, :].astype(F32)))
        readout = (normed * gain_ref[...] * gate).astype(BF16)
        if step == 3:
            ro[x] = readout
        else:
            ro_out[step] = readout
        if step == 0:
            ca0 = [
                cp.remote(ro_out.at[0, lo], ro_st.at[0], {"x": xp}, ro_send),
                cp.remote(ro_out.at[0, hi], ro_st.at[1], {"x": xm}, ro_send),
            ]
            for cc in ca0:
                cc.start()
        elif step < 3:
            ca.append(cp.remote(ro_out.at[step], ro.at[x], {"x": to}, ro_send))
            ca[-1].start()
            if step == 1:
                second_phase()
    stage("a1_wait")
    b1.near()
    b1.far()
    b2.start()
    a1.near()
    a1.far()
    a2.start()
    stage("a2a_relay")
    ca += [
        cp.remote(ro_st.at[0], ro.at[xm, lo], {"x": xp}, ro_send),
        cp.remote(ro_st.at[1], ro.at[xp, hi], {"x": xm}, ro_send),
    ]
    for i in range(2):
        ca0[i].wait_recv()
        ca[2 + i].start()

    stage("wout_fwd")
    c2.near()
    forward([wop.at[c, heads, lax.rem(a_pos + i, 4)] for i in (1, 3)], fo_recv, fo_send)
    wr.far()
    forward([wox.at[2, c]], fo_recv, fo_send)
    stage("c2_far")
    c2.far()
    forward([wop.at[c, heads, lax.rem(a_pos + 2, 4)]], fo_recv, fo_send)
    b2o.relay()
    stage("a2a_wait")
    l_re.wait()
    l_wp_all.wait()
    stage("wout")

    def project(j):
        head = ro.at[lax.rem(x + j, 4)]
        base = resid if j == 0 else mixed
        for t in range(4):
            cs_ = slice(512 * t, 512 * t + 512)
            w0 = wox[j, :, :, :, cs_].reshape(512 - 64 * KP, 512)
            at = [wop[t // 2, j, :, 2 * (t % 2) + i].reshape(64 * KP, 256) for i in range(2)]
            one = jnp.dot(head[:, 0 : 512 - 64 * KP], w0, preferred_element_type=F32) + jnp.dot(
                head[:, 512 - 64 * KP : 512],
                jnp.concatenate(at, axis=1),
                preferred_element_type=F32,
            )
            mixed[:, cs_] = base[:, cs_].astype(F32) + one.astype(BF16).astype(F32)

    project(0)
    stage("fo_wait")
    fo_all = cp.waiter(nrm, fo_send, fo_recv)
    fo_all.wait_recv()
    cp.drain.append(fo_all)
    stage("near_wait")
    ca[0].wait_recv()
    project(3)
    ca[1].wait_recv()
    project(1)
    stage("far_wait")
    ca[2].wait_recv()
    ca[3].wait_recv()
    stage("far_project")
    project(2)

    mx = mixed[...]
    factor = lax.rsqrt(jnp.mean(mx * mx, axis=1, keepdims=True) + EPS)
    nrm[0] = (mx * factor * ngain_ref[...]).astype(BF16)

    h01 = lambda j, h: nrm.at[j, pl.ds(HALF * h, HALF)]
    ag = Ring(
        cp, {"x": xp}, {"x": xm},
        lambda h: [h01(0, h)],
        lambda h: [h01(1 + h, 0)],
        lambda h: [h01(2 - h, 1)],
        [h01(1, 0)], [h01(1, 1)], [h01(3, 0)], [h01(3, 1)], nrm.at[0], nrm.at[three],
    )
    ag.start()
    up_most = cp.waiter(wu.at[three, :, 0], fw_send, fw_up)
    up_last = cp.waiter(wu.at[0, :, 0], fw_send, fw_up2)
    dn_most = cp.waiter(wd.at[three, :, 0], fw_send, fw_dn)
    dn_last = cp.waiter(wd.at[0, :, 0], fw_send, fw_dn2)
    cp.drain_later(wu, fw_send, fw_up)

    def up(j, zs, start=None, final=True):
        @pl.loop(0, 4)
        def _(t):
            cs_ = pl.ds(pl.multiple_of(t * 512, 512), 512)
            if zs is None:
                pre = jnp.dot(
                    nrm[j], wu[:, :, :, :, cs_].reshape(D, 512), preferred_element_type=F32
                )
            else:
                pre = start[:, cs_] if start is not None else None
                for zz in zs:
                    one = jnp.dot(
                        nrm[j, :, pl.ds(pl.multiple_of(512 * zz, 512), 512)],
                        wu[zz, :, :, :, cs_].reshape(512, 512),
                        preferred_element_type=F32,
                    )
                    pre = one if pre is None else pre + one
            if final:
                pre = jnp.maximum(pre, 0.0)
                hid[j, :, cs_] = (pre * pre).astype(BF16)
            else:
                acc2[:, cs_] = pre

    def down(j, first, last, sink):
        @pl.loop(first, last)
        def _(t):
            cs_ = pl.ds(pl.multiple_of(t * 512, 512), 512)
            w = jnp.concatenate([wd[t, i].reshape(D, 128) for i in range(4)], axis=1)
            sink(cs_, jnp.dot(hid[j], w, preferred_element_type=F32))

    def add_own(cs_, val):
        mixed[:, cs_] += val

    def to_part(j):
        def sink(cs_, val):
            part[j, :, cs_] = val.astype(BF16)

        return sink

    def to_acc(cs_, val):
        acc2[:, cs_] = val

    rs_send, rs_recv = cp.new_send(), cp.new_recv()
    cp.drain_later(nrm.at[three], rs_send, rs_recv)

    def first_sums(yy):
        w = jnp.concatenate([wd[i, yy].reshape(D, 128) for i in range(4)], axis=1)
        val = jnp.dot(hid[1], w, preferred_element_type=F32).astype(BF16)
        for i in range(4):
            strip = pl.ds(pl.multiple_of((4 * i + yy) * 128, 128), 128)
            part[0, :, strip] = val[:, 128 * i : 128 * i + 128]
        for i in range(4):
            strip = pl.ds(pl.multiple_of((4 * i + yy) * 128, 128), 128)
            for rows, side, to in ((hi, 0, xp), (lo, 1, xm)):
                cp.remote(
                    part.at[0, rows, strip], rs_in.at[side, rows, strip], {"x": to}, rs_send, rs_recv
                ).start()

    up_other, dn_other = (yp, ym, yf), (zp, zm, zf)
    lower, upper = [pl.ds(32 * h, 32) for h in range(2)], [pl.ds(512 * h, 512) for h in range(2)]

    def up_part(row, h):
        return [wu.at[row, o, c, lower[h]] for o in up_other]

    def dn_part(col, h):
        return [wd.at[o, col, c, upper[h]] for o in dn_other]

    stage("own_rows")
    forward([wu.at[z, :, c]], fw_up)
    forward([wd.at[:, y, c]], fw_dn)
    a2o.near()
    a2o.far()
    forward([wu.at[zp, y, c], wu.at[zm, y, c]], fw_up)
    forward([wu.at[zf, y, c]], fw_up2)
    stage("a2_relay")
    a2.relay()
    forward(up_part(zm, 0) + up_part(zp, 1), fw_up)
    stage("b2_relay")
    b2o.near()
    b2.relay()
    forward([wd.at[z, yp, c], wd.at[z, ym, c]], fw_dn)
    forward(dn_part(ym, 0) + dn_part(yp, 1), fw_dn)
    stage("a2_near")
    a2.near()
    forward(up_part(zm, 1) + up_part(zp, 0), fw_up)
    stage("b2_near")
    b2.near()
    forward(dn_part(ym, 1) + dn_part(yp, 0), fw_dn)
    stage("ag_relay")
    ag.relay()
    stage("up1_most")
    up_most.wait_recv()
    up(1, (z, zp, zm), final=False)
    stage("a2_far")
    a2.far()
    forward(up_part(zf, 0) + up_part(zf, 1), fw_up2)
    up_last.wait_recv()
    stage("up1_last")
    up(1, (zf,), start=acc2)
    stage("down1_most")
    dn_most.wait_recv()
    for yy in (y, yp, ym):
        first_sums(yy)
    stage("b2_far")
    b2o.far()
    b2.far()
    forward([wd.at[:, yf, c]], fw_dn2)
    stage("ag_far")
    ag.far()
    stage("up3")
    up(3, None)
    stage("down1_last")
    dn_last.wait_recv()
    first_sums(yf)
    stage("down3")
    rs2, rs3 = [], []
    for i in range(2):
        down(3, 2 * i, 2 * i + 2, to_part(1))
        wide = pl.ds(1024 * i, 1024)
        rs2.append(cp.remote(part.at[1, lo, wide], add_in.at[0, :, wide], {"x": xp}, rs_send))
        rs2.append(cp.remote(part.at[1, hi, wide], add_in.at[1, :, wide], {"x": xm}, rs_send))
        for part_rows, side, to in ((hi, 0, xp), (lo, 1, xm)):
            rs_rows = lo if side == 0 else hi
            rs3.append(
                cp.remote(
                    part.at[2, part_rows, wide], rs_in.at[side, rs_rows, wide], {"x": to},
                    rs_send, rs_recv,
                )
            )
        rs2[-2].start()
        rs2[-1].start()
    stage("ff2")
    ag.near()
    up(2, None)
    down(2, 0, 4, to_acc)
    for i in range(2):
        stage(f"rs_add{i}")
        lanes = slice(1024 * i, 1024 * i + 1024)
        for side in range(2):
            rs2[2 * i + side].wait_recv()
            rows = slice(HALF, ROWS) if side == 0 else slice(0, HALF)
            part[2, rows, lanes] = (
                acc2[rows, lanes] + add_in[side, :, lanes].astype(F32)
            ).astype(BF16)
            rs3[2 * i + side].start()
    stage("up0")
    up(0, None)
    stage("down0")
    down(0, 0, 4, add_own)
    l_mx = cp.local(mixed, own_out)
    l_mx.start()
    stage("rs_wait")
    cp.waiter(rs_in, rs_send, rs_recv).wait_recv()
    cp.drain_later(st_own, st_send, rs_recv)
    cp.drain_later(q_recv, q_sends, rs_recv)
    cp.drain_later(sc_recv, sc_sends, rs_recv)
    cp.drain_later(ro, ro_send, rs_recv)
    l_mx.wait()
    stage("drain")
    assert (cp.sends, cp.recvs, cp.locals) == N_SEMS, (cp.sends, cp.recvs, cp.locals)
    for r in cp.drain:
        r.wait_send()
    stage()


def shards(
    queries, keys, values, out_gate, input_gates, forget_gates, doc_ids,
    head_gain, w_out, resid, norm_gain, w_up, w_down,
):
    hbm = pl.BlockSpec(memory_space=pl.ANY)
    own, sums = pl.pallas_call(
        kernel,
        out_shape=(
            jax.ShapeDtypeStruct((ROWS, D), F32),
            jax.ShapeDtypeStruct((2, ROWS, D), BF16),
        ),
        in_specs=[hbm] * 13,
        out_specs=(hbm, hbm),
        scratch_shapes=[
            pltpu.VMEM((2, 1, T), F32),
            pltpu.VMEM((2, 1, T), F32),
            pltpu.VMEM((T,), jnp.int32),
            pltpu.VMEM((1, DV), F32),
            pltpu.VMEM((1, D), F32),
            pltpu.VMEM((4, 4, 2, 64, D), BF16),
            pltpu.VMEM((4, 4, 2, 1024, 128), BF16),
            pltpu.VMEM((4, 2, WX, 16, D), BF16),
            pltpu.VMEM((2, 4, 4, 4, KP, 16, 256), BF16),
            pltpu.VMEM((64, D), BF16),
            pltpu.VMEM((64, 1024), BF16),
            pltpu.VMEM((T, DK), BF16),
            pltpu.VMEM((T, DK), BF16),
            pltpu.VMEM((T, DV), BF16),
            pltpu.VMEM((T, DV), BF16),
            pltpu.VMEM((ROWS, D), BF16),
            pltpu.VMEM((3, 8, T), F32),
            pltpu.VMEM((T, 8), F32),
            pltpu.VMEM((T, DV), F32),
            pltpu.VMEM((T, DV), F32),
            pltpu.VMEM((T, 8), F32),
            pltpu.VMEM((2, 2, SROWS, DK), BF16),
            pltpu.VMEM((2, 2, SROWS, DK), BF16),
            pltpu.VMEM((2, 8, 128), F32),
            pltpu.VMEM((2, SROWS, DK), BF16),
            pltpu.VMEM((2, 2, 2, SROWS, DK), BF16),
            pltpu.VMEM((2, 2, 2, 8, 128), F32),
            pltpu.VMEM((2, 2, SROWS, DK), BF16),
            pltpu.VMEM((3, ROWS, DV), BF16),
            pltpu.VMEM((2, HALF, DV), BF16),
            pltpu.VMEM((4, ROWS, DV), BF16),
            pltpu.VMEM((ROWS, D), F32),
            pltpu.VMEM((4, ROWS, D), BF16),
            pltpu.VMEM((4, ROWS, D), BF16),
            pltpu.VMEM((3, ROWS, D), BF16),
            pltpu.VMEM((ROWS, D), F32),
            pltpu.VMEM((2, HALF, D), BF16),
            *(pltpu.SemaphoreType.DMA((k,)) for k in N_SEMS),
        ],
        compiler_params=pltpu.CompilerParams(
            collective_id=0, has_side_effects=True, vmem_limit_bytes=66 * 1024 * 1000
        ),
        name="layer",
    )(
        input_gates, forget_gates, doc_ids, head_gain.reshape(1, DV),
        norm_gain.reshape(1, D), queries, keys, values, out_gate, w_out.reshape(32, 16, D), resid, w_up,
        w_down.T,
    )
    return (own + sums[0].astype(F32) + sums[1].astype(F32)).astype(BF16)


def solution(mesh):
    split = Mesh(mesh.devices.reshape(4, 4, 2, mesh.shape["tp"]), ("z", "y", "c", "x"))
    sp = ("z", "y", "c")
    return jax.shard_map(
        shards,
        mesh=split,
        in_specs=(
            P(sp, "x"), P(sp, "x"), P(sp, "x"), P(sp, "x"),
            P(None, "x", sp), P(None, "x", sp), P(sp), P("x"), P("x", None),
            P((*sp, "x"), None), P(), P(sp, "x"), P("x", sp),
        ),
        out_specs=P((*sp, "x"), None),
        check_vma=False,
    )
```

```python
import contextlib

import jax
import jax.numpy as jnp
from jax import lax
from jax.experimental import pallas as pl
from jax.experimental.pallas import tpu as pltpu
from jax.sharding import Mesh
from jax.sharding import PartitionSpec as P

MESH = pl.DeviceIdType.MESH
F32 = jnp.float32
BF16 = jnp.bfloat16
EPS = 1e-06
FAR_LOW = -1e30

T = 768
ROWS = 192
HALF = 96
DK = 256
DV = 512
D = 2048
SROWS = 272
SCALE = DK ** (-0.5)
KP = 3
WX = 16 - 2 * KP
N_SEMS = (20, 60, 16)


class Stages:
    def __init__(self):
        self.scopes = contextlib.ExitStack()

    def __call__(self, name=None):
        self.scopes.close()
        if name:
            self.scopes.enter_context(jax.named_scope(name))


class Copies:
    def __init__(self, send, recv, loc):
        self.send, self.recv, self.loc = send, recv, loc
        self.sends = self.recvs = self.locals = 0
        self.drain = []

    def new_send(self):
        self.sends += 1
        return self.send.at[self.sends - 1]

    def new_recv(self):
        self.recvs += 1
        return self.recv.at[self.recvs - 1]

    def remote(self, src, dst, dev, send=None, recv=None):
        alone = send is None
        c = pltpu.make_async_remote_copy(
            src_ref=src,
            dst_ref=dst,
            send_sem=self.new_send() if alone else send,
            recv_sem=self.new_recv() if recv is None else recv,
            device_id=dev,
            device_id_type=MESH,
        )
        if alone:
            self.drain.append(c)
        return c

    def waiter(self, ref, send, recv):
        return pltpu.make_async_remote_copy(
            src_ref=ref,
            dst_ref=ref,
            send_sem=send,
            recv_sem=recv,
            device_id={"c": 1 - lax.axis_index("c")},
            device_id_type=MESH,
        )

    def drain_later(self, ref, send, recv):
        self.drain.append(self.waiter(ref, send, recv))

    def local(self, src, dst, again=False):
        self.locals += not again
        return pltpu.make_async_copy(src, dst, self.loc.at[self.locals - 1])


class Ring:
    def __init__(
        self, cp, plus, minus, own, put_plus, put_minus, near0, near1, far0, far1, block, three
    ):
        send = cp.new_send()
        self.first, self.second, self.third = (cp.new_recv() for _ in range(3))

        def group(srcs, dsts, dev, recv):
            return [cp.remote(s, d, dev, send, recv) for s, d in zip(srcs, dsts, strict=True)]

        self.out0 = group(own(0), put_plus(0), plus, self.first)
        self.out0 += group(own(1), put_minus(1), minus, self.first)
        self.out1 = group(own(1), put_plus(1), plus, self.second)
        self.out1 += group(own(0), put_minus(0), minus, self.second)
        self.on = group(near0, far0, plus, self.third) + group(near1, far1, minus, self.third)
        self.waits = [cp.waiter(block, send, r) for r in (self.first, self.second, self.third)]
        cp.drain_later(three, send, self.first)

    def start0(self):
        for c in self.out0:
            c.start()

    def start1(self):
        for c in self.out1:
            c.start()

    def start(self):
        self.start0()
        self.start1()

    def relay(self):
        self.waits[0].wait_recv()
        for c in self.on:
            c.start()

    def near(self):
        self.waits[1].wait_recv()

    def far(self):
        self.waits[2].wait_recv()


def slot_ring(cp, plus, minus, p, slots, block, three):
    up, down = lax.rem(p + 1, 4), lax.rem(p + 3, 4)
    at = lambda pos, h: [f(pos, h) for f in slots]
    own = lambda h: at(p, h)
    return Ring(
        cp, plus, minus, own, own, own, at(down, 0), at(up, 1), at(down, 0), at(up, 1), block, three
    )


def roll_lanes(x, shift):
    return pltpu.roll(x, shift % T, 1)


def kernel(
    ig_h, fg_h, doc_h, gain_h, ngain_h,
    q_h, k_h, v_h, og_h, wout_h, resid_h, wup_h, wdn_h,
    own_out, rs_in,
    ig_ref, fg_ref, doc_ref, gain_ref, ngain_ref,
    wu, wd, wox, wop, wa, wb, q, k, v, og, resid,
    arow, cols, numf, numb, dens,
    st_own, st_par, sc_pair, q_send, q_recv, sc_recv, cin,
    ro_out, ro_st, ro, mixed, nrm, hid, part, acc2, add_in,
    send_sem, recv_sem, loc_sem,
):
    z, y, c, x = (lax.axis_index(a) for a in ("z", "y", "c", "x"))
    other = 1 - c
    n = z * 4 + y
    n_up, n_dn = lax.rem(n + 1, 16), lax.rem(n + 15, 16)
    chip_up = {"z": lax.div(n_up, 4), "y": lax.rem(n_up, 4)}
    chip_dn = {"z": lax.div(n_dn, 4), "y": lax.rem(n_dn, 4)}
    partner = {"c": other}
    xp, xm, xf = lax.rem(x + 1, 4), lax.rem(x + 3, 4), lax.rem(x + 2, 4)
    cp = Copies(send_sem, recv_sem, loc_sem)
    stage = Stages()
    stage("loads")

    l_wd = cp.local(wdn_h, wa)
    l_wu = cp.local(wup_h, wu.at[z, y, c])
    l_wo = [cp.local(wout_h.at[pl.ds(WX * i, WX)], wox.at[0, i]) for i in range(2)]
    l_k = cp.local(k_h, k)
    l_v = cp.local(v_h, v)
    l_q = cp.local(q_h, q)
    l_og = cp.local(og_h, og)
    l_wp = [
        cp.local(
            wout_h.at[pl.ds(2 * WX + KP * i, KP), :, pl.ds(1024 * j + 256 * b, 256)],
            wop.at[j, 0, i, b],
            i + j + b > 0,
        )
        for i in range(4)
        for j in range(2)
        for b in range(4)
    ]
    l_wp_all = cp.local(wop.at[:, 0], wop.at[:, 0], True)
    l_re = cp.local(resid_h, resid)
    l_gate = [cp.local(a, b) for a, b in ((ig_h, ig_ref), (fg_h, fg_ref), (doc_h, doc_ref))]
    l_gain = [cp.local(gain_h, gain_ref), cp.local(ngain_h, ngain_ref)]
    loads = (l_wu, *l_gate, l_wd, *l_wo, l_k, l_v, l_q, l_og, *l_gain, *l_wp, l_re)

    stage("barrier")
    barrier = pltpu.get_barrier_semaphore()
    peers = (
        partner, {"y": lax.rem(y + 1, 4)}, {"y": lax.rem(y + 3, 4)}, {"z": lax.rem(z + 1, 4)},
        {"z": lax.rem(z + 3, 4)}, {"x": xp}, {"x": xm}, {"x": xf}, chip_up, chip_dn,
    )
    for dev in peers:
        pl.semaphore_signal(barrier, inc=1, device_id=dev, device_id_type=MESH)
    for l in loads:
        l.start()
    pl.semaphore_wait(barrier, len(peers))

    stage("first_sends")
    zp, zm, zf = lax.rem(z + 1, 4), lax.rem(z + 3, 4), lax.rem(z + 2, 4)
    yp, ym, yf = lax.rem(y + 1, 4), lax.rem(y + 3, 4), lax.rem(y + 2, 4)
    over_y, over_z = ({"y": yp}, {"y": ym}), ({"z": zp}, {"z": zm})
    up_half = lambda a, b, h: wu.at[a, b, c, pl.ds(32 * h, 32)]
    dn_half = lambda a, b, h: wd.at[a, b, c, pl.ds(512 * h, 512)]
    three = pl.ds(0, 3)
    a1 = slot_ring(
        cp, *over_y, y, [lambda p, h: up_half(z, p, h)], wu.at[z, y, c], wu.at[z, three, c]
    )
    a2o = slot_ring(
        cp, *over_z, z, [lambda p, h: up_half(p, y, h)], wu.at[z, y, c], wu.at[z, three, c]
    )
    a2 = slot_ring(
        cp, *over_z, z, [lambda p, h, o=o: up_half(p, o, h) for o in (yp, ym, yf)],
        wu.at[z, three, c], wu.at[three, three, c],
    )
    b1 = slot_ring(
        cp, *over_z, z, [lambda p, h: dn_half(p, y, h)], wd.at[z, y, c], wd.at[z, three, c]
    )
    b2o = slot_ring(
        cp, *over_y, y, [lambda p, h: dn_half(z, p, h)], wd.at[z, y, c], wd.at[z, three, c]
    )
    b2 = slot_ring(
        cp, *over_y, y, [lambda p, h, o=o: dn_half(o, p, h) for o in (zp, zm, zf)],
        wd.at[z, three, c], wd.at[three, three, c],
    )

    wx = lambda j, h: wox.at[j, c, pl.ds(WX // 2 * h, WX // 2)]
    wr = Ring(
        cp, {"x": xp}, {"x": xm},
        lambda h: [wx(0, h)], lambda h: [wx(3, h)], lambda h: [wx(1, h)],
        [wx(3, 0)], [wx(1, 1)], [wx(2, 0)], [wx(2, 1)], wox.at[0, c], wox.at[three, c],
    )
    a_pos, b_pos = jnp.where(c == 0, z, y), jnp.where(c == 0, y, z)
    cols_c = pl.ds(pl.multiple_of(1024 * c + 256 * b_pos, 256), 256)
    wp_send, wp_recv = cp.new_send(), cp.new_recv()
    wp = [
        cp.remote(
            wout_h.at[pl.ds(2 * WX + KP * a_pos, KP), :, cols_c], wop.at[c, j, a_pos, b_pos],
            {"x": to}, wp_send, wp_recv,
        )
        for to, j in ((xp, 3), (xm, 1), (xf, 2))
    ]
    wp_all = cp.waiter(wop.at[c, three, 0, 0], wp_send, wp_recv)
    cp.drain.append(wp_all)

    def dev_b(step):
        return {
            "z": jnp.where(c == 0, z, lax.rem(z + step, 4)),
            "y": jnp.where(c == 0, lax.rem(y + step, 4), y),
        }

    def dev_a(step):
        return {
            "z": jnp.where(c == 0, lax.rem(z + step, 4), z),
            "y": jnp.where(c == 0, y, lax.rem(y + step, 4)),
        }

    heads = pl.ds(1, 3)
    c1 = slot_ring(
        cp, dev_b(1), dev_b(3), b_pos,
        [lambda p, h: wop.at[c, heads, a_pos, p, :, :, pl.ds(128 * h, 128)]],
        wop.at[c, heads, 0, 0], wop.at[c, heads, 0, three],
    )
    c2 = slot_ring(
        cp, dev_a(1), dev_a(3), a_pos,
        [lambda p, h: wop.at[c, heads, p, :, :, :, pl.ds(128 * h, 128)]],
        wop.at[c, heads, 0], wop.at[c, heads, three],
    )

    for w in wp:
        w.start()
    l_wu.wait()
    a1.start0()
    a2o.start0()
    l_wd.wait()
    d_wd = cp.remote(wa.at[:, pl.ds(pl.multiple_of(1024 * other, 1024), 1024)], wb, partner)
    d_wd.start()
    for l in l_wo:
        l.wait()
    wr.start()

    stage("gates")
    for l in l_gate:
        l.wait()
    def row(ref, i):
        return jnp.broadcast_to(ref[i], (8, T))

    lane = lax.broadcasted_iota(jnp.int32, (8, T), 1)
    rowi = lax.broadcasted_iota(jnp.int32, (8, T), 0)
    doc = jnp.broadcast_to(doc_ref[...].astype(F32)[None, :], (8, T))

    def log_sigmoid(f):
        return jnp.minimum(f, 0.0) - jnp.log1p(jnp.exp(-jnp.abs(f)))

    cumf, cumb = log_sigmoid(row(fg_ref, 0)), log_sigmoid(row(fg_ref, 1))
    sh = 1
    while sh < T:
        cumf = cumf + jnp.where(lane >= sh, roll_lanes(cumf, sh), 0.0)
        cumb = cumb + jnp.where(lane < T - sh, roll_lanes(cumb, T - sh), 0.0)
        sh *= 2
    af, ab = row(ig_ref, 0) - cumf, row(ig_ref, 1) - cumb
    mf, mb = af, ab
    sh = 1
    while sh < T:
        same_f = (lane >= sh) & (roll_lanes(doc, sh) == doc)
        same_b = (lane < T - sh) & (roll_lanes(doc, T - sh) == doc)
        mf = jnp.where(same_f, jnp.maximum(mf, roll_lanes(mf, sh)), mf)
        mb = jnp.where(same_b, jnp.maximum(mb, roll_lanes(mb, T - sh)), mb)
        sh *= 2
    doc0, docl = doc[:, 0:1], doc[:, T - 1 : T]
    mxf, mxb = mf[:, T - 1 : T], mb[:, 0:1]
    totf, totb = cumf[:, T - 1 : T], cumb[:, 0:1]
    wf = jnp.where(doc == docl, jnp.exp(af - mxf), 0.0)
    wbk = jnp.where(doc == doc0, jnp.exp(ab - mxb), 0.0)
    arow[0] = af
    arow[1] = ab
    arow[2] = doc
    stack = jnp.where(
        rowi == 0, mf,
        jnp.where(rowi == 1, mb, jnp.where(rowi == 2, doc, jnp.where(rowi == 3, wf, wbk))),
    )
    cols[...] = stack.T
    r8 = lax.broadcasted_iota(jnp.int32, (8, 128), 0)
    scal = jnp.zeros((8, 128), F32)
    for i, val in enumerate((totf + mxf, totb + mxb, totf, totb, doc0, docl)):
        scal = jnp.where(r8 == i, jnp.broadcast_to(val, (8, 128)), scal)
    sc_pair[c] = scal
    d_sc = cp.remote(sc_pair.at[c], sc_pair.at[c], partner)
    d_sc.start()

    stage("state")
    l_k.wait()
    l_v.wait()
    keys = k[...].astype(F32)
    d_st = []
    st_send, q_sends, sc_sends, ro_send = (cp.new_send() for _ in range(4))
    for d in range(2):
        weighted = (keys * cols[:, 3 + d : 4 + d]).astype(BF16)
        st = lax.dot_general(
            v[...], weighted, (((0,), (0,)), ((), ())), preferred_element_type=F32
        ).astype(BF16)
        norm = jnp.sum(weighted.astype(F32), axis=0, keepdims=True)
        tail = jnp.broadcast_to(norm, (16, DK)).astype(BF16)
        for h in range(2):
            st_own[d, h, 0:256, :] = st[256 * h : 256 * h + 256]
            st_own[d, h, 256:SROWS, :] = tail
        d_st.append(cp.remote(st_own.at[d], st_par.at[d], partner, st_send))
        d_st[d].start()

    stage("wd_block")
    d_wd.wait_recv()
    ei = lax.broadcasted_iota(jnp.int32, (64, 128), 0)
    ej = lax.broadcasted_iota(jnp.int32, (64, 128), 1)
    put_own = jnp.where(ej == ei + 64 * c, 1.0, 0.0).astype(BF16)
    put_par = jnp.where(ej == ei + 64 * other, 1.0, 0.0).astype(BF16)
    mine = wa[:, pl.ds(pl.multiple_of(1024 * c, 1024), 1024)]
    tn = (((0,), (0,)), ((), ()))
    wd[z, y, c] = (
        lax.dot_general(mine, put_own, tn, preferred_element_type=F32)
        + lax.dot_general(wb[...], put_par, tn, preferred_element_type=F32)
    ).astype(BF16)
    b1.start0()

    stage("pair_wait")
    def pick(ref, i):
        return ref[i : i + 1, 0:1]

    def pair_terms(s0, s1, d):
        early, late = (s0, s1) if d == 0 else (s1, s0)
        e_last = early[5 - d : 6 - d, 0:1]
        l_first, l_last = late[4 + d : 5 + d, 0:1], late[5 - d : 6 - d, 0:1]
        linked = (l_first == e_last) & (l_first == l_last)
        e_top = early[d : d + 1, 0:1] + late[2 + d : 3 + d, 0:1]
        l_top = late[d : d + 1, 0:1]
        top = jnp.where(linked, jnp.maximum(l_top, e_top), l_top)
        f_early = jnp.where(linked, jnp.exp(jnp.minimum(e_top - top, 0.0)), 0.0)
        f_late = jnp.exp(l_top - top)
        total = early[2 + d : 3 + d, 0:1] + late[2 + d : 3 + d, 0:1]
        return top, total, f_early, f_late, l_last

    d_sc.wait_recv()
    s0, s1 = sc_pair[0], sc_pair[1]
    cq = []
    cs = []
    for d in range(2):
        pos = c if d == 0 else other
        _, _, f_early, f_late, _ = pair_terms(s0, s1, d)
        f_own = jnp.where(pos == 0, f_early, f_late)
        f_par = jnp.where(pos == 0, f_late, f_early)
        d_st[d].wait_recv()
        q_send[d] = (f_own * st_own[d, c].astype(F32) + f_par * st_par[d, c].astype(F32)).astype(BF16)
        to = chip_up if d == 0 else chip_dn
        cs.append(cp.remote(sc_pair, sc_recv.at[d, 0], to, sc_sends))
        cq.append(cp.remote(q_send.at[d], q_recv.at[d, 0, c], to, q_sends))
        cs[-1].start()
        cq[-1].start()

    stage("intra0")
    l_q.wait()

    def intra(r0, size):
        qb = q[r0 : r0 + size, :]
        mfc, mbc, dc = (cols[r0 : r0 + size, i : i + 1] for i in range(3))
        score = (
            lax.dot_general(qb, k[...], (((1,), (1,)), ((), ())), preferred_element_type=F32)
            * SCALE
        )
        for d in range(2):
            lo, hi = (0, r0 + size) if d == 0 else (r0, T)
            ti = r0 + lax.broadcasted_iota(jnp.int32, (size, hi - lo), 0)
            si = lo + lax.broadcasted_iota(jnp.int32, (size, hi - lo), 1)
            keep = ((si <= ti) if d == 0 else (si >= ti)) & (arow[2, 0:1, lo:hi] == dc)
            e = jnp.exp(jnp.minimum(arow[d, 0:1, lo:hi] - (mfc if d == 0 else mbc), 0.0))
            w = jnp.where(keep, score[:, lo:hi] * e, 0.0)
            dens[r0 : r0 + size, d : d + 1] = jnp.sum(w, axis=1, keepdims=True)
            num = jnp.dot(w.astype(BF16), v[lo:hi, :], preferred_element_type=F32)
            (numf if d == 0 else numb)[r0 : r0 + size, :] = num

    intra(0, 256)
    stage("pieces")
    wp_all.wait_recv()
    c1.start()
    stage("intra1")
    intra(256, 256)
    stage("intra2")
    intra(512, 256)

    stage("c1_relay")
    c1.relay()
    stage("carry_near")
    rq, rs, dq, dq_recv = [], [], [], cp.new_recv()
    for d in range(2):
        to = chip_up if d == 0 else chip_dn
        rs.append(cp.remote(sc_recv.at[d, 0], sc_recv.at[d, 1], to, sc_sends))
        rq.append(cp.remote(q_recv.at[d, 0, c], q_recv.at[d, 1, c], to, q_sends))
        dq.append(cp.remote(q_recv.at[d, 0, c], q_recv.at[d, 0, c], partner, q_sends, dq_recv))
        cs[d].wait_recv()
        rs[d].start()
        cq[d].wait_recv()
        rq[d].start()
        dq[d].start()
    stage("b1_relay")
    b1.start1()
    b1.relay()
    stage("wr_relay")
    wr.relay()
    stage("c1_wait")
    c1.near()
    c1.far()
    c2.start()
    a1.start1()
    a1.relay()
    fo_send, fo_recv = cp.new_send(), cp.new_recv()
    cp.remote(
        wop.at[c, heads, a_pos], wop.at[c, heads, a_pos], partner, fo_send, fo_recv
    ).start()

    stage("carry_far")
    dq2 = []
    for d in range(2):
        rs[d].wait_recv()
        rq[d].wait_recv()
        dq2.append(cp.remote(q_recv.at[d, 1, c], q_recv.at[d, 1, c], partner, q_sends, dq_recv))
        dq2[d].start()
    fw_send = cp.new_send()
    fw_up, fw_up2, fw_dn, fw_dn2 = (cp.new_recv() for _ in range(4))

    def forward(refs, recv, send=fw_send):
        for r in refs:
            cp.remote(r, r, partner, send, recv).start()

    def second_phase():
        stage("c2_relay")
        c2.relay()
        a2o.start1()
        b2o.start()
        a2o.relay()
        wr.near()
        forward([wox.at[j, c] for j in (1, 3)], fo_recv, fo_send)
        stage("emit_rest")

    stage("carry_combine")
    scal_in = []
    for d in range(2):
        pos = c if d == 0 else other
        chip = n if d == 0 else 15 - n
        own_s = sc_pair[c]
        par_s = sc_pair[other]
        first = own_s[4 + d : 5 + d, 0:1]
        t1, tot1, _, _, last1 = pair_terms(sc_recv[d, 0, 0], sc_recv[d, 0, 1], d)
        t2, _, _, _, last2 = pair_terms(sc_recv[d, 1, 0], sc_recv[d, 1, 1], d)
        l0 = (par_s[5 - d : 6 - d, 0:1] == first) & (pos == 1)
        l1 = (last1 == first) & (chip >= 1)
        l2 = (last2 == first) & (chip >= 2)
        shift = jnp.where(pos == 1, par_s[2 + d : 3 + d, 0:1], 0.0)
        e0 = jnp.where(l0, par_s[d : d + 1, 0:1], FAR_LOW)
        e1 = jnp.where(l1, t1 + shift, FAR_LOW)
        e2 = jnp.where(l2, t2 + tot1 + shift, FAR_LOW)
        top = jnp.maximum(e0, jnp.maximum(e1, e2))
        g0 = jnp.where(l0, jnp.exp(e0 - top), 0.0)
        g1 = jnp.where(l1, jnp.exp(e1 - top), 0.0)
        g2 = jnp.where(l2, jnp.exp(e2 - top), 0.0)
        late = jnp.where(pos == 1, 1.0, 0.0)
        linked = late * jnp.where(l0, 1.0, 0.0) + (1.0 - late) * jnp.where(l1, 1.0, 0.0)
        if d == 0:
            cp.waiter(q_recv.at[:, :, 0], q_sends, dq_recv).wait_recv()
        for h in range(2):
            cin[d, h] = (
                g0 * st_par[d, h].astype(F32)
                + g1 * q_recv[d, 0, h].astype(F32)
                + g2 * q_recv[d, 1, h].astype(F32)
            ).astype(BF16)
        scal_in.append((top, linked, first))

    stage("emit")
    for l in (l_og, *l_gain):
        l.wait()
    ca = []
    lo, hi = pl.ds(0, HALF), pl.ds(HALF, HALF)
    for step, to in enumerate((xf, xp, xm, x)):
        r0 = pl.multiple_of(to * ROWS, 64)
        rows = pl.ds(r0, ROWS)
        qb = q[rows, :]
        qw = qb.astype(F32)
        dc = cols[rows, 2:3]
        memory = None
        for d in range(2):
            top, linked, first = scal_in[d]
            m_loc = cols[rows, d : d + 1]
            usable = jnp.where(dc == first, linked, 0.0) > 0.5
            m = jnp.where(usable, jnp.maximum(m_loc, top), m_loc)
            keep = jnp.exp(m_loc - m)
            inter = jnp.where(usable, jnp.exp(jnp.minimum(top - m, 0.0)), 0.0) * SCALE
            nt = (((1,), (1,)), ((), ()))
            qc = jnp.concatenate(
                [
                    lax.dot_general(qb, cin[d, h, 0:256, :], nt, preferred_element_type=F32)
                    for h in range(2)
                ],
                axis=1,
            )
            norm = cin[d, 0, 256:257, :].astype(F32)
            num = keep * (numf if d == 0 else numb)[rows, :] + inter * qc
            den = keep * dens[rows, d : d + 1] + inter * jnp.sum(qw * norm, axis=1, keepdims=True)
            h_dir = num / jnp.maximum(jnp.abs(den), 1.0)
            memory = h_dir if memory is None else memory + h_dir
        normed = memory * lax.rsqrt(jnp.mean(memory * memory, axis=1, keepdims=True) + EPS)
        gate = 1.0 / (1.0 + jnp.exp(-og[rows, :].astype(F32)))
        readout = (normed * gain_ref[...] * gate).astype(BF16)
        if step == 3:
            ro[x] = readout
        else:
            ro_out[step] = readout
        if step == 0:
            ca0 = [
                cp.remote(ro_out.at[0, lo], ro_st.at[0], {"x": xp}, ro_send),
                cp.remote(ro_out.at[0, hi], ro_st.at[1], {"x": xm}, ro_send),
            ]
            for cc in ca0:
                cc.start()
        elif step < 3:
            ca.append(cp.remote(ro_out.at[step], ro.at[x], {"x": to}, ro_send))
            ca[-1].start()
            if step == 1:
                second_phase()
    stage("a1_wait")
    a1.near()
    a1.far()
    a2.start()
    b1.near()
    b1.far()
    b2.start()
    stage("a2a_relay")
    ca += [
        cp.remote(ro_st.at[0], ro.at[xm, lo], {"x": xp}, ro_send),
        cp.remote(ro_st.at[1], ro.at[xp, hi], {"x": xm}, ro_send),
    ]
    for i in range(2):
        ca0[i].wait_recv()
        ca[2 + i].start()

    stage("wout_fwd")
    c2.near()
    forward([wop.at[c, heads, lax.rem(a_pos + i, 4)] for i in (1, 3)], fo_recv, fo_send)
    wr.far()
    forward([wox.at[2, c]], fo_recv, fo_send)
    stage("c2_far")
    c2.far()
    forward([wop.at[c, heads, lax.rem(a_pos + 2, 4)]], fo_recv, fo_send)
    b2o.relay()
    stage("a2a_wait")
    l_re.wait()
    l_wp_all.wait()
    stage("wout")

    def project(j):
        head = ro.at[lax.rem(x + j, 4)]
        base = resid if j == 0 else mixed
        for t in range(4):
            cs_ = slice(512 * t, 512 * t + 512)
            w0 = wox[j, :, :, :, cs_].reshape(512 - 64 * KP, 512)
            at = [wop[t // 2, j, :, 2 * (t % 2) + i].reshape(64 * KP, 256) for i in range(2)]
            one = jnp.dot(head[:, 0 : 512 - 64 * KP], w0, preferred_element_type=F32) + jnp.dot(
                head[:, 512 - 64 * KP : 512],
                jnp.concatenate(at, axis=1),
                preferred_element_type=F32,
            )
            mixed[:, cs_] = base[:, cs_].astype(F32) + one.astype(BF16).astype(F32)

    project(0)
    stage("fo_wait")
    fo_all = cp.waiter(nrm, fo_send, fo_recv)
    fo_all.wait_recv()
    cp.drain.append(fo_all)
    stage("near_wait")
    ca[0].wait_recv()
    project(3)
    ca[1].wait_recv()
    project(1)
    stage("far_wait")
    ca[2].wait_recv()
    ca[3].wait_recv()
    stage("far_project")
    project(2)

    mx = mixed[...]
    factor = lax.rsqrt(jnp.mean(mx * mx, axis=1, keepdims=True) + EPS)
    nrm[0] = (mx * factor * ngain_ref[...]).astype(BF16)

    h01 = lambda j, h: nrm.at[j, pl.ds(HALF * h, HALF)]
    ag = Ring(
        cp, {"x": xp}, {"x": xm},
        lambda h: [h01(0, h)],
        lambda h: [h01(1 + h, 0)],
        lambda h: [h01(2 - h, 1)],
        [h01(1, 0)], [h01(1, 1)], [h01(3, 0)], [h01(3, 1)], nrm.at[0], nrm.at[three],
    )
    ag.start()
    up_most = cp.waiter(wu.at[three, :, 0], fw_send, fw_up)
    up_last = cp.waiter(wu.at[0, :, 0], fw_send, fw_up2)
    dn_most = cp.waiter(wd.at[three, :, 0], fw_send, fw_dn)
    dn_last = cp.waiter(wd.at[0, :, 0], fw_send, fw_dn2)
    cp.drain_later(wu, fw_send, fw_up)

    def up(j, zs, start=None, final=True):
        @pl.loop(0, 4)
        def _(t):
            cs_ = pl.ds(pl.multiple_of(t * 512, 512), 512)
            if zs is None:
                pre = jnp.dot(
                    nrm[j], wu[:, :, :, :, cs_].reshape(D, 512), preferred_element_type=F32
                )
            else:
                pre = start[:, cs_] if start is not None else None
                for zz in zs:
                    one = jnp.dot(
                        nrm[j, :, pl.ds(pl.multiple_of(512 * zz, 512), 512)],
                        wu[zz, :, :, :, cs_].reshape(512, 512),
                        preferred_element_type=F32,
                    )
                    pre = one if pre is None else pre + one
            if final:
                pre = jnp.maximum(pre, 0.0)
                hid[j, :, cs_] = (pre * pre).astype(BF16)
            else:
                acc2[:, cs_] = pre

    def down(j, first, last, sink):
        @pl.loop(first, last)
        def _(t):
            cs_ = pl.ds(pl.multiple_of(t * 512, 512), 512)
            w = jnp.concatenate([wd[t, i].reshape(D, 128) for i in range(4)], axis=1)
            sink(cs_, jnp.dot(hid[j], w, preferred_element_type=F32))

    def add_own(cs_, val):
        mixed[:, cs_] += val

    def to_part(j):
        def sink(cs_, val):
            part[j, :, cs_] = val.astype(BF16)

        return sink

    def to_acc(cs_, val):
        acc2[:, cs_] = val

    rs_send, rs_recv = cp.new_send(), cp.new_recv()
    cp.drain_later(nrm.at[three], rs_send, rs_recv)

    def first_sums(yy):
        w = jnp.concatenate([wd[i, yy].reshape(D, 128) for i in range(4)], axis=1)
        val = jnp.dot(hid[1], w, preferred_element_type=F32).astype(BF16)
        for i in range(4):
            strip = pl.ds(pl.multiple_of((4 * i + yy) * 128, 128), 128)
            part[0, :, strip] = val[:, 128 * i : 128 * i + 128]
        for i in range(4):
            strip = pl.ds(pl.multiple_of((4 * i + yy) * 128, 128), 128)
            for rows, side, to in ((hi, 0, xp), (lo, 1, xm)):
                cp.remote(
                    part.at[0, rows, strip], rs_in.at[side, rows, strip], {"x": to}, rs_send, rs_recv
                ).start()

    up_other, dn_other = (yp, ym, yf), (zp, zm, zf)
    lower, upper = [pl.ds(32 * h, 32) for h in range(2)], [pl.ds(512 * h, 512) for h in range(2)]

    def up_part(row, h):
        return [wu.at[row, o, c, lower[h]] for o in up_other]

    def dn_part(col, h):
        return [wd.at[o, col, c, upper[h]] for o in dn_other]

    stage("own_rows")
    forward([wu.at[z, :, c]], fw_up)
    forward([wd.at[:, y, c]], fw_dn)
    a2o.near()
    a2o.far()
    forward([wu.at[zp, y, c], wu.at[zm, y, c]], fw_up)
    forward([wu.at[zf, y, c]], fw_up2)
    stage("a2_relay")
    a2.relay()
    forward(up_part(zm, 0) + up_part(zp, 1), fw_up)
    stage("b2_relay")
    b2o.near()
    b2.relay()
    forward([wd.at[z, yp, c], wd.at[z, ym, c]], fw_dn)
    forward(dn_part(ym, 0) + dn_part(yp, 1), fw_dn)
    stage("a2_near")
    a2.near()
    forward(up_part(zm, 1) + up_part(zp, 0), fw_up)
    stage("b2_near")
    b2.near()
    forward(dn_part(ym, 1) + dn_part(yp, 0), fw_dn)
    stage("ag_relay")
    ag.relay()
    stage("up1_most")
    up_most.wait_recv()
    up(1, (z, zp, zm), final=False)
    stage("a2_far")
    a2.far()
    forward(up_part(zf, 0) + up_part(zf, 1), fw_up2)
    up_last.wait_recv()
    stage("up1_last")
    up(1, (zf,), start=acc2)
    stage("down1_most")
    dn_most.wait_recv()
    for yy in (y, yp, ym):
        first_sums(yy)
    stage("b2_far")
    b2o.far()
    b2.far()
    forward([wd.at[:, yf, c]], fw_dn2)
    stage("ag_far")
    ag.far()
    stage("up3")
    up(3, None)
    stage("down1_last")
    dn_last.wait_recv()
    first_sums(yf)
    stage("down3")
    rs2, rs3 = [], []
    for i in range(2):
        down(3, 2 * i, 2 * i + 2, to_part(1))
        wide = pl.ds(1024 * i, 1024)
        rs2.append(cp.remote(part.at[1, lo, wide], add_in.at[0, :, wide], {"x": xp}, rs_send))
        rs2.append(cp.remote(part.at[1, hi, wide], add_in.at[1, :, wide], {"x": xm}, rs_send))
        for part_rows, side, to in ((hi, 0, xp), (lo, 1, xm)):
            rs_rows = lo if side == 0 else hi
            rs3.append(
                cp.remote(
                    part.at[2, part_rows, wide], rs_in.at[side, rs_rows, wide], {"x": to},
                    rs_send, rs_recv,
                )
            )
        rs2[-2].start()
        rs2[-1].start()
    stage("ff2")
    ag.near()
    up(2, None)
    down(2, 0, 4, to_acc)
    for i in range(2):
        stage(f"rs_add{i}")
        lanes = slice(1024 * i, 1024 * i + 1024)
        for side in range(2):
            rs2[2 * i + side].wait_recv()
            rows = slice(HALF, ROWS) if side == 0 else slice(0, HALF)
            part[2, rows, lanes] = (
                acc2[rows, lanes] + add_in[side, :, lanes].astype(F32)
            ).astype(BF16)
            rs3[2 * i + side].start()
    stage("up0")
    up(0, None)
    stage("down0")
    down(0, 0, 4, add_own)
    l_mx = cp.local(mixed, own_out)
    l_mx.start()
    stage("rs_wait")
    cp.waiter(rs_in, rs_send, rs_recv).wait_recv()
    cp.drain_later(st_own, st_send, rs_recv)
    cp.drain_later(q_recv, q_sends, rs_recv)
    cp.drain_later(sc_recv, sc_sends, rs_recv)
    cp.drain_later(ro, ro_send, rs_recv)
    l_mx.wait()
    stage("drain")
    assert (cp.sends, cp.recvs, cp.locals) == N_SEMS, (cp.sends, cp.recvs, cp.locals)
    for r in cp.drain:
        r.wait_send()
    stage()


def shards(
    queries, keys, values, out_gate, input_gates, forget_gates, doc_ids,
    head_gain, w_out, resid, norm_gain, w_up, w_down,
):
    hbm = pl.BlockSpec(memory_space=pl.ANY)
    own, sums = pl.pallas_call(
        kernel,
        out_shape=(
            jax.ShapeDtypeStruct((ROWS, D), F32),
            jax.ShapeDtypeStruct((2, ROWS, D), BF16),
        ),
        in_specs=[hbm] * 13,
        out_specs=(hbm, hbm),
        scratch_shapes=[
            pltpu.VMEM((2, 1, T), F32),
            pltpu.VMEM((2, 1, T), F32),
            pltpu.VMEM((T,), jnp.int32),
            pltpu.VMEM((1, DV), F32),
            pltpu.VMEM((1, D), F32),
            pltpu.VMEM((4, 4, 2, 64, D), BF16),
            pltpu.VMEM((4, 4, 2, 1024, 128), BF16),
            pltpu.VMEM((4, 2, WX, 16, D), BF16),
            pltpu.VMEM((2, 4, 4, 4, KP, 16, 256), BF16),
            pltpu.VMEM((64, D), BF16),
            pltpu.VMEM((64, 1024), BF16),
            pltpu.VMEM((T, DK), BF16),
            pltpu.VMEM((T, DK), BF16),
            pltpu.VMEM((T, DV), BF16),
            pltpu.VMEM((T, DV), BF16),
            pltpu.VMEM((ROWS, D), BF16),
            pltpu.VMEM((3, 8, T), F32),
            pltpu.VMEM((T, 8), F32),
            pltpu.VMEM((T, DV), F32),
            pltpu.VMEM((T, DV), F32),
            pltpu.VMEM((T, 8), F32),
            pltpu.VMEM((2, 2, SROWS, DK), BF16),
            pltpu.VMEM((2, 2, SROWS, DK), BF16),
            pltpu.VMEM((2, 8, 128), F32),
            pltpu.VMEM((2, SROWS, DK), BF16),
            pltpu.VMEM((2, 2, 2, SROWS, DK), BF16),
            pltpu.VMEM((2, 2, 2, 8, 128), F32),
            pltpu.VMEM((2, 2, SROWS, DK), BF16),
            pltpu.VMEM((3, ROWS, DV), BF16),
            pltpu.VMEM((2, HALF, DV), BF16),
            pltpu.VMEM((4, ROWS, DV), BF16),
            pltpu.VMEM((ROWS, D), F32),
            pltpu.VMEM((4, ROWS, D), BF16),
            pltpu.VMEM((4, ROWS, D), BF16),
            pltpu.VMEM((3, ROWS, D), BF16),
            pltpu.VMEM((ROWS, D), F32),
            pltpu.VMEM((2, HALF, D), BF16),
            *(pltpu.SemaphoreType.DMA((k,)) for k in N_SEMS),
        ],
        compiler_params=pltpu.CompilerParams(
            collective_id=0, has_side_effects=True, vmem_limit_bytes=66 * 1024 * 1000
        ),
        name="layer",
    )(
        input_gates, forget_gates, doc_ids, head_gain.reshape(1, DV),
        norm_gain.reshape(1, D), queries, keys, values, out_gate, w_out.reshape(32, 16, D), resid, w_up,
        w_down.T,
    )
    return (own + sums[0].astype(F32) + sums[1].astype(F32)).astype(BF16)


def solution(mesh):
    split = Mesh(mesh.devices.reshape(4, 4, 2, mesh.shape["tp"]), ("z", "y", "c", "x"))
    sp = ("z", "y", "c")
    return jax.shard_map(
        shards,
        mesh=split,
        in_specs=(
            P(sp, "x"), P(sp, "x"), P(sp, "x"), P(sp, "x"),
            P(None, "x", sp), P(None, "x", sp), P(sp), P("x"), P("x", None),
            P((*sp, "x"), None), P(), P(sp, "x"), P("x", sp),
        ),
        out_specs=P((*sp, "x"), None),
        check_vma=False,
    )
```
